512 devices in a mesh: sp: 16 (over z), tp: 4 (over y), dp: 8 (over x, core).
Axes of the slice: x: 4, y: 4, z: 16, core: 2. Of those that a mesh axis runs over, the one named last changes fastest.
Arguments:
- latents: bfloat16 [16384, 2048], P(('dp', 'sp', 'tp')), parts along dimension 0, may hold values from -6 to 6
- sample_vector: float32 [8, 2048], P('dp'), parts along dimension 0, may hold values from -6 to 6
- context: bfloat16 [2048, 2048], P(('dp', 'sp')), parts along dimension 0, may hold values from -6 to 6
- context_vector: float32 [1, 2048], replicated, may hold values from -6 to 6
- norm_gain: float32 [2048], replicated, may hold values from 0.1 to 1.9
- modulator: bfloat16 [2048, 6144], P(None, ('sp', 'tp')), may hold values from -0.25 to 0.25
- query_weight: bfloat16 [2048, 1024], P('sp', 'tp'), may hold values from -0.125 to 0.125
- key_weight: bfloat16 [2048, 1024], P('sp', 'tp'), may hold values from -0.125 to 0.125
- value_weight: bfloat16 [2048, 2048], P('sp', 'tp'), may hold values from -0.125 to 0.125
- decay_down: bfloat16 [2048, 64], replicated, may hold values from -0.125 to 0.125
- decay_up: bfloat16 [2, 32, 1024], P(None, None, 'tp'), may hold values from -1 to 1
- decay_bias: float32 [2, 1024], P(None, 'tp'), as said below
- decay_extra: float32 [2, 16384, 8], P(None, ('dp', 'sp'), 'tp'), parts along dimension 1, may hold values from -2 to 0
- head_gain: float32 [256], replicated, may hold values from 0.1 to 1.9
- out_weight: bfloat16 [2048, 2048], P('tp'), may hold values from -0.125 to 0.125
Outputs:
- updated: bfloat16 [16384, 2048], P(('dp', 'sp', 'tp')), parts along dimension 0
The draws below stay inside these ranges and needn't reach their ends.
There are 8 independent parts, one for each index of `dp`. The reference program is written for one: setup_inputs(seed, part) draws one part's arguments, and reference() takes and returns one part's arrays. A program takes and returns all parts, laid end to end along the dimension named above; an argument that names none is the same for every part. Nothing has to cross between parts.
Inputs may be any that keep to these rules, and one draw needn't show every extreme that they name: `decay_bias`: offsets of the decay gates,.
All inputs are finite; a program needn't handle non-finite values.
Results may differ from the reference program's by a relative error of at most 0.012.
Values may be sent and summed in bfloat16 or wider, within the bound.
No kernel may reach another device: no remote copies, remote signals or barrier semaphores. Data moves between devices by JAX's collectives and lax.ppermute only.
A program may use at most 64 MiB of HBM per device.

```python
import jax
import jax.numpy as jnp
from jax import lax

D = 2048
HEADS = 8
DK = 128
DV = 256
RANK = 32
BLOCK = 64
CTX_LIFT = 4
CTX = 256
TOK_DEV = 128
TOKENS = 2048
N_TP = 4


def draw_decay_bias(key, part):
    pick_key, slow_key, fast_key = jax.random.split(jax.random.fold_in(key, 11), 3)
    fast_limit = 5
    is_fast = jax.random.randint(pick_key, (2, HEADS, 1), 0, 10) < fast_limit
    slow_level = jnp.log(1.65 * TOKENS / 4.8)
    slow = slow_level + jax.random.uniform(slow_key, (2, HEADS, DK), jnp.float32, -0.5, 0.5)
    fast = jax.random.uniform(fast_key, (2, HEADS, DK), jnp.float32, -0.5, 1.5)
    return jnp.where(is_fast, fast, slow).reshape(2, HEADS * DK).astype(jnp.float32)


def draw_decay_extra(key, part):
    base_key, place_key, size_key = jax.random.split(jax.random.fold_in(key, 23), 3)
    block_count = TOKENS // TOK_DEV
    rates = jnp.exp(jax.random.uniform(base_key, (2, block_count, HEADS), jnp.float32, jnp.log(0.4), jnp.log(2.5)))
    baseline_magnitude = -(0.8 / TOKENS) * jnp.repeat(rates, TOK_DEV, axis=1)
    places = jax.random.randint(place_key, (2, 2, HEADS), 0, TOKENS)
    objective_totals = jnp.log(1.0 - jax.random.uniform(size_key, (2, 2, HEADS), jnp.float32, 0.2, 0.5))
    positions = jnp.arange(TOKENS, dtype=jnp.int32)
    agreement_tally = positions[None, None, :, None] == places[:, :, None, :]
    cluster_batches = jnp.sum(jnp.where(agreement_tally, objective_totals[:, :, None, :], 0.0), axis=1)
    return (baseline_magnitude + cluster_batches).astype(jnp.float32)


def level_of(stream_key, extent, cuts, smallest, top_value):
    def one(dim, shards_of):
        draws = jax.random.uniform(jax.random.fold_in(jax.random.fold_in(stream_key, 6), dim), (shards_of,), jnp.float32, smallest / len(cuts), top_value / len(cuts))
        return jnp.repeat(jnp.exp(draws), extent[dim] // shards_of).reshape((-1,) + (1,) * (len(extent) - dim - 1))

    factor_of = one(*cuts[0])
    for cut in cuts[1:]:
        factor_of = factor_of * one(*cut)
    return factor_of


def centred(key, dims, width, limit, cuts=(), held_as=jnp.bfloat16):
    drawn = jax.random.normal(key, dims, jnp.float32) * width
    if len(cuts) > 0:
        drawn = level_of(key, dims, cuts, -0.22, 0.18) * drawn
    return jnp.clip(drawn, min=-limit, max=limit).astype(held_as)


def setup_inputs(seed: int = 0, part: int = 0) -> dict:
    splits = jax.random.split(jax.random.key(seed), 16)
    part_keys = jax.random.split(jax.random.fold_in(splits[15], part), 16)
    latents = centred(part_keys[0], (TOKENS, D), 1.0, 6.0, ((0, 64),))
    sample_vector = centred(part_keys[1], (1, D), 1.0, 6.0, (), jnp.float32)
    context = centred(part_keys[2], (CTX, D), 1.0, 6.0, ((0, 16),))
    context_vector = centred(splits[3], (1, D), 1.0, 6.0, (), jnp.float32)
    norm_gain = jnp.clip(1.0 + 0.18 * jax.random.normal(splits[4], (D,), jnp.float32), 0.1, 1.9)
    modulator = centred(splits[5], (D, 3 * D), (D // 4) ** -0.5, 0.25, ((1, 64),))
    query_weight = centred(splits[6], (D, HEADS * DK), D ** -0.5, 0.125, ((0, 16), (1, 4)))
    key_weight = centred(splits[7], (D, HEADS * DK), D ** -0.5, 0.125, ((0, 16), (1, 4)))
    value_weight = centred(splits[8], (D, HEADS * DV), D ** -0.5, 0.125, ((0, 16), (1, 4)))
    decay_down = centred(splits[9], (D, 2 * RANK), D ** -0.5, 0.125)
    decay_up = centred(splits[10], (2, RANK, HEADS * DK), RANK ** -0.5, 1.0, ((2, 4),))
    decay_bias = draw_decay_bias(jax.random.fold_in(splits[15], 71), part)
    decay_extra = draw_decay_extra(jax.random.fold_in(jax.random.fold_in(splits[15], part), 71), part)
    head_gain = jnp.clip(1.0 + 0.18 * jax.random.normal(splits[13], (DV,), jnp.float32), 0.1, 1.9)
    out_weight = centred(splits[14], (HEADS * DV, D), (HEADS * DV) ** -0.5, 0.125, ((0, 4),))
    return dict(latents=latents, sample_vector=sample_vector, context=context, context_vector=context_vector, norm_gain=norm_gain, modulator=modulator, query_weight=query_weight, key_weight=key_weight, value_weight=value_weight, decay_down=decay_down, decay_up=decay_up, decay_bias=decay_bias, decay_extra=decay_extra, head_gain=head_gain, out_weight=out_weight)


epsilon = 1e-06
exponential_sharpness = 16.0
precise = lax.Precision.HIGHEST

def rms_rows(values, gains):
    values = values.astype(jnp.float32)
    return values * lax.rsqrt(lax.optimization_barrier(jnp.mean(values * values, axis=-1, keepdims=True)) + epsilon) * gains

def modulated(tokens, gains, modulation, model_width):
    shift_vector = modulation[:model_width]
    scale_vector = modulation[model_width:2 * model_width]
    return (rms_rows(tokens, gains) * (1.0 + scale_vector) + shift_vector).astype(jnp.bfloat16)

def log_decays(low_rank, decay_up, decay_bias):
    fragment_sequence = []
    for direction in range(2):
        low_piece = lax.optimization_barrier(low_rank[:, direction * RANK:(direction + 1) * RANK]).astype(jnp.float32)
        unnormalized_ratings = jnp.dot(low_piece, decay_up[direction].astype(jnp.float32), precision=precise) + decay_bias[direction]
        fragment_sequence.append(jax.nn.log_sigmoid(unnormalized_ratings) / exponential_sharpness)
    return jnp.stack(fragment_sequence)

def sweep(queries, key_rows, value_rows, decays, carried):
    block_count = queries.shape[0] // BLOCK
    lower_mask = jnp.tril(jnp.ones((BLOCK, BLOCK), dtype=bool))

    def to_blocks(values):
        return values.reshape((block_count, BLOCK) + values.shape[1:])

    def advance(carried, inputs):
        query_block, key_block, value_block, decay_block = inputs
        within = jnp.cumsum(decay_block, axis=0)
        block_total = within[-1]
        query_dec = query_block * jnp.exp(within)
        scores = jnp.einsum('chd,shd->hcs', query_dec, key_block * jnp.exp(-within), precision=precise)
        scores = jnp.where(lower_mask[None], scores, 0.0)
        output = jnp.einsum('hcs,she->che', scores, value_block, precision=precise)
        output = output + jnp.einsum('chd,hde->che', query_dec, carried, precision=precise)
        update = jnp.einsum('shd,she->hde', key_block * jnp.exp(block_total - within), value_block, precision=precise)
        return (jnp.exp(block_total)[:, :, None] * carried + update, output)
    carried, outputs = lax.scan(advance, carried, (to_blocks(queries), to_blocks(key_rows), to_blocks(value_rows), to_blocks(decays)))
    return (carried, outputs.reshape(queries.shape[0], queries.shape[1], value_rows.shape[2]))

def reference(latents, sample_vector, context, context_vector, norm_gain, modulator, query_weight, key_weight, value_weight, decay_down, decay_up, decay_bias, decay_extra, head_gain, out_weight):
    model_width = latents.shape[1]
    conditions = jax.nn.silu(jnp.concatenate([sample_vector, context_vector], 0)).astype(jnp.bfloat16)
    modulation = jnp.dot(conditions, modulator, preferred_element_type=jnp.float32)
    hidden = modulated(latents, norm_gain, modulation[0], model_width)
    context_hidden = modulated(context, norm_gain, modulation[1], model_width)

    def project(token_rows, weight):
        return jnp.dot(token_rows, weight, preferred_element_type=jnp.float32).astype(jnp.bfloat16)

    def by_head(values, size):
        return lax.optimization_barrier(values).astype(jnp.float32).reshape(values.shape[0], HEADS, size)
    queries = by_head(project(hidden, query_weight), DK)
    key_rows = by_head(project(hidden, key_weight), DK)
    value_rows = by_head(project(hidden, value_weight), DV)
    context_keys = by_head(project(context_hidden, key_weight), DK)
    context_values = by_head(project(context_hidden, value_weight), DV)
    decays = log_decays(project(hidden, decay_down), decay_up, decay_bias).reshape(2, TOKENS, HEADS, DK) + decay_extra[:, :, :, None]
    context_decays = log_decays(project(context_hidden, decay_down), decay_up, decay_bias).reshape(2, CTX, HEADS, DK)
    zero_state = jnp.zeros((HEADS, DK, DV), jnp.float32)
    start_forward, _ = sweep(context_keys, context_keys, context_values, context_decays[0], zero_state)
    start_backward, _ = sweep(context_keys[::-1], context_keys[::-1], context_values[::-1], context_decays[1][::-1], zero_state)
    _, forward = sweep(queries, key_rows, value_rows, decays[0], CTX_LIFT * start_forward)
    _, backward = sweep(queries[::-1], key_rows[::-1], value_rows[::-1], decays[1][::-1], CTX_LIFT * start_backward)
    mixed = forward + backward[::-1]
    normed = rms_rows(mixed, head_gain).astype(jnp.bfloat16).reshape(TOKENS, HEADS * DV)
    group_width = HEADS * DV // N_TP
    summed = jnp.zeros((TOKENS, model_width), jnp.float32)
    for group_index in range(N_TP):
        lower_edge = group_index * group_width
        partial_value = jnp.dot(normed[:, lower_edge:lower_edge + group_width], out_weight[lower_edge:lower_edge + group_width], preferred_element_type=jnp.float32).astype(jnp.bfloat16)
        summed = summed + lax.optimization_barrier(partial_value).astype(jnp.float32)
    projected = lax.optimization_barrier(summed.astype(jnp.bfloat16)).astype(jnp.float32)
    gate_vector = modulation[0, 2 * model_width:]
    return (latents.astype(jnp.float32) + gate_vector * projected).astype(jnp.bfloat16)
```

```python
import jax
import jax.numpy as jnp
from jax import lax
from jax.experimental import pallas as pl
from jax.experimental.pallas import tpu as pltpu
from jax.sharding import Mesh, PartitionSpec as P

D = 2048
DK = 128
RANK = 32
BLOCK = 64
CTX_LIFT = 4.0
EPS = 1e-06
SHARP = 16.0
SEG = 512
CTX_SEG = 64
ROWS = SEG + CTX_SEG
PAYLOAD = 336
bf16 = jnp.bfloat16
f32 = jnp.float32
VM = pl.BlockSpec(memory_space=pltpu.VMEM)
SM = pl.BlockSpec(memory_space=pltpu.SMEM)


def to_everyone(x, axis):
    size = lax.axis_size(axis)
    return lax.all_to_all(jnp.broadcast_to(x[None], (size, *x.shape)), axis, 0, 0, tiled=True)


def three_parts(x):
    hi = x.astype(bf16)
    rest = x - hi.astype(f32)
    mid = rest.astype(bf16)
    lo = (rest - mid.astype(f32)).astype(bf16)
    return hi, mid, lo


def tri(rows, cols, upper):
    r = lax.broadcasted_iota(jnp.int32, (rows, cols), 0)
    c = lax.broadcasted_iota(jnp.int32, (rows, cols), 1)
    return (c >= r) if upper else (c <= r)


def summed_by(mask, a):
    m = mask.astype(f32).astype(bf16)
    stacked = jnp.concatenate(three_parts(a), axis=0)
    return jnp.dot(jnp.concatenate([m, m, m], axis=1), stacked, preferred_element_type=f32)


def nt(a, b):
    return lax.dot_general(a, b, (((1,), (1,)), ((), ())), preferred_element_type=f32)


def tn(a, b):
    return lax.dot_general(a, b, (((0,), (0,)), ((), ())), preferred_element_type=f32)


def project_kernel(
    place, x_ref, mod_ref, gain_ref, own_ref, other_ref, down_ref, up_ref, bias_ref, extra_ref,
    pay_ref, q_ref, k_ref, v_ref, cum_ref, h_ref, w_ref,
):
    seg, core = place[0], place[1]
    for xi in range(4):
        for z in range(16):
            at = z * 128 + xi * 32
            w_ref[pl.ds(pl.multiple_of(at + core * 16, 16), 16), 0:384] = own_ref[xi, z]
            w_ref[pl.ds(pl.multiple_of(at + 16 - core * 16, 16), 16), 0:384] = other_ref[xi, z]
    w_ref[:, 384:448] = down_ref[...]
    w_ref[:, 448:512] = jnp.zeros((D, 64), bf16)

    def normed_rows(rows, which):
        v = rows.astype(f32)
        r = lax.rsqrt(jnp.mean(v * v, axis=-1, keepdims=True) + EPS)
        scale = gain_ref[...] * (1.0 + mod_ref[which : which + 1, D : 2 * D])
        return (v * r * scale + mod_ref[which : which + 1, 0:D]).astype(bf16)

    def chunk(n, carry):
        y, zb = n // 4, n % 4
        rows = x_ref[y, pl.ds(pl.multiple_of(zb * 32, 32), 32), :]
        h_ref[pl.ds(pl.multiple_of(zb * 128 + y * 32, 32), 32), :] = normed_rows(rows, 0)
        return carry

    lax.fori_loop(0, 16, chunk, 0)
    for y in range(4):
        h_ref[SEG + y * 16 : SEG + y * 16 + 16, :] = normed_rows(x_ref[y, 128:144, :], 1)

    out = jnp.dot(h_ref[...], w_ref[...], preferred_element_type=f32).astype(bf16)
    q_ref[...] = out[:SEG, 0:128]
    k_ref[...] = out[:SEG, 128:256]
    v_ref[...] = out[:SEG, 256:384]
    low = out[:, 384:448]
    raw = jnp.dot(low, up_ref[...], preferred_element_type=f32) + bias_ref[...]
    logs = (jnp.minimum(raw, 0.0) - jnp.log1p(jnp.exp(-jnp.abs(raw)))) * (1.0 / SHARP)
    ef = extra_ref[:, 0:1]
    eb = extra_ref[:, 1:2]
    af = logs[:SEG, 0:128] + ef
    ab = logs[:SEG, 128:256] + eb
    low_mask = tri(BLOCK, BLOCK, False)
    up_mask = tri(BLOCK, BLOCK, True)
    wf, wb = [], []
    for n in range(SEG // BLOCK):
        sl = slice(n * BLOCK, (n + 1) * BLOCK)
        wf.append(summed_by(low_mask, af[sl]))
        wb.append(summed_by(up_mask, ab[sl]))
        cum_ref[0, sl, :] = wf[-1]
        cum_ref[1, sl, :] = wb[-1]
    tot_f = [w[BLOCK - 1 : BLOCK] for w in wf]
    tot_b = [w[0:1] for w in wb]
    dev_f = sum(tot_f)
    dev_b = sum(tot_b)
    kk = out[:SEG, 128:256].astype(f32)
    before = jnp.zeros((1, DK), f32)
    kf = []
    for n in range(SEG // BLOCK):
        kf.append(kk[n * BLOCK : (n + 1) * BLOCK] * jnp.exp(dev_f - before - wf[n]))
        before = before + tot_f[n]
    after = jnp.zeros((1, DK), f32)
    kb = [None] * (SEG // BLOCK)
    for n in reversed(range(SEG // BLOCK)):
        kb[n] = kk[n * BLOCK : (n + 1) * BLOCK] * jnp.exp(dev_b - after - wb[n])
        after = after + tot_b[n]
    both = jnp.concatenate(
        [jnp.concatenate(kf, 0).astype(bf16), jnp.concatenate(kb, 0).astype(bf16)], axis=1
    )
    states = tn(out[:SEG, 256:384], both).astype(bf16)

    def order(i):
        return ((i % 16) // 4) * 16 + (i // 16) * 4 + i % 4

    r = order(lax.broadcasted_iota(jnp.int32, (CTX_SEG, CTX_SEG), 0))
    c = order(lax.broadcasted_iota(jnp.int32, (CTX_SEG, CTX_SEG), 1))
    later = summed_by(c > r, logs[SEG:, 0:128])
    earlier = summed_by(c < r, logs[SEG:, 128:256])
    ctx_f = jnp.sum(logs[SEG:, 0:128], axis=0, keepdims=True)
    ctx_b = jnp.sum(logs[SEG:, 128:256], axis=0, keepdims=True)
    ck = out[SEG:, 128:256].astype(f32)
    ckf = (ck * jnp.exp(later)).astype(bf16)
    ckb = (ck * jnp.exp(earlier)).astype(bf16)
    cv = out[SEG:, 256:384]
    zero = jnp.zeros((7, DK), bf16)
    for peer in range(4):
        ahead = peer > seg
        pay_ref[peer, 0:128, :] = jnp.where(ahead, states[:, 0:128], states[:, 128:256])
        pay_ref[peer, 128:192, :] = ckf
        pay_ref[peer, 192:256, :] = ckb
        pay_ref[peer, 256:320, :] = cv
        dev = jnp.where(ahead, dev_f, dev_b)
        pay_ref[peer, 320:336, :] = jnp.concatenate(
            [*three_parts(dev), *three_parts(ctx_f), *three_parts(ctx_b), zero], axis=0
        )


def local_kernel(q_ref, k_ref, v_ref, cum_ref, o_ref, lift_f_ref, lift_b_ref):
    blocks = SEG // BLOCK
    low_mask = tri(BLOCK, BLOCK, False)
    up_mask = tri(BLOCK, BLOCK, True)
    tot_f = [cum_ref[0, (n + 1) * BLOCK - 1 : (n + 1) * BLOCK, :] for n in range(blocks)]
    tot_b = [cum_ref[1, n * BLOCK : n * BLOCK + 1, :] for n in range(blocks)]
    state = jnp.zeros((DK, DK), f32)
    before = jnp.zeros((1, DK), f32)
    for n in range(blocks):
        sl = slice(n * BLOCK, (n + 1) * BLOCK)
        q = q_ref[sl, :].astype(f32)
        k = k_ref[sl, :].astype(f32)
        v = v_ref[sl, :]
        wf = cum_ref[0, sl, :]
        wb = cum_ref[1, sl, :]
        mf = 0.5 * tot_f[n]
        mb = 0.5 * tot_b[n]
        sf = nt((q * jnp.exp(wf - mf)).astype(bf16), (k * jnp.exp(mf - wf)).astype(bf16))
        sb = nt((q * jnp.exp(wb - mb)).astype(bf16), (k * jnp.exp(mb - wb)).astype(bf16))
        scores = jnp.where(low_mask, sf, 0.0) + jnp.where(up_mask, sb, 0.0)
        out = jnp.dot(scores.astype(bf16), v, preferred_element_type=f32)
        qd = q * jnp.exp(wf)
        lift_f_ref[sl, :] = (qd * jnp.exp(before)).astype(bf16)
        if n > 0:
            out = out + nt(qd.astype(bf16), state.astype(bf16))
        o_ref[sl, :] = out
        if n < blocks - 1:
            state = jnp.exp(tot_f[n]) * state + tn(v, (k * jnp.exp(tot_f[n] - wf)).astype(bf16))
        before = before + tot_f[n]
    state = jnp.zeros((DK, DK), f32)
    after = jnp.zeros((1, DK), f32)
    for n in reversed(range(blocks)):
        sl = slice(n * BLOCK, (n + 1) * BLOCK)
        q = q_ref[sl, :].astype(f32)
        k = k_ref[sl, :].astype(f32)
        v = v_ref[sl, :]
        wb = cum_ref[1, sl, :]
        qd = q * jnp.exp(wb)
        lift_b_ref[sl, :] = (qd * jnp.exp(after)).astype(bf16)
        if n < blocks - 1:
            o_ref[sl, :] = o_ref[sl, :] + nt(qd.astype(bf16), state.astype(bf16))
        if n > 0:
            state = jnp.exp(tot_b[n]) * state + tn(v, (k * jnp.exp(tot_b[n] - wb)).astype(bf16))
        after = after + tot_b[n]


def combine_kernel(place, in_ref, o_ref, lift_f_ref, lift_b_ref, out_ref):
    seg = place[0]

    def vec(peer, at):
        rows = in_ref[peer, 320:336, :].astype(f32)
        return rows[at : at + 1] + rows[at + 1 : at + 2] + rows[at + 2 : at + 3]

    ctx_f = jnp.zeros((DK, DK), f32)
    ctx_b = jnp.zeros((DK, DK), f32)
    for q in range(4):
        ctx_f = jnp.exp(vec(q, 3)) * ctx_f + tn(in_ref[q, 256:320, :], in_ref[q, 128:192, :])
    for q in reversed(range(4)):
        ctx_b = jnp.exp(vec(q, 6)) * ctx_b + tn(in_ref[q, 256:320, :], in_ref[q, 192:256, :])
    fwd = CTX_LIFT * ctx_f
    for a in range(3):
        moved = jnp.exp(vec(a, 0)) * fwd + in_ref[a, 0:128, :].astype(f32)
        fwd = jnp.where(a < seg, moved, fwd)
    bwd = CTX_LIFT * ctx_b
    for a in (3, 2, 1):
        moved = jnp.exp(vec(a, 0)) * bwd + in_ref[a, 0:128, :].astype(f32)
        bwd = jnp.where(a > seg, moved, bwd)
    out = o_ref[...] + nt(lift_f_ref[...], fwd.astype(bf16)) + nt(lift_b_ref[...], bwd.astype(bf16))
    out_ref[...] = out.astype(bf16)


def output_kernel(mix_ref, gain_ref, w_ref, out_ref):
    total = None
    for h in range(2):
        v = jnp.concatenate([mix_ref[2 * h], mix_ref[2 * h + 1]], axis=1).astype(f32)
        r = lax.rsqrt(jnp.mean(v * v, axis=-1, keepdims=True) + EPS)
        n = (v * r * gain_ref[...]).astype(bf16)
        part = jnp.dot(n, w_ref[h * 256 : (h + 1) * 256, :], preferred_element_type=f32)
        total = part if total is None else total + part
    out_ref[...] = total.astype(bf16)


def final_kernel(parts_ref, lat_ref, gate_ref, out_ref):
    total = parts_ref[0].astype(f32)
    for g in range(1, 4):
        total = total + parts_ref[g].astype(f32)
    projected = total.astype(bf16).astype(f32)
    out_ref[...] = (lat_ref[...].astype(f32) + gate_ref[...] * projected).astype(bf16)


def per_device(
    latents,
    sample_vector,
    context,
    context_vector,
    norm_gain,
    modulator,
    query_weight,
    key_weight,
    value_weight,
    decay_down,
    decay_up,
    decay_bias,
    decay_extra,
    head_gain,
    out_weight,
):
    seg = lax.axis_index("A")
    sub = lax.axis_index("B")
    y = lax.axis_index("tp")
    core = lax.axis_index("core")
    dp = lax.axis_index("x") * 2 + core
    head = sub // 2
    place = jnp.stack([seg, core]).astype(jnp.int32)

    wq = lax.dynamic_slice_in_dim(query_weight, dp * 16, 16, 0)
    wk = lax.dynamic_slice_in_dim(key_weight, dp * 16, 16, 0)
    wv = lax.dynamic_slice_in_dim(value_weight, dp * 16, 16, 0)
    cut = jnp.stack(
        [
            jnp.concatenate(
                [
                    wq[:, (b // 2) * 128 : (b // 2 + 1) * 128],
                    wk[:, (b // 2) * 128 : (b // 2 + 1) * 128],
                    wv[:, b * 128 : (b + 1) * 128],
                ],
                axis=1,
            )
            for b in range(4)
        ]
    )
    cut = jnp.broadcast_to(cut[None], (4, 4, 16, 384)).reshape(16, 16, 384)
    with jax.named_scope("weights_z"):
        rows_z = lax.all_to_all(cut, ("A", "B"), 0, 0, tiled=True)

    conditions = jax.nn.silu(jnp.concatenate([sample_vector, context_vector], 0)).astype(bf16)
    local_mods = jnp.dot(conditions, modulator, preferred_element_type=f32)
    with jax.named_scope("modulation"):
        mods = to_everyone(local_mods, ("A", "B", "tp"))
    modulation = jnp.moveaxis(mods, 0, 1).reshape(2, 3 * D)

    ctx_rows = lax.dynamic_slice_in_dim(context, y * 4, 4, 0)
    extra = jnp.moveaxis(decay_extra, 1, 2).reshape(4, 128)
    extra_row = jnp.concatenate([p.reshape(1, 512) for p in three_parts(extra)], axis=1)
    extra_row = jnp.pad(extra_row, ((0, 3), (0, 512)))
    with jax.named_scope("rows_z"):
        near = to_everyone(jnp.concatenate([latents, ctx_rows, extra_row], 0), "B")
    extras = near[:, 36, :1536].astype(f32).reshape(4, 3, 2, 2, 128).sum(1)
    extras = lax.dynamic_index_in_dim(extras, head, 2, keepdims=False)
    extras = jnp.transpose(extras, (0, 2, 1)).reshape(SEG, 2)
    near_rows = jnp.concatenate(
        [near[:, :32].reshape(128, D), near[:, 32:36].reshape(16, D)], axis=0
    )
    with jax.named_scope("rows_y"):
        all_rows = to_everyone(near_rows, "tp")

    with jax.named_scope("weights_x"):
        own = to_everyone(rows_z, "x")
    with jax.named_scope("weights_core"):
        other = lax.ppermute(own, "core", [(0, 1), (1, 0)])

    up = lax.dynamic_slice_in_dim(decay_up, head * 128, 128, 2)
    up_both = jnp.concatenate(
        [jnp.pad(up[0], ((0, 0), (0, 128))), jnp.pad(up[1], ((0, 0), (128, 0)))], axis=0
    )
    bias = lax.dynamic_slice_in_dim(decay_bias, head * 128, 128, 1).reshape(1, 256)

    sds = jax.ShapeDtypeStruct
    payload, q, k, v, cum = pl.pallas_call(
        project_kernel,
        out_shape=(
            sds((4, PAYLOAD, DK), bf16),
            sds((SEG, DK), bf16),
            sds((SEG, DK), bf16),
            sds((SEG, DK), bf16),
            sds((2, SEG, DK), f32),
        ),
        in_specs=[SM] + [VM] * 9,
        out_specs=(VM,) * 5,
        scratch_shapes=[pltpu.VMEM((ROWS, D), bf16), pltpu.VMEM((D, 512), bf16)],
        name="project",
    )(
        place, all_rows, modulation, norm_gain.reshape(1, D), own, other, decay_down,
        up_both, bias, extras,
    )
    with jax.named_scope("states"):
        got = lax.all_to_all(payload, "A", 0, 0, tiled=True)
    local, lift_f, lift_b = pl.pallas_call(
        local_kernel,
        out_shape=(sds((SEG, DK), f32), sds((SEG, DK), bf16), sds((SEG, DK), bf16)),
        in_specs=[VM] * 4,
        out_specs=(VM,) * 3,
        name="local",
    )(q, k, v, cum)
    mixed = pl.pallas_call(
        combine_kernel,
        out_shape=sds((SEG, DK), bf16),
        in_specs=[SM] + [VM] * 4,
        out_specs=VM,
        name="combine",
    )(place, got, local, lift_f, lift_b)
    with jax.named_scope("mixed_z"):
        mine = lax.all_to_all(mixed.reshape(4, 128, DK), "B", 0, 0, tiled=True)
    partial = pl.pallas_call(
        output_kernel,
        out_shape=sds((128, D), bf16),
        in_specs=[VM] * 3,
        out_specs=VM,
        name="output",
    )(mine, head_gain.reshape(1, 256), out_weight)
    with jax.named_scope("summed_y"):
        parts = lax.all_to_all(partial.reshape(4, 32, D), "tp", 0, 0, tiled=True)
    return pl.pallas_call(
        final_kernel,
        out_shape=sds((32, D), bf16),
        in_specs=[VM] * 3,
        out_specs=VM,
        name="final",
    )(parts, latents, modulation[0:1, 2 * D :])


def solution(mesh):
    mesh = Mesh(mesh.devices.reshape(4, 4, 4, 4, 2), ("A", "B", "tp", "x", "core"))
    dp = ("x", "core")
    sp = ("A", "B")
    placed = (
        P((*dp, *sp, "tp"), None),
        P(dp, None),
        P((*dp, *sp), None),
        P(),
        P(),
        P(None, (*sp, "tp")),
        P(sp, "tp"),
        P(sp, "tp"),
        P(sp, "tp"),
        P(),
        P(None, None, "tp"),
        P(None, "tp"),
        P(None, (*dp, *sp), "tp"),
        P(),
        P("tp", None),
    )
    return jax.shard_map(
        per_device,
        mesh=mesh,
        in_specs=placed,
        out_specs=P((*dp, *sp, "tp"), None),
        check_vma=False,
    )
```

```python
import jax
import jax.numpy as jnp
from jax import lax
from jax.experimental import pallas as pl
from jax.experimental.pallas import tpu as pltpu
from jax.sharding import Mesh, PartitionSpec as P

D = 2048
DK = 128
RANK = 32
BLOCK = 64
CTX_LIFT = 4.0
EPS = 1e-06
SHARP = 16.0
SEG = 512
CTX_SEG = 64
ROWS = SEG + CTX_SEG
PAYLOAD = 336
bf16 = jnp.bfloat16
f32 = jnp.float32
VM = pl.BlockSpec(memory_space=pltpu.VMEM)
SM = pl.BlockSpec(memory_space=pltpu.SMEM)


def to_everyone(x, axis):
    size = lax.axis_size(axis)
    return lax.all_to_all(jnp.broadcast_to(x[None], (size, *x.shape)), axis, 0, 0, tiled=True)


def three_parts(x):
    hi = x.astype(bf16)
    rest = x - hi.astype(f32)
    mid = rest.astype(bf16)
    lo = (rest - mid.astype(f32)).astype(bf16)
    return hi, mid, lo


def three_pieces(x):
    hi = lax.reduce_precision(x, 8, 7)
    mid = lax.reduce_precision(x - hi, 8, 7)
    return hi.astype(bf16), mid.astype(bf16), (x - hi - mid).astype(bf16)


def tri(rows, cols, upper):
    r = lax.broadcasted_iota(jnp.int32, (rows, cols), 0)
    c = lax.broadcasted_iota(jnp.int32, (rows, cols), 1)
    return (c >= r) if upper else (c <= r)


def summed_by(mask, a):
    m = mask.astype(f32).astype(bf16)
    stacked = jnp.concatenate(three_parts(a), axis=0)
    return jnp.dot(jnp.concatenate([m, m, m], axis=1), stacked, preferred_element_type=f32)


def nt(a, b):
    return lax.dot_general(a, b, (((1,), (1,)), ((), ())), preferred_element_type=f32)


def tn(a, b):
    return lax.dot_general(a, b, (((0,), (0,)), ((), ())), preferred_element_type=f32)


def project_kernel(
    place, own_ref, minus_ref, plus_ref, low_ref, high_ref, mod_ref, gain_ref, mine_ref, other_ref,
    down_ref, up_ref, bias_ref, extra_ref,
    pay_ref, q_ref, k_ref, v_ref, cum_ref, h_ref, w_ref,
):
    seg, core, sub, y = place[0], place[1], place[2], place[3]
    for xi in range(4):
        for z in range(16):
            at = z * 128 + xi * 32
            here = pl.ds(pl.multiple_of(at + core * 16, 16), 16)
            there = pl.ds(pl.multiple_of(at + 16 - core * 16, 16), 16)
            w_ref[here, 0:384] = mine_ref[xi, z, :, 0:384]
            w_ref[there, 0:384] = other_ref[xi, z, :, 0:384]
    w_ref[:, 384:448] = down_ref[...]
    w_ref[:, 448:512] = jnp.zeros((D, 64), bf16)

    def normed_rows(rows, which):
        v = rows.astype(f32)
        r = lax.rsqrt(jnp.mean(v * v, axis=-1, keepdims=True) + EPS)
        scale = gain_ref[...] * (1.0 + mod_ref[which : which + 1, D : 2 * D])
        return (v * r * scale + mod_ref[which : which + 1, 0:D]).astype(bf16)

    y_of = [y, (y + 3) % 4, (y + 1) % 4, (y + 2) % 4]
    for slot in range(4):
        for j in range(4):
            if slot < 3:
                rows = (own_ref, minus_ref, plus_ref)[slot][j * 32 : j * 32 + 32, :]
            elif j < 2:
                rows = low_ref[j * 32 : j * 32 + 32, :]
            else:
                rows = high_ref[(j - 2) * 32 : (j - 2) * 32 + 32, :]
            at = pl.multiple_of((sub ^ j) * 128 + y_of[slot] * 32, 32)
            h_ref[pl.ds(at, 32), :] = normed_rows(rows, 0)
        rows = (own_ref, minus_ref, plus_ref)[slot][128:144, :] if slot < 3 else high_ref[64:80, :]
        h_ref[SEG + slot * 16 : SEG + slot * 16 + 16, :] = normed_rows(rows, 1)

    out = jnp.dot(h_ref[...], w_ref[...], preferred_element_type=f32).astype(bf16)
    q_ref[...] = out[:SEG, 0:128]
    k_ref[...] = out[:SEG, 128:256]
    v_ref[...] = out[:SEG, 256:384]
    low = out[:, 384:448]
    raw = jnp.dot(low, up_ref[...], preferred_element_type=f32) + bias_ref[...]
    logs = (jnp.minimum(raw, 0.0) - jnp.log1p(jnp.exp(-jnp.abs(raw)))) * (1.0 / SHARP)
    extra = jnp.concatenate([extra_ref[sub ^ zb] for zb in range(4)], axis=0)
    ef = extra[:, 0:1]
    eb = extra[:, 1:2]
    af = logs[:SEG, 0:128] + ef
    ab = logs[:SEG, 128:256] + eb
    low_mask = tri(BLOCK, BLOCK, False)
    up_mask = tri(BLOCK, BLOCK, True)
    wf, wb = [], []
    for n in range(SEG // BLOCK):
        sl = slice(n * BLOCK, (n + 1) * BLOCK)
        wf.append(summed_by(low_mask, af[sl]))
        wb.append(summed_by(up_mask, ab[sl]))
        cum_ref[0, sl, :] = wf[-1]
        cum_ref[1, sl, :] = wb[-1]
    tot_f = [w[BLOCK - 1 : BLOCK] for w in wf]
    tot_b = [w[0:1] for w in wb]
    dev_f = sum(tot_f)
    dev_b = sum(tot_b)
    kk = out[:SEG, 128:256].astype(f32)
    before = jnp.zeros((1, DK), f32)
    kf = []
    for n in range(SEG // BLOCK):
        kf.append(kk[n * BLOCK : (n + 1) * BLOCK] * jnp.exp(dev_f - before - wf[n]))
        before = before + tot_f[n]
    after = jnp.zeros((1, DK), f32)
    kb = [None] * (SEG // BLOCK)
    for n in reversed(range(SEG // BLOCK)):
        kb[n] = kk[n * BLOCK : (n + 1) * BLOCK] * jnp.exp(dev_b - after - wb[n])
        after = after + tot_b[n]
    both = jnp.concatenate(
        [jnp.concatenate(kf, 0).astype(bf16), jnp.concatenate(kb, 0).astype(bf16)], axis=1
    )
    states = tn(out[:SEG, 256:384], both).astype(bf16)

    def order(i):
        slot = i // 16
        step = jnp.where(slot == 0, 0, jnp.where(slot == 1, 3, slot - 1))
        return (((i % 16) // 4) ^ sub) * 16 + ((step + y) % 4) * 4 + i % 4

    r = order(lax.broadcasted_iota(jnp.int32, (CTX_SEG, CTX_SEG), 0))
    c = order(lax.broadcasted_iota(jnp.int32, (CTX_SEG, CTX_SEG), 1))
    later = summed_by(c > r, logs[SEG:, 0:128])
    earlier = summed_by(c < r, logs[SEG:, 128:256])
    ctx_f = jnp.sum(logs[SEG:, 0:128], axis=0, keepdims=True)
    ctx_b = jnp.sum(logs[SEG:, 128:256], axis=0, keepdims=True)
    ck = out[SEG:, 128:256].astype(f32)
    ckf = (ck * jnp.exp(later)).astype(bf16)
    ckb = (ck * jnp.exp(earlier)).astype(bf16)
    cv = out[SEG:, 256:384]
    zero = jnp.zeros((7, DK), bf16)
    for peer in range(4):
        ahead = peer > seg
        pay_ref[peer, 0:128, :] = jnp.where(ahead, states[:, 0:128], states[:, 128:256])
        pay_ref[peer, 128:192, :] = ckf
        pay_ref[peer, 192:256, :] = ckb
        pay_ref[peer, 256:320, :] = cv
        dev = jnp.where(ahead, dev_f, dev_b)
        pay_ref[peer, 320:336, :] = jnp.concatenate(
            [*three_parts(dev), *three_parts(ctx_f), *three_parts(ctx_b), zero], axis=0
        )


def local_kernel(q_ref, k_ref, v_ref, cum_ref, o_ref, lift_f_ref, lift_b_ref):
    blocks = SEG // BLOCK
    low_mask = tri(BLOCK, BLOCK, False)
    up_mask = tri(BLOCK, BLOCK, True)
    tot_f = [cum_ref[0, (n + 1) * BLOCK - 1 : (n + 1) * BLOCK, :] for n in range(blocks)]
    tot_b = [cum_ref[1, n * BLOCK : n * BLOCK + 1, :] for n in range(blocks)]
    state = jnp.zeros((DK, DK), f32)
    before = jnp.zeros((1, DK), f32)
    for n in range(blocks):
        sl = slice(n * BLOCK, (n + 1) * BLOCK)
        q = q_ref[sl, :].astype(f32)
        k = k_ref[sl, :].astype(f32)
        v = v_ref[sl, :]
        wf = cum_ref[0, sl, :]
        wb = cum_ref[1, sl, :]
        mf = 0.5 * tot_f[n]
        mb = 0.5 * tot_b[n]
        sf = nt((q * jnp.exp(wf - mf)).astype(bf16), (k * jnp.exp(mf - wf)).astype(bf16))
        sb = nt((q * jnp.exp(wb - mb)).astype(bf16), (k * jnp.exp(mb - wb)).astype(bf16))
        scores = jnp.where(low_mask, sf, 0.0) + jnp.where(up_mask, sb, 0.0)
        out = jnp.dot(scores.astype(bf16), v, preferred_element_type=f32)
        qd = q * jnp.exp(wf)
        lift_f_ref[sl, :] = (qd * jnp.exp(before)).astype(bf16)
        if n > 0:
            out = out + nt(qd.astype(bf16), state.astype(bf16))
        o_ref[sl, :] = out
        if n < blocks - 1:
            state = jnp.exp(tot_f[n]) * state + tn(v, (k * jnp.exp(tot_f[n] - wf)).astype(bf16))
        before = before + tot_f[n]
    state = jnp.zeros((DK, DK), f32)
    after = jnp.zeros((1, DK), f32)
    for n in reversed(range(blocks)):
        sl = slice(n * BLOCK, (n + 1) * BLOCK)
        q = q_ref[sl, :].astype(f32)
        k = k_ref[sl, :].astype(f32)
        v = v_ref[sl, :]
        wb = cum_ref[1, sl, :]
        qd = q * jnp.exp(wb)
        lift_b_ref[sl, :] = (qd * jnp.exp(after)).astype(bf16)
        if n < blocks - 1:
            o_ref[sl, :] = o_ref[sl, :] + nt(qd.astype(bf16), state.astype(bf16))
        if n > 0:
            state = jnp.exp(tot_b[n]) * state + tn(v, (k * jnp.exp(tot_b[n] - wb)).astype(bf16))
        after = after + tot_b[n]


def combine_kernel(place, in_ref, o_ref, lift_f_ref, lift_b_ref, out_ref):
    seg = place[0]

    def vec(peer, at):
        rows = in_ref[peer, 320:336, :].astype(f32)
        return rows[at : at + 1] + rows[at + 1 : at + 2] + rows[at + 2 : at + 3]

    ctx_f = jnp.zeros((DK, DK), f32)
    ctx_b = jnp.zeros((DK, DK), f32)
    for q in range(4):
        ctx_f = jnp.exp(vec(q, 3)) * ctx_f + tn(in_ref[q, 256:320, :], in_ref[q, 128:192, :])
    for q in reversed(range(4)):
        ctx_b = jnp.exp(vec(q, 6)) * ctx_b + tn(in_ref[q, 256:320, :], in_ref[q, 192:256, :])
    fwd = CTX_LIFT * ctx_f
    for a in range(3):
        moved = jnp.exp(vec(a, 0)) * fwd + in_ref[a, 0:128, :].astype(f32)
        fwd = jnp.where(a < seg, moved, fwd)
    bwd = CTX_LIFT * ctx_b
    for a in (3, 2, 1):
        moved = jnp.exp(vec(a, 0)) * bwd + in_ref[a, 0:128, :].astype(f32)
        bwd = jnp.where(a > seg, moved, bwd)
    out = o_ref[...] + nt(lift_f_ref[...], fwd.astype(bf16)) + nt(lift_b_ref[...], bwd.astype(bf16))
    out_ref[...] = out.astype(bf16)


def output_kernel(mix_ref, gain_ref, w_ref, out_ref):
    total = None
    for h in range(2):
        v = jnp.concatenate([mix_ref[2 * h], mix_ref[2 * h + 1]], axis=1).astype(f32)
        r = lax.rsqrt(jnp.mean(v * v, axis=-1, keepdims=True) + EPS)
        n = (v * r * gain_ref[...]).astype(bf16)
        part = jnp.dot(n, w_ref[h * 256 : (h + 1) * 256, :], preferred_element_type=f32)
        total = part if total is None else total + part
    out_ref[...] = total.astype(bf16)


def final_kernel(parts_ref, lat_ref, gate_ref, out_ref):
    total = parts_ref[0].astype(f32)
    for g in range(1, 4):
        total = total + parts_ref[g].astype(f32)
    projected = total.astype(bf16).astype(f32)
    out_ref[...] = (lat_ref[...].astype(f32) + gate_ref[...] * projected).astype(bf16)


def per_device(
    latents,
    sample_vector,
    context,
    context_vector,
    norm_gain,
    modulator,
    query_weight,
    key_weight,
    value_weight,
    decay_down,
    decay_up,
    decay_bias,
    decay_extra,
    head_gain,
    out_weight,
):
    seg = lax.axis_index("A")
    sub = lax.axis_index("B")
    y = lax.axis_index("tp")
    core = lax.axis_index("core")
    dp = lax.axis_index("x") * 2 + core
    head = sub // 2
    place = jnp.stack([seg, core, sub, y]).astype(jnp.int32)

    ctx_rows = lax.dynamic_slice_in_dim(context, y * 4, 4, 0)
    extra = jnp.moveaxis(decay_extra, 1, 2).reshape(4, 128)
    extra_row = jnp.concatenate([p.reshape(1, 512) for p in three_pieces(extra)], axis=1)
    extra_row = jnp.pad(extra_row, ((0, 3), (0, 512)))
    rows = jnp.concatenate([latents, ctx_rows, extra_row], 0)
    near = [rows]
    for j in range(1, 4):
        with jax.named_scope(f"rows_z{j}"):
            near.append(lax.ppermute(rows, "B", [(b, b ^ j) for b in range(4)]))
    extras = jnp.stack([n[36, :1536] for n in near]).astype(f32).reshape(4, 3, 2, 2, 128).sum(1)
    extras = lax.dynamic_index_in_dim(extras, head, 2, keepdims=False)
    extras = jnp.transpose(extras, (0, 2, 1))

    wq = lax.dynamic_slice_in_dim(query_weight, dp * 16, 16, 0)
    wk = lax.dynamic_slice_in_dim(key_weight, dp * 16, 16, 0)
    wv = lax.dynamic_slice_in_dim(value_weight, dp * 16, 16, 0)
    conditions = jax.nn.silu(jnp.concatenate([sample_vector, context_vector], 0)).astype(bf16)
    local_mods = jnp.dot(conditions, modulator, preferred_element_type=f32)
    riding = jnp.pad(jnp.concatenate(three_pieces(local_mods), axis=0), ((0, 10), (0, 32)))
    cut = jnp.stack(
        [
            jnp.concatenate(
                [
                    wq[:, (b // 2) * 128 : (b // 2 + 1) * 128],
                    wk[:, (b // 2) * 128 : (b // 2 + 1) * 128],
                    wv[:, b * 128 : (b + 1) * 128],
                    riding,
                ],
                axis=1,
            )
            for b in range(4)
        ]
    )
    cut = jnp.broadcast_to(cut[None], (4, 4, 16, 512)).reshape(16, 16, 512)
    with jax.named_scope("weights_z"):
        rows_z = lax.all_to_all(cut, ("A", "B"), 0, 0, tiled=True)
    mods = rows_z[:, 0:8, 384:512]
    around = [mods]
    for j in range(1, 4):
        with jax.named_scope(f"mods_y{j}"):
            around.append(lax.ppermute(mods, "tp", [(i, i ^ j) for i in range(4)]))
    with jax.named_scope("weights_x"):
        mine = to_everyone(rows_z, "x")
    with jax.named_scope("weights_core"):
        other = lax.ppermute(mine, "core", [(0, 1), (1, 0)])
    around = jnp.stack(around)
    around = jnp.stack([lax.dynamic_index_in_dim(around, y ^ t, 0, keepdims=False) for t in range(4)])
    parts = around[:, :, 0:6, 0:96].astype(f32)
    parts = parts[:, :, 0:2] + parts[:, :, 2:4] + parts[:, :, 4:6]
    modulation = jnp.transpose(parts, (2, 1, 0, 3)).reshape(2, 3 * D)

    own = jnp.concatenate([n[:32] for n in near] + [n[32:36] for n in near], axis=0)
    up_shift = [(i, (i + 1) % 4) for i in range(4)]
    down_shift = [(i, (i + 3) % 4) for i in range(4)]
    with jax.named_scope("rows_up"):
        minus = lax.ppermute(own, "tp", up_shift)
    with jax.named_scope("rows_down"):
        plus = lax.ppermute(own, "tp", down_shift)
    with jax.named_scope("rows_up2"):
        low = lax.ppermute(minus[:64], "tp", up_shift)
    with jax.named_scope("rows_down2"):
        high = lax.ppermute(plus[64:], "tp", down_shift)

    up = lax.dynamic_slice_in_dim(decay_up, head * 128, 128, 2)
    up_both = jnp.concatenate(
        [jnp.pad(up[0], ((0, 0), (0, 128))), jnp.pad(up[1], ((0, 0), (128, 0)))], axis=0
    )
    bias = lax.dynamic_slice_in_dim(decay_bias, head * 128, 128, 1).reshape(1, 256)

    sds = jax.ShapeDtypeStruct
    payload, q, k, v, cum = pl.pallas_call(
        project_kernel,
        out_shape=(
            sds((4, PAYLOAD, DK), bf16),
            sds((SEG, DK), bf16),
            sds((SEG, DK), bf16),
            sds((SEG, DK), bf16),
            sds((2, SEG, DK), f32),
        ),
        in_specs=[SM] + [VM] * 13,
        out_specs=(VM,) * 5,
        scratch_shapes=[pltpu.VMEM((ROWS, D), bf16), pltpu.VMEM((D, 512), bf16)],
        name="project",
    )(
        place, own, minus, plus, low, high, modulation, norm_gain.reshape(1, D), mine, other,
        decay_down, up_both, bias, extras,
    )
    with jax.named_scope("states"):
        got = lax.all_to_all(payload, "A", 0, 0, tiled=True)
    local, lift_f, lift_b = pl.pallas_call(
        local_kernel,
        out_shape=(sds((SEG, DK), f32), sds((SEG, DK), bf16), sds((SEG, DK), bf16)),
        in_specs=[VM] * 4,
        out_specs=(VM,) * 3,
        name="local",
    )(q, k, v, cum)
    mixed = pl.pallas_call(
        combine_kernel,
        out_shape=sds((SEG, DK), bf16),
        in_specs=[SM] + [VM] * 4,
        out_specs=VM,
        name="combine",
    )(place, got, local, lift_f, lift_b)
    with jax.named_scope("mixed_z"):
        heads = lax.all_to_all(mixed.reshape(4, 128, DK), "B", 0, 0, tiled=True)
    partial = pl.pallas_call(
        output_kernel,
        out_shape=sds((128, D), bf16),
        in_specs=[VM] * 3,
        out_specs=VM,
        name="output",
    )(heads, head_gain.reshape(1, 256), out_weight)
    with jax.named_scope("summed_y"):
        shares = lax.all_to_all(partial.reshape(4, 32, D), "tp", 0, 0, tiled=True)
    return pl.pallas_call(
        final_kernel,
        out_shape=sds((32, D), bf16),
        in_specs=[VM] * 3,
        out_specs=VM,
        name="final",
    )(shares, latents, modulation[0:1, 2 * D :])


def solution(mesh):
    mesh = Mesh(mesh.devices.reshape(4, 4, 4, 4, 2), ("A", "B", "tp", "x", "core"))
    dp = ("x", "core")
    sp = ("A", "B")
    placed = (
        P((*dp, *sp, "tp"), None),
        P(dp, None),
        P((*dp, *sp), None),
        P(),
        P(),
        P(None, (*sp, "tp")),
        P(sp, "tp"),
        P(sp, "tp"),
        P(sp, "tp"),
        P(),
        P(None, None, "tp"),
        P(None, "tp"),
        P(None, (*dp, *sp), "tp"),
        P(),
        P("tp", None),
    )
    return jax.shard_map(
        per_device,
        mesh=mesh,
        in_specs=placed,
        out_specs=P((*dp, *sp, "tp"), None),
        check_vma=False,
    )
```

```python
import jax
import jax.numpy as jnp
from jax import lax
from jax.experimental import pallas as pl
from jax.experimental.pallas import tpu as pltpu
from jax.sharding import Mesh, PartitionSpec as P


D = 2048
DK = 128
BLOCK = 64
CTX_LIFT = 4.0
EPS = 1e-06
SHARP = 16.0
SEG = 512
CTX_SEG = 64
ROWS = SEG + CTX_SEG
PAYLOAD = 336
bf16 = jnp.bfloat16
f32 = jnp.float32
VM = pl.BlockSpec(memory_space=pltpu.VMEM)
SM = pl.BlockSpec(memory_space=pltpu.SMEM)


def to_everyone(x, axis):
    size = lax.axis_size(axis)
    return lax.all_to_all(jnp.broadcast_to(x[None], (size, *x.shape)), axis, 0, 0, tiled=True)


def three_parts(x):
    hi = x.astype(bf16)
    rest = x - hi.astype(f32)
    mid = rest.astype(bf16)
    lo = (rest - mid.astype(f32)).astype(bf16)
    return hi, mid, lo


def three_pieces(x):
    hi = lax.reduce_precision(x, 8, 7)
    mid = lax.reduce_precision(x - hi, 8, 7)
    return hi.astype(bf16), mid.astype(bf16), (x - hi - mid).astype(bf16)


def tri(rows, cols, upper):
    r = lax.broadcasted_iota(jnp.int32, (rows, cols), 0)
    c = lax.broadcasted_iota(jnp.int32, (rows, cols), 1)
    return (c >= r) if upper else (c <= r)


def summed_by(mask, a):
    m = mask.astype(f32).astype(bf16)
    stacked = jnp.concatenate(three_parts(a), axis=0)
    return jnp.dot(jnp.concatenate([m, m, m], axis=1), stacked, preferred_element_type=f32)


def nt(a, b):
    return lax.dot_general(a, b, (((1,), (1,)), ((), ())), preferred_element_type=f32)


def tn(a, b):
    return lax.dot_general(a, b, (((0,), (0,)), ((), ())), preferred_element_type=f32)


def project_kernel(
    place, own_ref, minus_ref, plus_ref, low_ref, high_ref, mod_ref, gain_ref, mine_ref, other_ref,
    down_ref, up_ref, bias_ref, extra_ref,
    pay_ref, q_ref, k_ref, v_ref, cum_ref, h_ref, w_ref,
):
    seg, core, sub, y = place[0], place[1], place[2], place[3]
    for xi in range(4):
        for z in range(16):
            at = z * 128 + xi * 32
            here = pl.ds(pl.multiple_of(at + core * 16, 16), 16)
            there = pl.ds(pl.multiple_of(at + 16 - core * 16, 16), 16)
            w_ref[here, 0:384] = mine_ref[xi, z, :, 0:384]
            w_ref[there, 0:384] = other_ref[xi, z, :, 0:384]
    w_ref[:, 384:448] = down_ref[...]
    w_ref[:, 448:512] = jnp.zeros((D, 64), bf16)

    def normed_rows(rows, which):
        v = rows.astype(f32)
        r = lax.rsqrt(jnp.mean(v * v, axis=-1, keepdims=True) + EPS)
        scale = gain_ref[...] * (1.0 + mod_ref[which : which + 1, D : 2 * D])
        return (v * r * scale + mod_ref[which : which + 1, 0:D]).astype(bf16)

    y_of = [y, (y + 3) % 4, (y + 1) % 4, (y + 2) % 4]
    for slot in range(4):
        for j in range(4):
            if slot < 3:
                rows = (own_ref, minus_ref, plus_ref)[slot][j * 32 : j * 32 + 32, :]
            elif j < 2:
                rows = low_ref[j * 32 : j * 32 + 32, :]
            else:
                rows = high_ref[(j - 2) * 32 : (j - 2) * 32 + 32, :]
            at = pl.multiple_of((sub ^ j) * 128 + y_of[slot] * 32, 32)
            h_ref[pl.ds(at, 32), :] = normed_rows(rows, 0)
        rows = (own_ref, minus_ref, plus_ref)[slot][128:144, :] if slot < 3 else high_ref[64:80, :]
        h_ref[SEG + slot * 16 : SEG + slot * 16 + 16, :] = normed_rows(rows, 1)

    out = jnp.dot(h_ref[...], w_ref[...], preferred_element_type=f32).astype(bf16)
    q_ref[...] = out[:SEG, 0:128]
    k_ref[...] = out[:SEG, 128:256]
    v_ref[...] = out[:SEG, 256:384]
    low = out[:, 384:448]
    raw = jnp.dot(low, up_ref[...], preferred_element_type=f32) + bias_ref[...]
    logs = (jnp.minimum(raw, 0.0) - jnp.log1p(jnp.exp(-jnp.abs(raw)))) * (1.0 / SHARP)
    extra = jnp.concatenate([extra_ref[zb] for zb in range(4)], axis=0)
    ef = extra[:, 0:1]
    eb = extra[:, 1:2]
    af = logs[:SEG, 0:128] + ef
    ab = logs[:SEG, 128:256] + eb
    low_mask = tri(BLOCK, BLOCK, False)
    up_mask = tri(BLOCK, BLOCK, True)
    wf, wb = [], []
    for n in range(SEG // BLOCK):
        sl = slice(n * BLOCK, (n + 1) * BLOCK)
        wf.append(summed_by(low_mask, af[sl]))
        wb.append(summed_by(up_mask, ab[sl]))
        cum_ref[0, sl, :] = wf[-1]
        cum_ref[1, sl, :] = wb[-1]
    tot_f = [w[BLOCK - 1 : BLOCK] for w in wf]
    tot_b = [w[0:1] for w in wb]
    dev_f = sum(tot_f)
    dev_b = sum(tot_b)
    kk = out[:SEG, 128:256].astype(f32)
    before = jnp.zeros((1, DK), f32)
    kf = []
    for n in range(SEG // BLOCK):
        kf.append(kk[n * BLOCK : (n + 1) * BLOCK] * jnp.exp(dev_f - before - wf[n]))
        before = before + tot_f[n]
    after = jnp.zeros((1, DK), f32)
    kb = [None] * (SEG // BLOCK)
    for n in reversed(range(SEG // BLOCK)):
        kb[n] = kk[n * BLOCK : (n + 1) * BLOCK] * jnp.exp(dev_b - after - wb[n])
        after = after + tot_b[n]
    both = jnp.concatenate(
        [jnp.concatenate(kf, 0).astype(bf16), jnp.concatenate(kb, 0).astype(bf16)], axis=1
    )
    states = tn(out[:SEG, 256:384], both).astype(bf16)

    def order(i):
        slot = i // 16
        step = jnp.where(slot == 0, 0, jnp.where(slot == 1, 3, slot - 1))
        return (((i % 16) // 4) ^ sub) * 16 + ((step + y) % 4) * 4 + i % 4

    r = order(lax.broadcasted_iota(jnp.int32, (CTX_SEG, CTX_SEG), 0))
    c = order(lax.broadcasted_iota(jnp.int32, (CTX_SEG, CTX_SEG), 1))
    later = summed_by(c > r, logs[SEG:, 0:128])
    earlier = summed_by(c < r, logs[SEG:, 128:256])
    ctx_f = jnp.sum(logs[SEG:, 0:128], axis=0, keepdims=True)
    ctx_b = jnp.sum(logs[SEG:, 128:256], axis=0, keepdims=True)
    ck = out[SEG:, 128:256].astype(f32)
    ckf = (ck * jnp.exp(later)).astype(bf16)
    ckb = (ck * jnp.exp(earlier)).astype(bf16)
    cv = out[SEG:, 256:384]
    zero = jnp.zeros((7, DK), bf16)
    for peer in range(4):
        ahead = peer > seg
        pay_ref[peer, 0:128, :] = jnp.where(ahead, states[:, 0:128], states[:, 128:256])
        pay_ref[peer, 128:192, :] = ckf
        pay_ref[peer, 192:256, :] = ckb
        pay_ref[peer, 256:320, :] = cv
        dev = jnp.where(ahead, dev_f, dev_b)
        pay_ref[peer, 320:336, :] = jnp.concatenate(
            [*three_parts(dev), *three_parts(ctx_f), *three_parts(ctx_b), zero], axis=0
        )


def local_kernel(q_ref, k_ref, v_ref, cum_ref, o_ref, lift_f_ref, lift_b_ref):
    blocks = SEG // BLOCK
    low_mask = tri(BLOCK, BLOCK, False)
    up_mask = tri(BLOCK, BLOCK, True)
    tot_f = [cum_ref[0, (n + 1) * BLOCK - 1 : (n + 1) * BLOCK, :] for n in range(blocks)]
    tot_b = [cum_ref[1, n * BLOCK : n * BLOCK + 1, :] for n in range(blocks)]
    state = jnp.zeros((DK, DK), f32)
    before = jnp.zeros((1, DK), f32)
    for n in range(blocks):
        sl = slice(n * BLOCK, (n + 1) * BLOCK)
        q = q_ref[sl, :].astype(f32)
        k = k_ref[sl, :].astype(f32)
        v = v_ref[sl, :]
        wf = cum_ref[0, sl, :]
        wb = cum_ref[1, sl, :]
        mf = 0.5 * tot_f[n]
        mb = 0.5 * tot_b[n]
        sf = nt((q * jnp.exp(wf - mf)).astype(bf16), (k * jnp.exp(mf - wf)).astype(bf16))
        sb = nt((q * jnp.exp(wb - mb)).astype(bf16), (k * jnp.exp(mb - wb)).astype(bf16))
        scores = jnp.where(low_mask, sf, 0.0) + jnp.where(up_mask, sb, 0.0)
        out = jnp.dot(scores.astype(bf16), v, preferred_element_type=f32)
        qd = q * jnp.exp(wf)
        lift_f_ref[sl, :] = (qd * jnp.exp(before)).astype(bf16)
        if n > 0:
            out = out + nt(qd.astype(bf16), state.astype(bf16))
        o_ref[sl, :] = out
        if n < blocks - 1:
            state = jnp.exp(tot_f[n]) * state + tn(v, (k * jnp.exp(tot_f[n] - wf)).astype(bf16))
        before = before + tot_f[n]
    state = jnp.zeros((DK, DK), f32)
    after = jnp.zeros((1, DK), f32)
    for n in reversed(range(blocks)):
        sl = slice(n * BLOCK, (n + 1) * BLOCK)
        q = q_ref[sl, :].astype(f32)
        k = k_ref[sl, :].astype(f32)
        v = v_ref[sl, :]
        wb = cum_ref[1, sl, :]
        qd = q * jnp.exp(wb)
        lift_b_ref[sl, :] = (qd * jnp.exp(after)).astype(bf16)
        if n < blocks - 1:
            o_ref[sl, :] = o_ref[sl, :] + nt(qd.astype(bf16), state.astype(bf16))
        if n > 0:
            state = jnp.exp(tot_b[n]) * state + tn(v, (k * jnp.exp(tot_b[n] - wb)).astype(bf16))
        after = after + tot_b[n]


def combine_kernel(place, in_ref, o_ref, lift_f_ref, lift_b_ref, out_ref):
    seg = place[0]

    def vec(peer, at):
        rows = in_ref[peer, 320:336, :].astype(f32)
        return rows[at : at + 1] + rows[at + 1 : at + 2] + rows[at + 2 : at + 3]

    ctx_f = jnp.zeros((DK, DK), f32)
    ctx_b = jnp.zeros((DK, DK), f32)
    for q in range(4):
        ctx_f = jnp.exp(vec(q, 3)) * ctx_f + tn(in_ref[q, 256:320, :], in_ref[q, 128:192, :])
    for q in reversed(range(4)):
        ctx_b = jnp.exp(vec(q, 6)) * ctx_b + tn(in_ref[q, 256:320, :], in_ref[q, 192:256, :])
    fwd = CTX_LIFT * ctx_f
    for a in range(3):
        moved = jnp.exp(vec(a, 0)) * fwd + in_ref[a, 0:128, :].astype(f32)
        fwd = jnp.where(a < seg, moved, fwd)
    bwd = CTX_LIFT * ctx_b
    for a in (3, 2, 1):
        moved = jnp.exp(vec(a, 0)) * bwd + in_ref[a, 0:128, :].astype(f32)
        bwd = jnp.where(a > seg, moved, bwd)
    out = o_ref[...] + nt(lift_f_ref[...], fwd.astype(bf16)) + nt(lift_b_ref[...], bwd.astype(bf16))
    out_ref[...] = out.astype(bf16)


def output_kernel(mix_ref, gain_ref, w_ref, out_ref):
    total = None
    for h in range(2):
        v = jnp.concatenate([mix_ref[2 * h], mix_ref[2 * h + 1]], axis=1).astype(f32)
        r = lax.rsqrt(jnp.mean(v * v, axis=-1, keepdims=True) + EPS)
        n = (v * r * gain_ref[...]).astype(bf16)
        part = jnp.dot(n, w_ref[h * 256 : (h + 1) * 256, :], preferred_element_type=f32)
        total = part if total is None else total + part
    out_ref[...] = total.astype(bf16)


def final_kernel(parts_ref, lat_ref, gate_ref, out_ref):
    total = parts_ref[0].astype(f32)
    for g in range(1, 4):
        total = total + parts_ref[g].astype(f32)
    projected = total.astype(bf16).astype(f32)
    out_ref[...] = (lat_ref[...].astype(f32) + gate_ref[...] * projected).astype(bf16)


def device_body(
    latents,
    sample_vector,
    context,
    context_vector,
    norm_gain,
    modulator,
    query_weight,
    key_weight,
    value_weight,
    decay_down,
    decay_up,
    decay_bias,
    decay_extra,
    head_gain,
    out_weight,
):
    seg = lax.axis_index("A")
    sub = lax.axis_index("B")
    y = lax.axis_index("tp")
    core = lax.axis_index("core")
    dp = lax.axis_index("x") * 2 + core
    head = sub // 2
    place = jnp.stack([seg, core, sub, y]).astype(jnp.int32)

    ctx_rows = lax.dynamic_slice_in_dim(context, y * 4, 4, 0)
    rows = jnp.concatenate([latents, ctx_rows], 0)
    near = [rows]
    for j in range(1, 4):
        near.append(lax.ppermute(rows, "B", [(b, b ^ j) for b in range(4)]))

    wq = lax.dynamic_slice_in_dim(query_weight, dp * 16, 16, 0)
    wk = lax.dynamic_slice_in_dim(key_weight, dp * 16, 16, 0)
    wv = lax.dynamic_slice_in_dim(value_weight, dp * 16, 16, 0)
    conditions = jax.nn.silu(jnp.concatenate([sample_vector, context_vector], 0)).astype(bf16)
    local_mods = jnp.dot(conditions, modulator, preferred_element_type=f32)
    extra = jnp.moveaxis(decay_extra, 1, 2).reshape(4, 128)
    riding = jnp.pad(jnp.concatenate(three_pieces(local_mods), axis=0), ((0, 0), (0, 32)))
    riding = jnp.concatenate([riding, *three_pieces(extra)[:2], jnp.zeros((2, 128), bf16)], axis=0)
    cut = jnp.stack(
        [
            jnp.concatenate(
                [
                    wq[:, (b // 2) * 128 : (b // 2 + 1) * 128],
                    wk[:, (b // 2) * 128 : (b // 2 + 1) * 128],
                    wv[:, b * 128 : (b + 1) * 128],
                    riding,
                ],
                axis=1,
            )
            for b in range(4)
        ]
    )
    cut = jnp.broadcast_to(cut[None], (4, 4, 16, 512)).reshape(16, 16, 512)
    rows_z = lax.all_to_all(cut, ("A", "B"), 0, 0, tiled=True)
    mods = rows_z[:, 0:8, 384:512]
    extras = lax.dynamic_slice_in_dim(rows_z, seg * 4, 4, 0)[:, 6:14, 384:512].astype(f32)
    extras = (extras[:, 0:4] + extras[:, 4:8]).reshape(4, 2, 2, 128)
    extras = lax.dynamic_index_in_dim(extras, head, 2, keepdims=False)
    extras = jnp.transpose(extras, (0, 2, 1))
    around = [mods]
    for j in range(1, 4):
        around.append(lax.ppermute(mods, "tp", [(i, i ^ j) for i in range(4)]))
    mine = to_everyone(rows_z, "x")
    other = lax.ppermute(mine, "core", [(0, 1), (1, 0)])
    around = jnp.stack(around)
    around = jnp.stack([lax.dynamic_index_in_dim(around, y ^ t, 0, keepdims=False) for t in range(4)])
    parts = around[:, :, 0:6, 0:96].astype(f32)
    parts = parts[:, :, 0:2] + parts[:, :, 2:4] + parts[:, :, 4:6]
    modulation = jnp.transpose(parts, (2, 1, 0, 3)).reshape(2, 3 * D)

    own = jnp.concatenate([n[:32] for n in near] + [n[32:36] for n in near], axis=0)
    up_shift = [(i, (i + 1) % 4) for i in range(4)]
    down_shift = [(i, (i + 3) % 4) for i in range(4)]
    minus = lax.ppermute(own, "tp", up_shift)
    plus = lax.ppermute(own, "tp", down_shift)
    low = lax.ppermute(minus[:64], "tp", up_shift)
    high = lax.ppermute(plus[64:], "tp", down_shift)

    up = lax.dynamic_slice_in_dim(decay_up, head * 128, 128, 2)
    up_both = jnp.concatenate(
        [jnp.pad(up[0], ((0, 0), (0, 128))), jnp.pad(up[1], ((0, 0), (128, 0)))], axis=0
    )
    bias = lax.dynamic_slice_in_dim(decay_bias, head * 128, 128, 1).reshape(1, 256)

    sds = jax.ShapeDtypeStruct
    payload, q, k, v, cum = pl.pallas_call(
        project_kernel,
        out_shape=(
            sds((4, PAYLOAD, DK), bf16),
            sds((SEG, DK), bf16),
            sds((SEG, DK), bf16),
            sds((SEG, DK), bf16),
            sds((2, SEG, DK), f32),
        ),
        in_specs=[SM] + [VM] * 13,
        out_specs=(VM,) * 5,
        scratch_shapes=[pltpu.VMEM((ROWS, D), bf16), pltpu.VMEM((D, 512), bf16)],
        name="project",
    )(
        place, own, minus, plus, low, high, modulation, norm_gain.reshape(1, D), mine, other,
        decay_down, up_both, bias, extras,
    )
    got = lax.all_to_all(payload, "A", 0, 0, tiled=True)
    local, lift_f, lift_b = pl.pallas_call(
        local_kernel,
        out_shape=(sds((SEG, DK), f32), sds((SEG, DK), bf16), sds((SEG, DK), bf16)),
        in_specs=[VM] * 4,
        out_specs=(VM,) * 3,
        name="local",
    )(q, k, v, cum)
    mixed = pl.pallas_call(
        combine_kernel,
        out_shape=sds((SEG, DK), bf16),
        in_specs=[SM] + [VM] * 4,
        out_specs=VM,
        name="combine",
    )(place, got, local, lift_f, lift_b)
    heads = lax.all_to_all(mixed.reshape(4, 128, DK), "B", 0, 0, tiled=True)
    partial = pl.pallas_call(
        output_kernel,
        out_shape=sds((128, D), bf16),
        in_specs=[VM] * 3,
        out_specs=VM,
        name="output",
    )(heads, head_gain.reshape(1, 256), out_weight)
    shares = lax.all_to_all(partial.reshape(4, 32, D), "tp", 0, 0, tiled=True)
    return pl.pallas_call(
        final_kernel,
        out_shape=sds((32, D), bf16),
        in_specs=[VM] * 3,
        out_specs=VM,
        name="final",
    )(shares, latents, modulation[0:1, 2 * D :])


def solution(mesh):
    mesh = Mesh(mesh.devices.reshape(4, 4, 4, 4, 2), ("A", "B", "tp", "x", "core"))
    dp = ("x", "core")
    sp = ("A", "B")
    placed = (
        P((*dp, *sp, "tp"), None),
        P(dp, None),
        P((*dp, *sp), None),
        P(),
        P(),
        P(None, (*sp, "tp")),
        P(sp, "tp"),
        P(sp, "tp"),
        P(sp, "tp"),
        P(),
        P(None, None, "tp"),
        P(None, "tp"),
        P(None, (*dp, *sp), "tp"),
        P(),
        P("tp", None),
    )
    return jax.shard_map(
        device_body,
        mesh=mesh,
        in_specs=placed,
        out_specs=P((*dp, *sp, "tp"), None),
        check_vma=False,
    )
```

```python
import jax
import jax.numpy as jnp
from jax import lax
from jax.experimental import pallas as pl
from jax.experimental.pallas import tpu as pltpu
from jax.sharding import Mesh, PartitionSpec as P


D = 2048
DK = 128
RANK = 32
BLOCK = 64
CTX_LIFT = 4.0
EPS = 1e-06
SHARP = 16.0
SEG = 512
CTX_SEG = 64
ROWS = SEG + CTX_SEG
PAYLOAD = 336
bf16 = jnp.bfloat16
f32 = jnp.float32
VM = pl.BlockSpec(memory_space=pltpu.VMEM)
SM = pl.BlockSpec(memory_space=pltpu.SMEM)


def to_everyone(x, axis):
    size = lax.axis_size(axis)
    return lax.all_to_all(jnp.broadcast_to(x[None], (size, *x.shape)), axis, 0, 0, tiled=True)


def three_parts(x):
    hi = x.astype(bf16)
    rest = x - hi.astype(f32)
    mid = rest.astype(bf16)
    lo = (rest - mid.astype(f32)).astype(bf16)
    return hi, mid, lo


def tri(rows, cols, upper):
    r = lax.broadcasted_iota(jnp.int32, (rows, cols), 0)
    c = lax.broadcasted_iota(jnp.int32, (rows, cols), 1)
    return (c >= r) if upper else (c <= r)


def summed_by(mask, a):
    m = mask.astype(f32).astype(bf16)
    stacked = jnp.concatenate(three_parts(a), axis=0)
    return jnp.dot(jnp.concatenate([m, m, m], axis=1), stacked, preferred_element_type=f32)


def nt(a, b):
    return lax.dot_general(a, b, (((1,), (1,)), ((), ())), preferred_element_type=f32)


def tn(a, b):
    return lax.dot_general(a, b, (((0,), (0,)), ((), ())), preferred_element_type=f32)


def pack_kernel(
    lat_ref, ctx_ref, sv_ref, cv_ref, mod_ref, wq_ref, wk_ref, wv_ref, extra_ref, rows_ref, cut_ref
):
    y = lax.axis_index("tp")
    dp = lax.axis_index("x") * 2 + lax.axis_index("core")
    rows_ref[0:32, :] = lat_ref[...]
    ctx = ctx_ref[...].astype(f32)
    picked = ctx[12:16]
    for i in range(3):
        picked = jnp.where(y == i, ctx[4 * i : 4 * i + 4], picked)
    rows_ref[32:36, :] = picked.astype(bf16)

    both = jnp.concatenate([sv_ref[...], cv_ref[...]], axis=0)
    conditions = (both / (1.0 + jnp.exp(-both))).astype(bf16)
    local_mods = nt(conditions, mod_ref[...])
    mods = jnp.concatenate([p.astype(f32) for p in three_parts(local_mods)], axis=0)
    mods = jnp.concatenate([mods, jnp.zeros((6, 32), f32)], axis=1)
    extra = jnp.concatenate([p.astype(f32) for p in three_parts(extra_ref[...])[:2]], axis=0)
    riding = jnp.concatenate([mods, extra, jnp.zeros((2, 128), f32)], axis=0).astype(bf16)
    mine = pl.ds(pl.multiple_of(dp * 16, 16), 16)
    for d in range(16):
        b = d % 4
        cut_ref[d, :, 0:128] = wq_ref[mine, (b // 2) * 128 : (b // 2 + 1) * 128]
        cut_ref[d, :, 128:256] = wk_ref[mine, (b // 2) * 128 : (b // 2 + 1) * 128]
        cut_ref[d, :, 256:384] = wv_ref[mine, b * 128 : (b + 1) * 128]
        cut_ref[d, :, 384:512] = riding


def project_kernel(
    own_ref, minus_ref, plus_ref, low_ref, high_ref, mod_ref, gain_ref, mine_ref, other_ref,
    down_ref, up_ref, bias_ref, ride_ref,
    pay_ref, q_ref, k_ref, v_ref, cum_ref, h_ref, w_ref,
):
    seg, sub = lax.axis_index("A"), lax.axis_index("B")
    y, core = lax.axis_index("tp"), lax.axis_index("core")
    second = sub >= 2
    for xi in range(4):
        for z in range(16):
            at = z * 128 + xi * 32
            here = pl.ds(pl.multiple_of(at + core * 16, 16), 16)
            there = pl.ds(pl.multiple_of(at + 16 - core * 16, 16), 16)
            w_ref[here, :] = mine_ref[xi, z]
            w_ref[there, :] = other_ref[xi, z]

    def normed_rows(rows, which):
        v = rows.astype(f32)
        r = lax.rsqrt(jnp.mean(v * v, axis=-1, keepdims=True) + EPS)
        scale = gain_ref[...] * (1.0 + mod_ref[which : which + 1, D : 2 * D])
        return (v * r * scale + mod_ref[which : which + 1, 0:D]).astype(bf16)

    y_of = [y, (y + 3) % 4, (y + 1) % 4, (y + 2) % 4]
    for slot in range(4):
        for j in range(4):
            if slot < 3:
                rows = (own_ref, minus_ref, plus_ref)[slot][j * 32 : j * 32 + 32, :]
            elif j < 2:
                rows = low_ref[j * 32 : j * 32 + 32, :]
            else:
                rows = high_ref[(j - 2) * 32 : (j - 2) * 32 + 32, :]
            at = pl.multiple_of((sub ^ j) * 128 + y_of[slot] * 32, 32)
            h_ref[pl.ds(at, 32), :] = normed_rows(rows, 0)
        rows = (own_ref, minus_ref, plus_ref)[slot][128:144, :] if slot < 3 else high_ref[64:80, :]
        h_ref[SEG + slot * 16 : SEG + slot * 16 + 16, :] = normed_rows(rows, 1)

    out = jnp.dot(h_ref[...], w_ref[...], preferred_element_type=f32).astype(bf16)
    q_ref[...] = out[:SEG, 0:128]
    k_ref[...] = out[:SEG, 128:256]
    v_ref[...] = out[:SEG, 256:384]
    low = nt(h_ref[...], down_ref[...]).astype(bf16)

    def of_head(a):
        return jnp.where(second, a[:, 128:256].astype(f32), a[:, 0:128].astype(f32))

    raw = []
    for z in range(2):
        up = of_head(up_ref[z]).astype(bf16)
        part = jnp.dot(low[:, z * RANK : (z + 1) * RANK], up, preferred_element_type=f32)
        raw.append(part + of_head(bias_ref[z : z + 1, :]))
    raw = jnp.concatenate(raw, axis=1)
    logs = (jnp.minimum(raw, 0.0) - jnp.log1p(jnp.exp(-jnp.abs(raw)))) * (1.0 / SHARP)
    ef, eb = [], []
    for zb in range(4):
        t = jnp.transpose(ride_ref[seg * 4 + zb].astype(f32))
        ef.append(jnp.where(second, t[:, 7:8] + t[:, 11:12], t[:, 6:7] + t[:, 10:11]))
        eb.append(jnp.where(second, t[:, 9:10] + t[:, 13:14], t[:, 8:9] + t[:, 12:13]))
    ef = jnp.concatenate(ef, axis=0)
    eb = jnp.concatenate(eb, axis=0)
    af = logs[:SEG, 0:128] + ef
    ab = logs[:SEG, 128:256] + eb
    low_mask = tri(BLOCK, BLOCK, False)
    up_mask = tri(BLOCK, BLOCK, True)
    wf, wb = [], []
    for n in range(SEG // BLOCK):
        sl = slice(n * BLOCK, (n + 1) * BLOCK)
        wf.append(summed_by(low_mask, af[sl]))
        wb.append(summed_by(up_mask, ab[sl]))
        cum_ref[0, sl, :] = wf[-1]
        cum_ref[1, sl, :] = wb[-1]
    tot_f = [w[BLOCK - 1 : BLOCK] for w in wf]
    tot_b = [w[0:1] for w in wb]
    dev_f = sum(tot_f)
    dev_b = sum(tot_b)
    kk = out[:SEG, 128:256].astype(f32)
    before = jnp.zeros((1, DK), f32)
    kf = []
    for n in range(SEG // BLOCK):
        kf.append(kk[n * BLOCK : (n + 1) * BLOCK] * jnp.exp(dev_f - before - wf[n]))
        before = before + tot_f[n]
    after = jnp.zeros((1, DK), f32)
    kb = [None] * (SEG // BLOCK)
    for n in reversed(range(SEG // BLOCK)):
        kb[n] = kk[n * BLOCK : (n + 1) * BLOCK] * jnp.exp(dev_b - after - wb[n])
        after = after + tot_b[n]
    both = jnp.concatenate(
        [jnp.concatenate(kf, 0).astype(bf16), jnp.concatenate(kb, 0).astype(bf16)], axis=1
    )
    states = tn(out[:SEG, 256:384], both).astype(bf16)

    def order(i):
        slot = i // 16
        step = jnp.where(slot == 0, 0, jnp.where(slot == 1, 3, slot - 1))
        return (((i % 16) // 4) ^ sub) * 16 + ((step + y) % 4) * 4 + i % 4

    r = order(lax.broadcasted_iota(jnp.int32, (CTX_SEG, CTX_SEG), 0))
    c = order(lax.broadcasted_iota(jnp.int32, (CTX_SEG, CTX_SEG), 1))
    later = summed_by(c > r, logs[SEG:, 0:128])
    earlier = summed_by(c < r, logs[SEG:, 128:256])
    ctx_f = jnp.sum(logs[SEG:, 0:128], axis=0, keepdims=True)
    ctx_b = jnp.sum(logs[SEG:, 128:256], axis=0, keepdims=True)
    ck = out[SEG:, 128:256].astype(f32)
    ckf = (ck * jnp.exp(later)).astype(bf16)
    ckb = (ck * jnp.exp(earlier)).astype(bf16)
    cv = out[SEG:, 256:384]
    zero = jnp.zeros((7, DK), bf16)
    for peer in range(4):
        ahead = peer > seg
        pay_ref[peer, 0:128, :] = jnp.where(ahead, states[:, 0:128], states[:, 128:256])
        pay_ref[peer, 128:192, :] = ckf
        pay_ref[peer, 192:256, :] = ckb
        pay_ref[peer, 256:320, :] = cv
        dev = jnp.where(ahead, dev_f, dev_b)
        pay_ref[peer, 320:336, :] = jnp.concatenate(
            [*three_parts(dev), *three_parts(ctx_f), *three_parts(ctx_b), zero], axis=0
        )


def local_kernel(q_ref, k_ref, v_ref, cum_ref, o_ref, lift_f_ref, lift_b_ref):
    blocks = SEG // BLOCK
    low_mask = tri(BLOCK, BLOCK, False)
    up_mask = tri(BLOCK, BLOCK, True)
    tot_f = [cum_ref[0, (n + 1) * BLOCK - 1 : (n + 1) * BLOCK, :] for n in range(blocks)]
    tot_b = [cum_ref[1, n * BLOCK : n * BLOCK + 1, :] for n in range(blocks)]
    state = jnp.zeros((DK, DK), f32)
    before = jnp.zeros((1, DK), f32)
    for n in range(blocks):
        sl = slice(n * BLOCK, (n + 1) * BLOCK)
        q = q_ref[sl, :].astype(f32)
        k = k_ref[sl, :].astype(f32)
        v = v_ref[sl, :]
        wf = cum_ref[0, sl, :]
        wb = cum_ref[1, sl, :]
        mf = 0.5 * tot_f[n]
        mb = 0.5 * tot_b[n]
        sf = nt((q * jnp.exp(wf - mf)).astype(bf16), (k * jnp.exp(mf - wf)).astype(bf16))
        sb = nt((q * jnp.exp(wb - mb)).astype(bf16), (k * jnp.exp(mb - wb)).astype(bf16))
        scores = jnp.where(low_mask, sf, 0.0) + jnp.where(up_mask, sb, 0.0)
        out = jnp.dot(scores.astype(bf16), v, preferred_element_type=f32)
        qd = q * jnp.exp(wf)
        lift_f_ref[sl, :] = (qd * jnp.exp(before)).astype(bf16)
        if n > 0:
            out = out + nt(qd.astype(bf16), state.astype(bf16))
        o_ref[sl, :] = out
        if n < blocks - 1:
            state = jnp.exp(tot_f[n]) * state + tn(v, (k * jnp.exp(tot_f[n] - wf)).astype(bf16))
        before = before + tot_f[n]
    state = jnp.zeros((DK, DK), f32)
    after = jnp.zeros((1, DK), f32)
    for n in reversed(range(blocks)):
        sl = slice(n * BLOCK, (n + 1) * BLOCK)
        q = q_ref[sl, :].astype(f32)
        k = k_ref[sl, :].astype(f32)
        v = v_ref[sl, :]
        wb = cum_ref[1, sl, :]
        qd = q * jnp.exp(wb)
        lift_b_ref[sl, :] = (qd * jnp.exp(after)).astype(bf16)
        if n < blocks - 1:
            o_ref[sl, :] = o_ref[sl, :] + nt(qd.astype(bf16), state.astype(bf16))
        if n > 0:
            state = jnp.exp(tot_b[n]) * state + tn(v, (k * jnp.exp(tot_b[n] - wb)).astype(bf16))
        after = after + tot_b[n]


def combine_kernel(in_ref, o_ref, lift_f_ref, lift_b_ref, out_ref):
    seg = lax.axis_index("A")

    def vec(peer, at):
        rows = in_ref[peer, 320:336, :].astype(f32)
        return rows[at : at + 1] + rows[at + 1 : at + 2] + rows[at + 2 : at + 3]

    ctx_f = jnp.zeros((DK, DK), f32)
    ctx_b = jnp.zeros((DK, DK), f32)
    for q in range(4):
        ctx_f = jnp.exp(vec(q, 3)) * ctx_f + tn(in_ref[q, 256:320, :], in_ref[q, 128:192, :])
    for q in reversed(range(4)):
        ctx_b = jnp.exp(vec(q, 6)) * ctx_b + tn(in_ref[q, 256:320, :], in_ref[q, 192:256, :])
    fwd = CTX_LIFT * ctx_f
    for a in range(3):
        moved = jnp.exp(vec(a, 0)) * fwd + in_ref[a, 0:128, :].astype(f32)
        fwd = jnp.where(a < seg, moved, fwd)
    bwd = CTX_LIFT * ctx_b
    for a in (3, 2, 1):
        moved = jnp.exp(vec(a, 0)) * bwd + in_ref[a, 0:128, :].astype(f32)
        bwd = jnp.where(a > seg, moved, bwd)
    out = o_ref[...] + nt(lift_f_ref[...], fwd.astype(bf16)) + nt(lift_b_ref[...], bwd.astype(bf16))
    out_ref[...] = out.astype(bf16)


def output_kernel(mix_ref, gain_ref, w_ref, out_ref):
    total = None
    for h in range(2):
        v = jnp.concatenate([mix_ref[2 * h], mix_ref[2 * h + 1]], axis=1).astype(f32)
        r = lax.rsqrt(jnp.mean(v * v, axis=-1, keepdims=True) + EPS)
        n = (v * r * gain_ref[...]).astype(bf16)
        part = jnp.dot(n, w_ref[h * 256 : (h + 1) * 256, :], preferred_element_type=f32)
        total = part if total is None else total + part
    out_ref[...] = total.astype(bf16)


def device_body(
    latents,
    sample_vector,
    context,
    context_vector,
    norm_gain,
    modulator,
    query_weight,
    key_weight,
    value_weight,
    decay_down,
    decay_up,
    decay_bias,
    decay_extra,
    head_gain,
    out_weight,
):
    y = lax.axis_index("tp")
    sds = jax.ShapeDtypeStruct
    rows, cut = pl.pallas_call(
        pack_kernel,
        out_shape=(sds((36, D), bf16), sds((16, 16, 512), bf16)),
        in_specs=[VM] * 9,
        out_specs=(VM, VM),
        name="pack",
    )(
        latents, context, sample_vector, context_vector, modulator.T,
        query_weight, key_weight, value_weight, jnp.moveaxis(decay_extra, 1, 2).reshape(4, 128),
    )
    near = [rows]
    for j in range(1, 4):
        near.append(lax.ppermute(rows, "B", [(b, b ^ j) for b in range(4)]))
    rows_z = lax.all_to_all(cut, ("A", "B"), 0, 0, tiled=True)
    mine = to_everyone(rows_z[:, :, 0:384], "x")
    other = lax.ppermute(mine, "core", [(0, 1), (1, 0)])
    ride = rows_z[:, :, 384:512]
    beside = lax.ppermute(ride, "tp", [(i, i ^ 1) for i in range(4)])
    pair = jnp.stack([ride, beside])
    across = lax.ppermute(pair, "tp", [(i, i ^ 3) for i in range(4)])
    parts = [p[:, 0:6, 0:96].astype(f32) for p in (ride, beside, across[0], across[1])]
    parts = [p[:, 0:2] + p[:, 2:4] + p[:, 4:6] for p in parts]
    odd, high_half = (y % 2) == 1, y >= 2
    near0, near1 = jnp.where(odd, parts[1], parts[0]), jnp.where(odd, parts[0], parts[1])
    far0, far1 = jnp.where(odd, parts[2], parts[3]), jnp.where(odd, parts[3], parts[2])
    ordered = [
        jnp.where(high_half, far0, near0),
        jnp.where(high_half, far1, near1),
        jnp.where(high_half, near0, far0),
        jnp.where(high_half, near1, far1),
    ]
    modulation = jnp.transpose(jnp.stack(ordered, axis=1), (2, 0, 1, 3)).reshape(2, 3 * D)

    own = jnp.concatenate([n[:32] for n in near] + [n[32:36] for n in near], axis=0)
    up_shift = [(i, (i + 1) % 4) for i in range(4)]
    down_shift = [(i, (i + 3) % 4) for i in range(4)]
    minus = lax.ppermute(own, "tp", up_shift)
    plus = lax.ppermute(own, "tp", down_shift)
    low = lax.ppermute(minus[:64], "tp", up_shift)
    high = lax.ppermute(plus[64:], "tp", down_shift)

    payload, q, k, v, cum = pl.pallas_call(
        project_kernel,
        out_shape=(
            sds((4, PAYLOAD, DK), bf16),
            sds((SEG, DK), bf16),
            sds((SEG, DK), bf16),
            sds((SEG, DK), bf16),
            sds((2, SEG, DK), f32),
        ),
        in_specs=[VM] * 13,
        out_specs=(VM,) * 5,
        scratch_shapes=[pltpu.VMEM((ROWS, D), bf16), pltpu.VMEM((D, 384), bf16)],
        name="project",
    )(
        own, minus, plus, low, high, modulation, norm_gain.reshape(1, D), mine, other,
        decay_down.T, decay_up, decay_bias, ride,
    )
    got = lax.all_to_all(payload, "A", 0, 0, tiled=True)
    local, lift_f, lift_b = pl.pallas_call(
        local_kernel,
        out_shape=(sds((SEG, DK), f32), sds((SEG, DK), bf16), sds((SEG, DK), bf16)),
        in_specs=[VM] * 4,
        out_specs=(VM,) * 3,
        name="local",
    )(q, k, v, cum)
    mixed = pl.pallas_call(
        combine_kernel,
        out_shape=sds((SEG, DK), bf16),
        in_specs=[VM] * 4,
        out_specs=VM,
        name="combine",
    )(got, local, lift_f, lift_b)
    heads = lax.all_to_all(mixed.reshape(4, 128, DK), "B", 0, 0, tiled=True)
    partial = pl.pallas_call(
        output_kernel,
        out_shape=sds((128, D), bf16),
        in_specs=[VM] * 3,
        out_specs=VM,
        name="output",
    )(heads, head_gain.reshape(1, 256), out_weight)
    shares = lax.all_to_all(partial.reshape(4, 32, D), "tp", 0, 0, tiled=True)
    projected = shares.astype(f32).sum(axis=0)
    projected = lax.optimization_barrier(projected.astype(bf16)).astype(f32)
    return (latents.astype(f32) + modulation[0:1, 2 * D :] * projected).astype(bf16)


def solution(mesh):
    mesh = Mesh(mesh.devices.reshape(4, 4, 4, 4, 2), ("A", "B", "tp", "x", "core"))
    dp = ("x", "core")
    sp = ("A", "B")
    placed = (
        P((*dp, *sp, "tp"), None),
        P(dp, None),
        P((*dp, *sp), None),
        P(),
        P(),
        P(None, (*sp, "tp")),
        P(sp, "tp"),
        P(sp, "tp"),
        P(sp, "tp"),
        P(),
        P(None, None, "tp"),
        P(None, "tp"),
        P(None, (*dp, *sp), "tp"),
        P(),
        P("tp", None),
    )
    return jax.shard_map(
        device_body,
        mesh=mesh,
        in_specs=placed,
        out_specs=P((*dp, *sp, "tp"), None),
        check_vma=False,
    )
```

```python
import jax
import jax.numpy as jnp
from jax import lax
from jax.experimental import pallas as pl
from jax.experimental.pallas import tpu as pltpu
from jax.sharding import Mesh, PartitionSpec as P


D = 2048
DK = 128
RANK = 32
BLOCK = 64
CTX_LIFT = 4.0
EPS = 1e-06
SHARP = 16.0
SEG = 512
CTX_SEG = 64
ROWS = SEG + CTX_SEG
PAYLOAD = 336
bf16 = jnp.bfloat16
f32 = jnp.float32
VM = pl.BlockSpec(memory_space=pltpu.VMEM)
SM = pl.BlockSpec(memory_space=pltpu.SMEM)


def to_everyone(x, axis):
    size = lax.axis_size(axis)
    return lax.all_to_all(jnp.broadcast_to(x[None], (size, *x.shape)), axis, 0, 0, tiled=True)


def three_parts(x):
    hi = x.astype(bf16)
    rest = x - hi.astype(f32)
    mid = rest.astype(bf16)
    lo = (rest - mid.astype(f32)).astype(bf16)
    return hi, mid, lo


def tri(rows, cols, upper):
    r = lax.broadcasted_iota(jnp.int32, (rows, cols), 0)
    c = lax.broadcasted_iota(jnp.int32, (rows, cols), 1)
    return (c >= r) if upper else (c <= r)


def summed_by(mask, a):
    m = mask.astype(f32).astype(bf16)
    stacked = jnp.concatenate(three_parts(a), axis=0)
    return jnp.dot(jnp.concatenate([m, m, m], axis=1), stacked, preferred_element_type=f32)


def nt(a, b):
    return lax.dot_general(a, b, (((1,), (1,)), ((), ())), preferred_element_type=f32)


def tn(a, b):
    return lax.dot_general(a, b, (((0,), (0,)), ((), ())), preferred_element_type=f32)


def pack_kernel(
    lat_ref, ctx_ref, sv_ref, cv_ref, mod_ref, wq_ref, wk_ref, wv_ref, extra_ref, rows_ref, cut_ref
):
    y = lax.axis_index("tp")
    dp = lax.axis_index("x") * 2 + lax.axis_index("core")
    rows_ref[0:32, :] = lat_ref[...]
    ctx = ctx_ref[...].astype(f32)
    picked = ctx[12:16]
    for i in range(3):
        picked = jnp.where(y == i, ctx[4 * i : 4 * i + 4], picked)
    rows_ref[32:36, :] = picked.astype(bf16)

    both = jnp.concatenate([sv_ref[...], cv_ref[...]], axis=0)
    conditions = (both / (1.0 + jnp.exp(-both))).astype(bf16)
    local_mods = nt(conditions, mod_ref[...])
    mods = jnp.concatenate([p.astype(f32) for p in three_parts(local_mods)], axis=0)
    mods = jnp.concatenate([mods, jnp.zeros((6, 32), f32)], axis=1)
    extra = jnp.concatenate([p.astype(f32) for p in three_parts(extra_ref[...])[:2]], axis=0)
    riding = jnp.concatenate([mods, extra, jnp.zeros((2, 128), f32)], axis=0).astype(bf16)
    mine = pl.ds(pl.multiple_of(dp * 16, 16), 16)
    for d in range(16):
        b = d % 4
        cut_ref[d, :, 0:128] = wq_ref[mine, (b // 2) * 128 : (b // 2 + 1) * 128]
        cut_ref[d, :, 128:256] = wk_ref[mine, (b // 2) * 128 : (b // 2 + 1) * 128]
        cut_ref[d, :, 256:384] = wv_ref[mine, b * 128 : (b + 1) * 128]
        cut_ref[d, :, 384:512] = riding


def project_kernel(
    own_ref, minus_ref, plus_ref, low_ref, high_ref, mod_ref, gain_ref, mine_ref, other_ref,
    down_ref, up_ref, bias_ref, ride_ref,
    pay_ref, q_ref, k_ref, v_ref, cum_ref, h_ref, w_ref,
):
    seg, sub = lax.axis_index("A"), lax.axis_index("B")
    y, core = lax.axis_index("tp"), lax.axis_index("core")
    second = sub >= 2
    for xi in range(4):
        for z in range(16):
            at = z * 128 + xi * 32
            here = pl.ds(pl.multiple_of(at + core * 16, 16), 16)
            there = pl.ds(pl.multiple_of(at + 16 - core * 16, 16), 16)
            w_ref[here, :] = mine_ref[xi, z]
            w_ref[there, :] = other_ref[xi, z]

    def normed_rows(rows, which):
        v = rows.astype(f32)
        r = lax.rsqrt(jnp.mean(v * v, axis=-1, keepdims=True) + EPS)
        scale = gain_ref[...] * (1.0 + mod_ref[which : which + 1, D : 2 * D])
        return (v * r * scale + mod_ref[which : which + 1, 0:D]).astype(bf16)

    y_of = [y, (y + 3) % 4, (y + 1) % 4, (y + 2) % 4]
    for slot in range(4):
        for j in range(4):
            if slot < 3:
                rows = (own_ref, minus_ref, plus_ref)[slot][j * 32 : j * 32 + 32, :]
            elif j < 2:
                rows = low_ref[j * 32 : j * 32 + 32, :]
            else:
                rows = high_ref[(j - 2) * 32 : (j - 2) * 32 + 32, :]
            at = pl.multiple_of((sub ^ j) * 128 + y_of[slot] * 32, 32)
            h_ref[pl.ds(at, 32), :] = normed_rows(rows, 0)
        rows = (own_ref, minus_ref, plus_ref)[slot][128:144, :] if slot < 3 else high_ref[64:80, :]
        h_ref[SEG + slot * 16 : SEG + slot * 16 + 16, :] = normed_rows(rows, 1)

    out = jnp.dot(h_ref[...], w_ref[...], preferred_element_type=f32).astype(bf16)
    q_ref[...] = out[:SEG, 0:128]
    k_ref[...] = out[:SEG, 128:256]
    v_ref[...] = out[:SEG, 256:384]
    low = nt(h_ref[...], down_ref[...]).astype(bf16)

    def of_head(a):
        return jnp.where(second, a[:, 128:256].astype(f32), a[:, 0:128].astype(f32))

    raw = []
    for z in range(2):
        up = of_head(up_ref[z]).astype(bf16)
        part = jnp.dot(low[:, z * RANK : (z + 1) * RANK], up, preferred_element_type=f32)
        raw.append(part + of_head(bias_ref[z : z + 1, :]))
    raw = jnp.concatenate(raw, axis=1)
    logs = (jnp.minimum(raw, 0.0) - jnp.log1p(jnp.exp(-jnp.abs(raw)))) * (1.0 / SHARP)
    ef, eb = [], []
    for zb in range(4):
        t = jnp.transpose(ride_ref[seg * 4 + zb].astype(f32))
        ef.append(jnp.where(second, t[:, 7:8] + t[:, 11:12], t[:, 6:7] + t[:, 10:11]))
        eb.append(jnp.where(second, t[:, 9:10] + t[:, 13:14], t[:, 8:9] + t[:, 12:13]))
    ef = jnp.concatenate(ef, axis=0)
    eb = jnp.concatenate(eb, axis=0)
    af = logs[:SEG, 0:128] + ef
    ab = logs[:SEG, 128:256] + eb
    low_mask = tri(BLOCK, BLOCK, False)
    up_mask = tri(BLOCK, BLOCK, True)
    wf, wb = [], []
    for n in range(SEG // BLOCK):
        sl = slice(n * BLOCK, (n + 1) * BLOCK)
        wf.append(summed_by(low_mask, af[sl]))
        wb.append(summed_by(up_mask, ab[sl]))
        cum_ref[0, sl, :] = wf[-1]
        cum_ref[1, sl, :] = wb[-1]
    tot_f = [w[BLOCK - 1 : BLOCK] for w in wf]
    tot_b = [w[0:1] for w in wb]
    dev_f = sum(tot_f)
    dev_b = sum(tot_b)
    kk = out[:SEG, 128:256].astype(f32)
    before = jnp.zeros((1, DK), f32)
    kf = []
    for n in range(SEG // BLOCK):
        kf.append(kk[n * BLOCK : (n + 1) * BLOCK] * jnp.exp(dev_f - before - wf[n]))
        before = before + tot_f[n]
    after = jnp.zeros((1, DK), f32)
    kb = [None] * (SEG // BLOCK)
    for n in reversed(range(SEG // BLOCK)):
        kb[n] = kk[n * BLOCK : (n + 1) * BLOCK] * jnp.exp(dev_b - after - wb[n])
        after = after + tot_b[n]
    both = jnp.concatenate(
        [jnp.concatenate(kf, 0).astype(bf16), jnp.concatenate(kb, 0).astype(bf16)], axis=1
    )
    states = tn(out[:SEG, 256:384], both).astype(bf16)

    def order(i):
        slot = i // 16
        step = jnp.where(slot == 0, 0, jnp.where(slot == 1, 3, slot - 1))
        return (((i % 16) // 4) ^ sub) * 16 + ((step + y) % 4) * 4 + i % 4

    r = order(lax.broadcasted_iota(jnp.int32, (CTX_SEG, CTX_SEG), 0))
    c = order(lax.broadcasted_iota(jnp.int32, (CTX_SEG, CTX_SEG), 1))
    later = summed_by(c > r, logs[SEG:, 0:128])
    earlier = summed_by(c < r, logs[SEG:, 128:256])
    ctx_f = jnp.sum(logs[SEG:, 0:128], axis=0, keepdims=True)
    ctx_b = jnp.sum(logs[SEG:, 128:256], axis=0, keepdims=True)
    ck = out[SEG:, 128:256].astype(f32)
    ckf = (ck * jnp.exp(later)).astype(bf16)
    ckb = (ck * jnp.exp(earlier)).astype(bf16)
    cv = out[SEG:, 256:384]
    zero = jnp.zeros((7, DK), bf16)
    for peer in range(4):
        ahead = peer > seg
        pay_ref[peer, 0:128, :] = jnp.where(ahead, states[:, 0:128], states[:, 128:256])
        pay_ref[peer, 128:192, :] = ckf
        pay_ref[peer, 192:256, :] = ckb
        pay_ref[peer, 256:320, :] = cv
        dev = jnp.where(ahead, dev_f, dev_b)
        pay_ref[peer, 320:336, :] = jnp.concatenate(
            [*three_parts(dev), *three_parts(ctx_f), *three_parts(ctx_b), zero], axis=0
        )


def local_kernel(q_ref, k_ref, v_ref, cum_ref, o_ref, lift_f_ref, lift_b_ref):
    blocks = SEG // BLOCK
    low_mask = tri(BLOCK, BLOCK, False)
    up_mask = tri(BLOCK, BLOCK, True)
    tot_f = [cum_ref[0, (n + 1) * BLOCK - 1 : (n + 1) * BLOCK, :] for n in range(blocks)]
    tot_b = [cum_ref[1, n * BLOCK : n * BLOCK + 1, :] for n in range(blocks)]
    state = jnp.zeros((DK, DK), f32)
    before = jnp.zeros((1, DK), f32)
    for n in range(blocks):
        sl = slice(n * BLOCK, (n + 1) * BLOCK)
        q = q_ref[sl, :].astype(f32)
        k = k_ref[sl, :].astype(f32)
        v = v_ref[sl, :]
        wf = cum_ref[0, sl, :]
        wb = cum_ref[1, sl, :]
        mf = 0.5 * tot_f[n]
        mb = 0.5 * tot_b[n]
        sf = nt((q * jnp.exp(wf - mf)).astype(bf16), (k * jnp.exp(mf - wf)).astype(bf16))
        sb = nt((q * jnp.exp(wb - mb)).astype(bf16), (k * jnp.exp(mb - wb)).astype(bf16))
        scores = jnp.where(low_mask, sf, 0.0) + jnp.where(up_mask, sb, 0.0)
        out = jnp.dot(scores.astype(bf16), v, preferred_element_type=f32)
        qd = q * jnp.exp(wf)
        lift_f_ref[sl, :] = (qd * jnp.exp(before)).astype(bf16)
        if n > 0:
            out = out + nt(qd.astype(bf16), state.astype(bf16))
        o_ref[sl, :] = out
        if n < blocks - 1:
            state = jnp.exp(tot_f[n]) * state + tn(v, (k * jnp.exp(tot_f[n] - wf)).astype(bf16))
        before = before + tot_f[n]
    state = jnp.zeros((DK, DK), f32)
    after = jnp.zeros((1, DK), f32)
    for n in reversed(range(blocks)):
        sl = slice(n * BLOCK, (n + 1) * BLOCK)
        q = q_ref[sl, :].astype(f32)
        k = k_ref[sl, :].astype(f32)
        v = v_ref[sl, :]
        wb = cum_ref[1, sl, :]
        qd = q * jnp.exp(wb)
        lift_b_ref[sl, :] = (qd * jnp.exp(after)).astype(bf16)
        if n < blocks - 1:
            o_ref[sl, :] = o_ref[sl, :] + nt(qd.astype(bf16), state.astype(bf16))
        if n > 0:
            state = jnp.exp(tot_b[n]) * state + tn(v, (k * jnp.exp(tot_b[n] - wb)).astype(bf16))
        after = after + tot_b[n]


def combine_kernel(in_ref, o_ref, lift_f_ref, lift_b_ref, out_ref):
    seg = lax.axis_index("A")

    def vec(peer, at):
        rows = in_ref[peer, 320:336, :].astype(f32)
        return rows[at : at + 1] + rows[at + 1 : at + 2] + rows[at + 2 : at + 3]

    ctx_f = jnp.zeros((DK, DK), f32)
    ctx_b = jnp.zeros((DK, DK), f32)
    for q in range(4):
        ctx_f = jnp.exp(vec(q, 3)) * ctx_f + tn(in_ref[q, 256:320, :], in_ref[q, 128:192, :])
    for q in reversed(range(4)):
        ctx_b = jnp.exp(vec(q, 6)) * ctx_b + tn(in_ref[q, 256:320, :], in_ref[q, 192:256, :])
    fwd = CTX_LIFT * ctx_f
    for a in range(3):
        moved = jnp.exp(vec(a, 0)) * fwd + in_ref[a, 0:128, :].astype(f32)
        fwd = jnp.where(a < seg, moved, fwd)
    bwd = CTX_LIFT * ctx_b
    for a in (3, 2, 1):
        moved = jnp.exp(vec(a, 0)) * bwd + in_ref[a, 0:128, :].astype(f32)
        bwd = jnp.where(a > seg, moved, bwd)
    out = o_ref[...] + nt(lift_f_ref[...], fwd.astype(bf16)) + nt(lift_b_ref[...], bwd.astype(bf16))
    out_ref[...] = out.astype(bf16)


def output_kernel(mix_ref, gain_ref, w_ref, out_ref):
    total = None
    for h in range(2):
        v = jnp.concatenate([mix_ref[2 * h], mix_ref[2 * h + 1]], axis=1).astype(f32)
        r = lax.rsqrt(jnp.mean(v * v, axis=-1, keepdims=True) + EPS)
        n = (v * r * gain_ref[...]).astype(bf16)
        part = jnp.dot(n, w_ref[h * 256 : (h + 1) * 256, :], preferred_element_type=f32)
        total = part if total is None else total + part
    out_ref[...] = total.astype(bf16)


def device_body(
    latents,
    sample_vector,
    context,
    context_vector,
    norm_gain,
    modulator,
    query_weight,
    key_weight,
    value_weight,
    decay_down,
    decay_up,
    decay_bias,
    decay_extra,
    head_gain,
    out_weight,
):
    y = lax.axis_index("tp")
    sds = jax.ShapeDtypeStruct
    rows, cut = pl.pallas_call(
        pack_kernel,
        out_shape=(sds((36, D), bf16), sds((16, 16, 512), bf16)),
        in_specs=[VM] * 9,
        out_specs=(VM, VM),
        name="pack",
    )(
        latents, context, sample_vector, context_vector, modulator.T,
        query_weight, key_weight, value_weight, jnp.moveaxis(decay_extra, 1, 2).reshape(4, 128),
    )
    near = [rows]
    for j in range(1, 4):
        near.append(lax.ppermute(rows, "B", [(b, b ^ j) for b in range(4)]))
    rows_z = lax.all_to_all(cut, ("A", "B"), 0, 0, tiled=True)
    mine = to_everyone(rows_z[:, :, 0:384], "x")
    other = lax.ppermute(mine, "core", [(0, 1), (1, 0)])
    ride = rows_z[:, :, 384:512]
    mods = rows_z[:, 0:8, 384:512]
    beside = lax.ppermute(mods, "tp", [(i, i ^ 1) for i in range(4)])
    pair = jnp.stack([mods, beside])
    across = lax.ppermute(pair, "tp", [(i, i ^ 3) for i in range(4)])
    parts = [p[:, 0:6, 0:96].astype(f32) for p in (mods, beside, across[0], across[1])]
    parts = [p[:, 0:2] + p[:, 2:4] + p[:, 4:6] for p in parts]
    odd, high_half = (y % 2) == 1, y >= 2
    near0, near1 = jnp.where(odd, parts[1], parts[0]), jnp.where(odd, parts[0], parts[1])
    far0, far1 = jnp.where(odd, parts[2], parts[3]), jnp.where(odd, parts[3], parts[2])
    ordered = [
        jnp.where(high_half, far0, near0),
        jnp.where(high_half, far1, near1),
        jnp.where(high_half, near0, far0),
        jnp.where(high_half, near1, far1),
    ]
    modulation = jnp.transpose(jnp.stack(ordered, axis=1), (2, 0, 1, 3)).reshape(2, 3 * D)

    own = jnp.concatenate([n[:32] for n in near] + [n[32:36] for n in near], axis=0)
    up_shift = [(i, (i + 1) % 4) for i in range(4)]
    down_shift = [(i, (i + 3) % 4) for i in range(4)]
    minus = lax.ppermute(own, "tp", up_shift)
    plus = lax.ppermute(own, "tp", down_shift)
    low = lax.ppermute(minus[:64], "tp", up_shift)
    high = lax.ppermute(plus[64:], "tp", down_shift)

    payload, q, k, v, cum = pl.pallas_call(
        project_kernel,
        out_shape=(
            sds((4, PAYLOAD, DK), bf16),
            sds((SEG, DK), bf16),
            sds((SEG, DK), bf16),
            sds((SEG, DK), bf16),
            sds((2, SEG, DK), f32),
        ),
        in_specs=[VM] * 13,
        out_specs=(VM,) * 5,
        scratch_shapes=[pltpu.VMEM((ROWS, D), bf16), pltpu.VMEM((D, 384), bf16)],
        name="project",
    )(
        own, minus, plus, low, high, modulation, norm_gain.reshape(1, D), mine, other,
        decay_down.T, decay_up, decay_bias, ride,
    )
    got = lax.all_to_all(payload, "A", 0, 0, tiled=True)
    local, lift_f, lift_b = pl.pallas_call(
        local_kernel,
        out_shape=(sds((SEG, DK), f32), sds((SEG, DK), bf16), sds((SEG, DK), bf16)),
        in_specs=[VM] * 4,
        out_specs=(VM,) * 3,
        name="local",
    )(q, k, v, cum)
    mixed = pl.pallas_call(
        combine_kernel,
        out_shape=sds((SEG, DK), bf16),
        in_specs=[VM] * 4,
        out_specs=VM,
        name="combine",
    )(got, local, lift_f, lift_b)
    heads = lax.all_to_all(mixed.reshape(4, 128, DK), "B", 0, 0, tiled=True)
    partial = pl.pallas_call(
        output_kernel,
        out_shape=sds((128, D), bf16),
        in_specs=[VM] * 3,
        out_specs=VM,
        name="output",
    )(heads, head_gain.reshape(1, 256), out_weight)
    shares = lax.all_to_all(partial.reshape(4, 32, D), "tp", 0, 0, tiled=True)
    projected = shares.astype(f32).sum(axis=0)
    projected = lax.optimization_barrier(projected.astype(bf16)).astype(f32)
    return (latents.astype(f32) + modulation[0:1, 2 * D :] * projected).astype(bf16)


def solution(mesh):
    mesh = Mesh(mesh.devices.reshape(4, 4, 4, 4, 2), ("A", "B", "tp", "x", "core"))
    dp = ("x", "core")
    sp = ("A", "B")
    placed = (
        P((*dp, *sp, "tp"), None),
        P(dp, None),
        P((*dp, *sp), None),
        P(),
        P(),
        P(None, (*sp, "tp")),
        P(sp, "tp"),
        P(sp, "tp"),
        P(sp, "tp"),
        P(),
        P(None, None, "tp"),
        P(None, "tp"),
        P(None, (*dp, *sp), "tp"),
        P(),
        P("tp", None),
    )
    return jax.shard_map(
        device_body,
        mesh=mesh,
        in_specs=placed,
        out_specs=P((*dp, *sp, "tp"), None),
        check_vma=False,
    )
```

```python
import jax
import jax.numpy as jnp
from jax import lax
from jax.experimental import pallas as pl
from jax.experimental.pallas import tpu as pltpu
from jax.sharding import Mesh, PartitionSpec as P


D = 2048
DK = 128
RANK = 32
BLOCK = 64
CTX_LIFT = 4.0
EPS = 1e-06
SHARP = 16.0
SEG = 512
CTX_SEG = 64
ROWS = SEG + CTX_SEG
PAYLOAD = 336
bf16 = jnp.bfloat16
f32 = jnp.float32
VM = pl.BlockSpec(memory_space=pltpu.VMEM)
SM = pl.BlockSpec(memory_space=pltpu.SMEM)


def to_everyone(x, axis):
    size = lax.axis_size(axis)
    return lax.all_to_all(jnp.broadcast_to(x[None], (size, *x.shape)), axis, 0, 0, tiled=True)


def three_parts(x):
    hi = x.astype(bf16)
    rest = x - hi.astype(f32)
    mid = rest.astype(bf16)
    lo = (rest - mid.astype(f32)).astype(bf16)
    return hi, mid, lo


def tri(rows, cols, upper):
    r = lax.broadcasted_iota(jnp.int32, (rows, cols), 0)
    c = lax.broadcasted_iota(jnp.int32, (rows, cols), 1)
    return (c >= r) if upper else (c <= r)


def summed_by(mask, a):
    m = mask.astype(f32).astype(bf16)
    stacked = jnp.concatenate(three_parts(a), axis=0)
    return jnp.dot(jnp.concatenate([m, m, m], axis=1), stacked, preferred_element_type=f32)


def nt(a, b):
    return lax.dot_general(a, b, (((1,), (1,)), ((), ())), preferred_element_type=f32)


def tn(a, b):
    return lax.dot_general(a, b, (((0,), (0,)), ((), ())), preferred_element_type=f32)


def rows_kernel(lat_ref, ctx_ref, sv_ref, cv_ref, mod_ref, rows_ref, mods_ref):
    y = lax.axis_index("tp")
    rows_ref[0:32, :] = lat_ref[...]
    ctx = ctx_ref[...].astype(f32)
    picked = ctx[12:16]
    for i in range(3):
        picked = jnp.where(y == i, ctx[4 * i : 4 * i + 4], picked)
    rows_ref[32:36, :] = picked.astype(bf16)
    both = jnp.concatenate([sv_ref[...], cv_ref[...]], axis=0)
    conditions = (both / (1.0 + jnp.exp(-both))).astype(bf16)
    local_mods = nt(conditions, mod_ref[...])
    for i in range(4):
        mods_ref[i] = local_mods


def pack_kernel(mods_ref, wq_ref, wk_ref, wv_ref, extra_ref, cut_ref):
    dp = lax.axis_index("x") * 2 + lax.axis_index("core")
    mods = jnp.concatenate([mods_ref[i] for i in range(4)], axis=1)
    hi, mid, _ = three_parts(mods)
    pieces = [p[:, 128 * j : 128 * (j + 1)].astype(f32) for p in (hi, mid) for j in range(3)]
    e_hi, e_mid, _ = three_parts(extra_ref[...])
    e_hi, e_mid = e_hi.astype(f32), e_mid.astype(f32)
    riding = []
    for h in range(2):
        added = [e_hi[h : h + 1], e_mid[h : h + 1], e_hi[2 + h : 3 + h], e_mid[2 + h : 3 + h]]
        riding.append(jnp.concatenate([*pieces, *added], axis=0).astype(bf16))
    mine = pl.ds(pl.multiple_of(dp * 16, 16), 16)
    for d in range(16):
        b = d % 4
        h = b // 2
        cut_ref[d, :, 0:128] = wq_ref[mine, h * 128 : (h + 1) * 128]
        cut_ref[d, :, 128:256] = wk_ref[mine, h * 128 : (h + 1) * 128]
        cut_ref[d, :, 256:384] = wv_ref[mine, b * 128 : (b + 1) * 128]
        cut_ref[d, :, 384:512] = riding[h]


def normed_rows(rows, which, mod_ref, gain_ref):
    v = rows.astype(f32)
    r = lax.rsqrt(jnp.mean(v * v, axis=-1, keepdims=True) + EPS)
    scale = gain_ref[...] * (1.0 + mod_ref[which : which + 1, D : 2 * D])
    return (v * r * scale + mod_ref[which : which + 1, 0:D]).astype(bf16)


def hidden_kernel(own_ref, minus_ref, plus_ref, ride_ref, gain_ref, h_ref, mod_ref):
    for z in range(16):
        r = ride_ref[z].astype(f32)
        for j in range(3):
            both = r[2 * j : 2 * j + 2] + r[6 + 2 * j : 8 + 2 * j]
            mod_ref[:, (z * 3 + j) * 128 : (z * 3 + j + 1) * 128] = both
    for slot, ref in enumerate((own_ref, minus_ref, plus_ref)):
        for j in range(4):
            at = slot * 144 + j * 32
            h_ref[at : at + 32, :] = normed_rows(ref[j * 32 : j * 32 + 32, :], 0, mod_ref, gain_ref)
        at = slot * 144 + 128
        h_ref[at : at + 16, :] = normed_rows(ref[128:144, :], 1, mod_ref, gain_ref)


def project_kernel(
    h_ref, low_ref, high_ref, mod_ref, gain_ref, mine_ref, other_ref,
    down_ref, up_ref, bias_ref, ride_ref,
    pay_ref, q_ref, k_ref, v_ref, cum_ref, far_ref, w_ref, out_ref,
):
    seg, sub = lax.axis_index("A"), lax.axis_index("B")
    y, core = lax.axis_index("tp"), lax.axis_index("core")
    second = sub >= 2
    for xi in range(4):
        for z in range(16):
            at = z * 128 + xi * 32
            here = pl.ds(pl.multiple_of(at + core * 16, 16), 16)
            there = pl.ds(pl.multiple_of(at + 16 - core * 16, 16), 16)
            w_ref[here, :] = mine_ref[xi, z]
            w_ref[there, :] = other_ref[xi, z]
    for j in range(4):
        rows = (low_ref, high_ref)[j // 2][(j % 2) * 32 : (j % 2) * 32 + 32, :]
        far_ref[j * 32 : j * 32 + 32, :] = normed_rows(rows, 0, mod_ref, gain_ref)
    far_ref[128:144, :] = normed_rows(high_ref[64:80, :], 1, mod_ref, gain_ref)
    y_of = [y, (y + 3) % 4, (y + 1) % 4, (y + 2) % 4]
    for first, rows in ((0, h_ref[...]), (3, far_ref[...])):
        res = jnp.dot(rows, w_ref[...], preferred_element_type=f32).astype(bf16)
        res = jnp.concatenate([res, nt(rows, down_ref[...]).astype(bf16)], axis=1)
        for n in range(rows.shape[0] // 144):
            for j in range(4):
                at = pl.multiple_of((sub ^ j) * 128 + y_of[first + n] * 32, 32)
                out_ref[pl.ds(at, 32), 0:448] = res[n * 144 + j * 32 : n * 144 + j * 32 + 32]
            at = SEG + (first + n) * 16
            out_ref[at : at + 16, 0:448] = res[n * 144 + 128 : n * 144 + 144]
    out = out_ref[:, 0:448]
    q_ref[...] = out[:SEG, 0:128]
    k_ref[...] = out[:SEG, 128:256]
    v_ref[...] = out[:SEG, 256:384]
    low = out[:, 384:448]

    def of_head(a):
        return jnp.where(second, a[:, 128:256].astype(f32), a[:, 0:128].astype(f32))

    raw = []
    for z in range(2):
        up = of_head(up_ref[z]).astype(bf16)
        part = jnp.dot(low[:, z * RANK : (z + 1) * RANK], up, preferred_element_type=f32)
        raw.append(part + of_head(bias_ref[z : z + 1, :]))
    raw = jnp.concatenate(raw, axis=1)
    logs = (jnp.minimum(raw, 0.0) - jnp.log1p(jnp.exp(-jnp.abs(raw)))) * (1.0 / SHARP)
    ef, eb = [], []
    for zb in range(4):
        t = jnp.transpose(ride_ref[seg * 4 + zb].astype(f32))
        ef.append(t[:, 12:13] + t[:, 13:14])
        eb.append(t[:, 14:15] + t[:, 15:16])
    ef = jnp.concatenate(ef, axis=0)
    eb = jnp.concatenate(eb, axis=0)
    af = logs[:SEG, 0:128] + ef
    ab = logs[:SEG, 128:256] + eb
    low_mask = tri(BLOCK, BLOCK, False)
    up_mask = tri(BLOCK, BLOCK, True)
    wf, wb = [], []
    for n in range(SEG // BLOCK):
        sl = slice(n * BLOCK, (n + 1) * BLOCK)
        wf.append(summed_by(low_mask, af[sl]))
        wb.append(summed_by(up_mask, ab[sl]))
        cum_ref[0, sl, :] = wf[-1]
        cum_ref[1, sl, :] = wb[-1]
    tot_f = [w[BLOCK - 1 : BLOCK] for w in wf]
    tot_b = [w[0:1] for w in wb]
    dev_f = sum(tot_f)
    dev_b = sum(tot_b)
    kk = out[:SEG, 128:256].astype(f32)
    before = jnp.zeros((1, DK), f32)
    kf = []
    for n in range(SEG // BLOCK):
        kf.append(kk[n * BLOCK : (n + 1) * BLOCK] * jnp.exp(dev_f - before - wf[n]))
        before = before + tot_f[n]
    after = jnp.zeros((1, DK), f32)
    kb = [None] * (SEG // BLOCK)
    for n in reversed(range(SEG // BLOCK)):
        kb[n] = kk[n * BLOCK : (n + 1) * BLOCK] * jnp.exp(dev_b - after - wb[n])
        after = after + tot_b[n]
    both = jnp.concatenate(
        [jnp.concatenate(kf, 0).astype(bf16), jnp.concatenate(kb, 0).astype(bf16)], axis=1
    )
    states = tn(out[:SEG, 256:384], both).astype(bf16)

    def order(i):
        slot = i // 16
        step = jnp.where(slot == 0, 0, jnp.where(slot == 1, 3, slot - 1))
        return (((i % 16) // 4) ^ sub) * 16 + ((step + y) % 4) * 4 + i % 4

    r = order(lax.broadcasted_iota(jnp.int32, (CTX_SEG, CTX_SEG), 0))
    c = order(lax.broadcasted_iota(jnp.int32, (CTX_SEG, CTX_SEG), 1))
    later = summed_by(c > r, logs[SEG:, 0:128])
    earlier = summed_by(c < r, logs[SEG:, 128:256])
    ctx_f = jnp.sum(logs[SEG:, 0:128], axis=0, keepdims=True)
    ctx_b = jnp.sum(logs[SEG:, 128:256], axis=0, keepdims=True)
    ck = out[SEG:, 128:256].astype(f32)
    ckf = (ck * jnp.exp(later)).astype(bf16)
    ckb = (ck * jnp.exp(earlier)).astype(bf16)
    cv = out[SEG:, 256:384]
    zero = jnp.zeros((7, DK), bf16)
    for peer in range(4):
        ahead = peer > seg
        pay_ref[peer, 0:128, :] = jnp.where(ahead, states[:, 0:128], states[:, 128:256])
        pay_ref[peer, 128:192, :] = ckf
        pay_ref[peer, 192:256, :] = ckb
        pay_ref[peer, 256:320, :] = cv
        dev = jnp.where(ahead, dev_f, dev_b)
        pay_ref[peer, 320:336, :] = jnp.concatenate(
            [*three_parts(dev), *three_parts(ctx_f), *three_parts(ctx_b), zero], axis=0
        )


def local_kernel(q_ref, k_ref, v_ref, cum_ref, o_ref, lift_f_ref, lift_b_ref):
    blocks = SEG // BLOCK
    low_mask = tri(BLOCK, BLOCK, False)
    up_mask = tri(BLOCK, BLOCK, True)
    tot_f = [cum_ref[0, (n + 1) * BLOCK - 1 : (n + 1) * BLOCK, :] for n in range(blocks)]
    tot_b = [cum_ref[1, n * BLOCK : n * BLOCK + 1, :] for n in range(blocks)]
    state = jnp.zeros((DK, DK), f32)
    before = jnp.zeros((1, DK), f32)
    for n in range(blocks):
        sl = slice(n * BLOCK, (n + 1) * BLOCK)
        q = q_ref[sl, :].astype(f32)
        k = k_ref[sl, :].astype(f32)
        v = v_ref[sl, :]
        wf = cum_ref[0, sl, :]
        wb = cum_ref[1, sl, :]
        mf = 0.5 * tot_f[n]
        mb = 0.5 * tot_b[n]
        sf = nt((q * jnp.exp(wf - mf)).astype(bf16), (k * jnp.exp(mf - wf)).astype(bf16))
        sb = nt((q * jnp.exp(wb - mb)).astype(bf16), (k * jnp.exp(mb - wb)).astype(bf16))
        scores = jnp.where(low_mask, sf, 0.0) + jnp.where(up_mask, sb, 0.0)
        out = jnp.dot(scores.astype(bf16), v, preferred_element_type=f32)
        qd = q * jnp.exp(wf)
        lift_f_ref[sl, :] = (qd * jnp.exp(before)).astype(bf16)
        if n > 0:
            out = out + nt(qd.astype(bf16), state.astype(bf16))
        o_ref[sl, :] = out
        if n < blocks - 1:
            state = jnp.exp(tot_f[n]) * state + tn(v, (k * jnp.exp(tot_f[n] - wf)).astype(bf16))
        before = before + tot_f[n]
    state = jnp.zeros((DK, DK), f32)
    after = jnp.zeros((1, DK), f32)
    for n in reversed(range(blocks)):
        sl = slice(n * BLOCK, (n + 1) * BLOCK)
        q = q_ref[sl, :].astype(f32)
        k = k_ref[sl, :].astype(f32)
        v = v_ref[sl, :]
        wb = cum_ref[1, sl, :]
        qd = q * jnp.exp(wb)
        lift_b_ref[sl, :] = (qd * jnp.exp(after)).astype(bf16)
        if n < blocks - 1:
            o_ref[sl, :] = o_ref[sl, :] + nt(qd.astype(bf16), state.astype(bf16))
        if n > 0:
            state = jnp.exp(tot_b[n]) * state + tn(v, (k * jnp.exp(tot_b[n] - wb)).astype(bf16))
        after = after + tot_b[n]


def combine_kernel(in_ref, o_ref, lift_f_ref, lift_b_ref, out_ref):
    seg = lax.axis_index("A")

    def vec(peer, at):
        rows = in_ref[peer, 320:336, :].astype(f32)
        return rows[at : at + 1] + rows[at + 1 : at + 2] + rows[at + 2 : at + 3]

    ctx_f = jnp.zeros((DK, DK), f32)
    ctx_b = jnp.zeros((DK, DK), f32)
    for q in range(4):
        ctx_f = jnp.exp(vec(q, 3)) * ctx_f + tn(in_ref[q, 256:320, :], in_ref[q, 128:192, :])
    for q in reversed(range(4)):
        ctx_b = jnp.exp(vec(q, 6)) * ctx_b + tn(in_ref[q, 256:320, :], in_ref[q, 192:256, :])
    fwd = CTX_LIFT * ctx_f
    for a in range(3):
        moved = jnp.exp(vec(a, 0)) * fwd + in_ref[a, 0:128, :].astype(f32)
        fwd = jnp.where(a < seg, moved, fwd)
    bwd = CTX_LIFT * ctx_b
    for a in (3, 2, 1):
        moved = jnp.exp(vec(a, 0)) * bwd + in_ref[a, 0:128, :].astype(f32)
        bwd = jnp.where(a > seg, moved, bwd)
    out = o_ref[...] + nt(lift_f_ref[...], fwd.astype(bf16)) + nt(lift_b_ref[...], bwd.astype(bf16))
    out_ref[...] = out.astype(bf16)


def output_kernel(mix_ref, gain_ref, w_ref, out_ref):
    total = None
    for h in range(2):
        v = jnp.concatenate([mix_ref[2 * h], mix_ref[2 * h + 1]], axis=1).astype(f32)
        r = lax.rsqrt(jnp.mean(v * v, axis=-1, keepdims=True) + EPS)
        n = (v * r * gain_ref[...]).astype(bf16)
        part = jnp.dot(n, w_ref[h * 256 : (h + 1) * 256, :], preferred_element_type=f32)
        total = part if total is None else total + part
    out_ref[...] = total.astype(bf16)


def device_body(
    latents,
    sample_vector,
    context,
    context_vector,
    norm_gain,
    modulator,
    query_weight,
    key_weight,
    value_weight,
    decay_down,
    decay_up,
    decay_bias,
    decay_extra,
    head_gain,
    out_weight,
):
    sds = jax.ShapeDtypeStruct
    rows, mods = pl.pallas_call(
        rows_kernel,
        out_shape=(sds((36, D), bf16), sds((4, 2, 96), f32)),
        in_specs=[VM] * 5,
        out_specs=(VM, VM),
        name="rows",
    )(latents, context, sample_vector, context_vector, modulator.T)
    mods = lax.all_to_all(mods, "tp", 0, 0, tiled=True)
    near = [rows]
    for j in range(1, 4):
        near.append(lax.ppermute(rows, "B", [(b, b ^ j) for b in range(4)]))
    cut = pl.pallas_call(
        pack_kernel,
        out_shape=sds((16, 16, 512), bf16),
        in_specs=[VM] * 5,
        out_specs=VM,
        name="pack",
    )(
        mods, query_weight, key_weight, value_weight,
        jnp.moveaxis(decay_extra, 1, 2).reshape(4, 128),
    )
    rows_z = lax.all_to_all(cut, ("A", "B"), 0, 0, tiled=True)
    mine = to_everyone(rows_z[:, :, 0:384], "x")
    other = lax.ppermute(mine, "core", [(0, 1), (1, 0)])
    ride = rows_z[:, :, 384:512]

    own = jnp.concatenate([n[:32] for n in near] + [n[32:36] for n in near], axis=0)
    up_shift = [(i, (i + 1) % 4) for i in range(4)]
    down_shift = [(i, (i + 3) % 4) for i in range(4)]
    minus = lax.ppermute(own, "tp", up_shift)
    plus = lax.ppermute(own, "tp", down_shift)
    low = lax.ppermute(minus[:64], "tp", up_shift)
    high = lax.ppermute(plus[64:], "tp", down_shift)

    near_hidden, modulation = pl.pallas_call(
        hidden_kernel,
        out_shape=(sds((432, D), bf16), sds((2, 3 * D), f32)),
        in_specs=[VM] * 5,
        out_specs=(VM, VM),
        name="hidden",
    )(own, minus, plus, ride, norm_gain.reshape(1, D))
    payload, q, k, v, cum = pl.pallas_call(
        project_kernel,
        out_shape=(
            sds((4, PAYLOAD, DK), bf16),
            sds((SEG, DK), bf16),
            sds((SEG, DK), bf16),
            sds((SEG, DK), bf16),
            sds((2, SEG, DK), f32),
        ),
        in_specs=[VM] * 11,
        out_specs=(VM,) * 5,
        scratch_shapes=[
            pltpu.VMEM((144, D), bf16),
            pltpu.VMEM((D, 384), bf16),
            pltpu.VMEM((ROWS, 512), bf16),
        ],
        name="project",
    )(
        near_hidden, low, high, modulation, norm_gain.reshape(1, D), mine, other,
        decay_down.T, decay_up, decay_bias, ride,
    )
    got = lax.all_to_all(payload, "A", 0, 0, tiled=True)
    local, lift_f, lift_b = pl.pallas_call(
        local_kernel,
        out_shape=(sds((SEG, DK), f32), sds((SEG, DK), bf16), sds((SEG, DK), bf16)),
        in_specs=[VM] * 4,
        out_specs=(VM,) * 3,
        name="local",
    )(q, k, v, cum)
    mixed = pl.pallas_call(
        combine_kernel,
        out_shape=sds((SEG, DK), bf16),
        in_specs=[VM] * 4,
        out_specs=VM,
        name="combine",
    )(got, local, lift_f, lift_b)
    heads = lax.all_to_all(mixed.reshape(4, 128, DK), "B", 0, 0, tiled=True)
    partial = pl.pallas_call(
        output_kernel,
        out_shape=sds((128, D), bf16),
        in_specs=[VM] * 3,
        out_specs=VM,
        name="output",
    )(heads, head_gain.reshape(1, 256), out_weight)
    shares = lax.all_to_all(partial.reshape(4, 32, D), "tp", 0, 0, tiled=True)
    projected = shares.astype(f32).sum(axis=0)
    projected = lax.optimization_barrier(projected.astype(bf16)).astype(f32)
    return (latents.astype(f32) + modulation[0:1, 2 * D :] * projected).astype(bf16)


def solution(mesh):
    mesh = Mesh(mesh.devices.reshape(4, 4, 4, 4, 2), ("A", "B", "tp", "x", "core"))
    dp = ("x", "core")
    sp = ("A", "B")
    placed = (
        P((*dp, *sp, "tp"), None),
        P(dp, None),
        P((*dp, *sp), None),
        P(),
        P(),
        P(None, (*sp, "tp")),
        P(sp, "tp"),
        P(sp, "tp"),
        P(sp, "tp"),
        P(),
        P(None, None, "tp"),
        P(None, "tp"),
        P(None, (*dp, *sp), "tp"),
        P(),
        P("tp", None),
    )
    return jax.shard_map(
        device_body,
        mesh=mesh,
        in_specs=placed,
        out_specs=P((*dp, *sp, "tp"), None),
        check_vma=False,
    )
```

```python
import jax
import jax.numpy as jnp
from jax import lax
from jax.experimental import pallas as pl
from jax.experimental.pallas import tpu as pltpu
from jax.sharding import Mesh, PartitionSpec as P


D = 2048
DK = 128
RANK = 32
BLOCK = 64
CTX_LIFT = 4.0
EPS = 1e-06
SHARP = 16.0
SEG = 512
CTX_SEG = 64
ROWS = SEG + CTX_SEG
PAYLOAD = 336
bf16 = jnp.bfloat16
f32 = jnp.float32
VM = pl.BlockSpec(memory_space=pltpu.VMEM)
SM = pl.BlockSpec(memory_space=pltpu.SMEM)


def on_chip(*arrays):
    return tuple(pltpu.with_memory_space_constraint(a, pltpu.VMEM) for a in arrays)


def off_chip(*arrays):
    return tuple(pltpu.with_memory_space_constraint(a, pltpu.HBM) for a in arrays)


def to_everyone(x, axis):
    size = lax.axis_size(axis)
    return lax.all_to_all(jnp.broadcast_to(x[None], (size, *x.shape)), axis, 0, 0, tiled=True)


def three_parts(x):
    hi = x.astype(bf16)
    rest = x - hi.astype(f32)
    mid = rest.astype(bf16)
    lo = (rest - mid.astype(f32)).astype(bf16)
    return hi, mid, lo


def tri(rows, cols, upper):
    r = lax.broadcasted_iota(jnp.int32, (rows, cols), 0)
    c = lax.broadcasted_iota(jnp.int32, (rows, cols), 1)
    return (c >= r) if upper else (c <= r)


def summed_by(mask, a):
    m = mask.astype(f32).astype(bf16)
    stacked = jnp.concatenate(three_parts(a), axis=0)
    return jnp.dot(jnp.concatenate([m, m, m], axis=1), stacked, preferred_element_type=f32)


def nt(a, b):
    return lax.dot_general(a, b, (((1,), (1,)), ((), ())), preferred_element_type=f32)


def tn(a, b):
    return lax.dot_general(a, b, (((0,), (0,)), ((), ())), preferred_element_type=f32)


def rows_kernel(lat_ref, ctx_ref, sv_ref, cv_ref, mod_ref, rows_ref, mods_ref):
    y = lax.axis_index("tp")
    rows_ref[0:32, :] = lat_ref[...]
    ctx = ctx_ref[...].astype(f32)
    picked = ctx[12:16]
    for i in range(3):
        picked = jnp.where(y == i, ctx[4 * i : 4 * i + 4], picked)
    rows_ref[32:36, :] = picked.astype(bf16)
    both = jnp.concatenate([sv_ref[...], cv_ref[...]], axis=0)
    conditions = (both / (1.0 + jnp.exp(-both))).astype(bf16)
    local_mods = nt(conditions, mod_ref[...])
    for i in range(4):
        mods_ref[i] = local_mods


def pack_kernel(mods_ref, wq_ref, wk_ref, wv_ref, extra_ref, cut_ref):
    dp = lax.axis_index("x") * 2 + lax.axis_index("core")
    mods = jnp.concatenate([mods_ref[i] for i in range(4)], axis=1)
    hi, mid, _ = three_parts(mods)
    pieces = [p[:, 128 * j : 128 * (j + 1)].astype(f32) for p in (hi, mid) for j in range(3)]
    e_hi, e_mid, _ = three_parts(extra_ref[...])
    e_hi, e_mid = e_hi.astype(f32), e_mid.astype(f32)
    riding = []
    for h in range(2):
        added = [e_hi[h : h + 1], e_mid[h : h + 1], e_hi[2 + h : 3 + h], e_mid[2 + h : 3 + h]]
        riding.append(jnp.concatenate([*pieces, *added], axis=0).astype(bf16))
    mine = pl.ds(pl.multiple_of(dp * 16, 16), 16)
    for d in range(16):
        b = d % 4
        h = b // 2
        cut_ref[d, :, 0:128] = wq_ref[mine, h * 128 : (h + 1) * 128]
        cut_ref[d, :, 128:256] = wk_ref[mine, h * 128 : (h + 1) * 128]
        cut_ref[d, :, 256:384] = wv_ref[mine, b * 128 : (b + 1) * 128]
        cut_ref[d, :, 384:512] = riding[h]


def normed_rows(rows, which, mod_ref, gain_ref):
    v = rows.astype(f32)
    r = lax.rsqrt(jnp.mean(v * v, axis=-1, keepdims=True) + EPS)
    scale = gain_ref[...] * (1.0 + mod_ref[which : which + 1, D : 2 * D])
    return (v * r * scale + mod_ref[which : which + 1, 0:D]).astype(bf16)


def hidden_kernel(own_ref, minus_ref, plus_ref, ride_ref, gain_ref, h_ref, mod_ref):
    for z in range(16):
        r = ride_ref[z].astype(f32)
        for j in range(3):
            both = r[2 * j : 2 * j + 2] + r[6 + 2 * j : 8 + 2 * j]
            mod_ref[:, (z * 3 + j) * 128 : (z * 3 + j + 1) * 128] = both
    for slot, ref in enumerate((own_ref, minus_ref, plus_ref)):
        for j in range(4):
            at = slot * 144 + j * 32
            h_ref[at : at + 32, :] = normed_rows(ref[j * 32 : j * 32 + 32, :], 0, mod_ref, gain_ref)
        at = slot * 144 + 128
        h_ref[at : at + 16, :] = normed_rows(ref[128:144, :], 1, mod_ref, gain_ref)


def project_kernel(
    h_ref, low_ref, high_ref, mod_ref, gain_ref, mine_ref, other_ref,
    down_ref, up_ref, bias_ref, ride_ref,
    pay_ref, q_ref, k_ref, v_ref, cum_ref, far_ref, w_ref, out_ref,
):
    seg, sub = lax.axis_index("A"), lax.axis_index("B")
    y, core = lax.axis_index("tp"), lax.axis_index("core")
    second = sub >= 2
    for xi in range(4):
        for z in range(16):
            at = z * 128 + xi * 32
            here = pl.ds(pl.multiple_of(at + core * 16, 16), 16)
            there = pl.ds(pl.multiple_of(at + 16 - core * 16, 16), 16)
            w_ref[here, :] = mine_ref[xi, z]
            w_ref[there, :] = other_ref[xi, z]
    for j in range(4):
        rows = (low_ref, high_ref)[j // 2][(j % 2) * 32 : (j % 2) * 32 + 32, :]
        far_ref[j * 32 : j * 32 + 32, :] = normed_rows(rows, 0, mod_ref, gain_ref)
    far_ref[128:144, :] = normed_rows(high_ref[64:80, :], 1, mod_ref, gain_ref)
    y_of = [y, (y + 3) % 4, (y + 1) % 4, (y + 2) % 4]
    for first, rows in ((0, h_ref[...]), (3, far_ref[...])):
        res = jnp.dot(rows, w_ref[...], preferred_element_type=f32).astype(bf16)
        res = jnp.concatenate([res, nt(rows, down_ref[...]).astype(bf16)], axis=1)
        for n in range(rows.shape[0] // 144):
            for j in range(4):
                at = pl.multiple_of((sub ^ j) * 128 + y_of[first + n] * 32, 32)
                out_ref[pl.ds(at, 32), 0:448] = res[n * 144 + j * 32 : n * 144 + j * 32 + 32]
            at = SEG + (first + n) * 16
            out_ref[at : at + 16, 0:448] = res[n * 144 + 128 : n * 144 + 144]
    out = out_ref[:, 0:448]
    q_ref[...] = out[:SEG, 0:128]
    k_ref[...] = out[:SEG, 128:256]
    v_ref[...] = out[:SEG, 256:384]
    low = out[:, 384:448]

    def of_head(a):
        return jnp.where(second, a[:, 128:256].astype(f32), a[:, 0:128].astype(f32))

    raw = []
    for z in range(2):
        up = of_head(up_ref[z]).astype(bf16)
        part = jnp.dot(low[:, z * RANK : (z + 1) * RANK], up, preferred_element_type=f32)
        raw.append(part + of_head(bias_ref[z : z + 1, :]))
    raw = jnp.concatenate(raw, axis=1)
    logs = (jnp.minimum(raw, 0.0) - jnp.log1p(jnp.exp(-jnp.abs(raw)))) * (1.0 / SHARP)
    ef, eb = [], []
    for zb in range(4):
        t = jnp.transpose(ride_ref[seg * 4 + zb].astype(f32))
        ef.append(t[:, 12:13] + t[:, 13:14])
        eb.append(t[:, 14:15] + t[:, 15:16])
    ef = jnp.concatenate(ef, axis=0)
    eb = jnp.concatenate(eb, axis=0)
    af = logs[:SEG, 0:128] + ef
    ab = logs[:SEG, 128:256] + eb
    low_mask = tri(BLOCK, BLOCK, False)
    up_mask = tri(BLOCK, BLOCK, True)
    wf, wb = [], []
    for n in range(SEG // BLOCK):
        sl = slice(n * BLOCK, (n + 1) * BLOCK)
        wf.append(summed_by(low_mask, af[sl]))
        wb.append(summed_by(up_mask, ab[sl]))
        cum_ref[0, sl, :] = wf[-1]
        cum_ref[1, sl, :] = wb[-1]
    tot_f = [w[BLOCK - 1 : BLOCK] for w in wf]
    tot_b = [w[0:1] for w in wb]
    dev_f = sum(tot_f)
    dev_b = sum(tot_b)
    kk = out[:SEG, 128:256].astype(f32)
    before = jnp.zeros((1, DK), f32)
    kf = []
    for n in range(SEG // BLOCK):
        kf.append(kk[n * BLOCK : (n + 1) * BLOCK] * jnp.exp(dev_f - before - wf[n]))
        before = before + tot_f[n]
    after = jnp.zeros((1, DK), f32)
    kb = [None] * (SEG // BLOCK)
    for n in reversed(range(SEG // BLOCK)):
        kb[n] = kk[n * BLOCK : (n + 1) * BLOCK] * jnp.exp(dev_b - after - wb[n])
        after = after + tot_b[n]
    both = jnp.concatenate(
        [jnp.concatenate(kf, 0).astype(bf16), jnp.concatenate(kb, 0).astype(bf16)], axis=1
    )
    states = tn(out[:SEG, 256:384], both).astype(bf16)

    def order(i):
        slot = i // 16
        step = jnp.where(slot == 0, 0, jnp.where(slot == 1, 3, slot - 1))
        return (((i % 16) // 4) ^ sub) * 16 + ((step + y) % 4) * 4 + i % 4

    r = order(lax.broadcasted_iota(jnp.int32, (CTX_SEG, CTX_SEG), 0))
    c = order(lax.broadcasted_iota(jnp.int32, (CTX_SEG, CTX_SEG), 1))
    later = summed_by(c > r, logs[SEG:, 0:128])
    earlier = summed_by(c < r, logs[SEG:, 128:256])
    ctx_f = jnp.sum(logs[SEG:, 0:128], axis=0, keepdims=True)
    ctx_b = jnp.sum(logs[SEG:, 128:256], axis=0, keepdims=True)
    ck = out[SEG:, 128:256].astype(f32)
    ckf = (ck * jnp.exp(later)).astype(bf16)
    ckb = (ck * jnp.exp(earlier)).astype(bf16)
    cv = out[SEG:, 256:384]
    zero = jnp.zeros((7, DK), bf16)
    for peer in range(4):
        ahead = peer > seg
        pay_ref[peer, 0:128, :] = jnp.where(ahead, states[:, 0:128], states[:, 128:256])
        pay_ref[peer, 128:192, :] = ckf
        pay_ref[peer, 192:256, :] = ckb
        pay_ref[peer, 256:320, :] = cv
        dev = jnp.where(ahead, dev_f, dev_b)
        pay_ref[peer, 320:336, :] = jnp.concatenate(
            [*three_parts(dev), *three_parts(ctx_f), *three_parts(ctx_b), zero], axis=0
        )


def local_kernel(q_ref, k_ref, v_ref, cum_ref, o_ref, lift_f_ref, lift_b_ref):
    blocks = SEG // BLOCK
    low_mask = tri(BLOCK, BLOCK, False)
    up_mask = tri(BLOCK, BLOCK, True)
    tot_f = [cum_ref[0, (n + 1) * BLOCK - 1 : (n + 1) * BLOCK, :] for n in range(blocks)]
    tot_b = [cum_ref[1, n * BLOCK : n * BLOCK + 1, :] for n in range(blocks)]
    state = jnp.zeros((DK, DK), f32)
    before = jnp.zeros((1, DK), f32)
    for n in range(blocks):
        sl = slice(n * BLOCK, (n + 1) * BLOCK)
        q = q_ref[sl, :].astype(f32)
        k = k_ref[sl, :].astype(f32)
        v = v_ref[sl, :]
        wf = cum_ref[0, sl, :]
        wb = cum_ref[1, sl, :]
        mf = 0.5 * tot_f[n]
        mb = 0.5 * tot_b[n]
        sf = nt((q * jnp.exp(wf - mf)).astype(bf16), (k * jnp.exp(mf - wf)).astype(bf16))
        sb = nt((q * jnp.exp(wb - mb)).astype(bf16), (k * jnp.exp(mb - wb)).astype(bf16))
        scores = jnp.where(low_mask, sf, 0.0) + jnp.where(up_mask, sb, 0.0)
        out = jnp.dot(scores.astype(bf16), v, preferred_element_type=f32)
        qd = q * jnp.exp(wf)
        lift_f_ref[sl, :] = (qd * jnp.exp(before)).astype(bf16)
        if n > 0:
            out = out + nt(qd.astype(bf16), state.astype(bf16))
        o_ref[sl, :] = out
        if n < blocks - 1:
            state = jnp.exp(tot_f[n]) * state + tn(v, (k * jnp.exp(tot_f[n] - wf)).astype(bf16))
        before = before + tot_f[n]
    state = jnp.zeros((DK, DK), f32)
    after = jnp.zeros((1, DK), f32)
    for n in reversed(range(blocks)):
        sl = slice(n * BLOCK, (n + 1) * BLOCK)
        q = q_ref[sl, :].astype(f32)
        k = k_ref[sl, :].astype(f32)
        v = v_ref[sl, :]
        wb = cum_ref[1, sl, :]
        qd = q * jnp.exp(wb)
        lift_b_ref[sl, :] = (qd * jnp.exp(after)).astype(bf16)
        if n < blocks - 1:
            o_ref[sl, :] = o_ref[sl, :] + nt(qd.astype(bf16), state.astype(bf16))
        if n > 0:
            state = jnp.exp(tot_b[n]) * state + tn(v, (k * jnp.exp(tot_b[n] - wb)).astype(bf16))
        after = after + tot_b[n]


def combine_kernel(in_ref, o_ref, lift_f_ref, lift_b_ref, out_ref):
    seg = lax.axis_index("A")

    def vec(peer, at):
        rows = in_ref[peer, 320:336, :].astype(f32)
        return rows[at : at + 1] + rows[at + 1 : at + 2] + rows[at + 2 : at + 3]

    ctx_f = jnp.zeros((DK, DK), f32)
    ctx_b = jnp.zeros((DK, DK), f32)
    for q in range(4):
        ctx_f = jnp.exp(vec(q, 3)) * ctx_f + tn(in_ref[q, 256:320, :], in_ref[q, 128:192, :])
    for q in reversed(range(4)):
        ctx_b = jnp.exp(vec(q, 6)) * ctx_b + tn(in_ref[q, 256:320, :], in_ref[q, 192:256, :])
    fwd = CTX_LIFT * ctx_f
    for a in range(3):
        moved = jnp.exp(vec(a, 0)) * fwd + in_ref[a, 0:128, :].astype(f32)
        fwd = jnp.where(a < seg, moved, fwd)
    bwd = CTX_LIFT * ctx_b
    for a in (3, 2, 1):
        moved = jnp.exp(vec(a, 0)) * bwd + in_ref[a, 0:128, :].astype(f32)
        bwd = jnp.where(a > seg, moved, bwd)
    out = o_ref[...] + nt(lift_f_ref[...], fwd.astype(bf16)) + nt(lift_b_ref[...], bwd.astype(bf16))
    out_ref[...] = out.astype(bf16)


def output_kernel(mix_ref, gain_ref, w_ref, out_ref):
    total = None
    for h in range(2):
        v = jnp.concatenate([mix_ref[2 * h], mix_ref[2 * h + 1]], axis=1).astype(f32)
        r = lax.rsqrt(jnp.mean(v * v, axis=-1, keepdims=True) + EPS)
        n = (v * r * gain_ref[...]).astype(bf16)
        part = jnp.dot(n, w_ref[h * 256 : (h + 1) * 256, :], preferred_element_type=f32)
        total = part if total is None else total + part
    out_ref[...] = total.astype(bf16)


def device_body(
    latents,
    sample_vector,
    context,
    context_vector,
    norm_gain,
    modulator,
    query_weight,
    key_weight,
    value_weight,
    decay_down,
    decay_up,
    decay_bias,
    decay_extra,
    head_gain,
    out_weight,
):
    sds = jax.ShapeDtypeStruct
    rows, mods = pl.pallas_call(
        rows_kernel,
        out_shape=(sds((36, D), bf16), sds((4, 2, 96), f32)),
        in_specs=[VM] * 5,
        out_specs=(VM, VM),
        compiler_params=pltpu.CompilerParams(vmem_limit_bytes=12 * 1024 * 1024),
        name="rows",
    )(*off_chip(latents, context, sample_vector, context_vector, modulator.T))
    mods = lax.all_to_all(mods, "tp", 0, 0, tiled=True)
    near = [rows]
    for j in range(1, 4):
        near.append(lax.ppermute(rows, "B", [(b, b ^ j) for b in range(4)]))
    cut = pl.pallas_call(
        pack_kernel,
        out_shape=sds((16, 16, 512), bf16),
        in_specs=[VM] * 5,
        out_specs=VM,
        compiler_params=pltpu.CompilerParams(vmem_limit_bytes=12 * 1024 * 1024),
        name="pack",
    )(
        *on_chip(mods),
        *off_chip(
            query_weight, key_weight, value_weight,
            jnp.moveaxis(decay_extra, 1, 2).reshape(4, 128),
        ),
    )
    rows_z = lax.all_to_all(cut, ("A", "B"), 0, 0, tiled=True)
    mine = to_everyone(rows_z[:, :, 0:384], "x")
    other = lax.ppermute(mine, "core", [(0, 1), (1, 0)])
    ride = rows_z[:, :, 384:512]

    own = jnp.concatenate([n[:32] for n in near] + [n[32:36] for n in near], axis=0)
    up_shift = [(i, (i + 1) % 4) for i in range(4)]
    down_shift = [(i, (i + 3) % 4) for i in range(4)]
    minus = lax.ppermute(own, "tp", up_shift)
    plus = lax.ppermute(own, "tp", down_shift)
    low = lax.ppermute(minus[:64], "tp", up_shift)
    high = lax.ppermute(plus[64:], "tp", down_shift)

    near_hidden, modulation = pl.pallas_call(
        hidden_kernel,
        out_shape=(sds((432, D), bf16), pltpu.HBM((2, 3 * D), f32)),
        in_specs=[VM] * 5,
        out_specs=(VM, VM),
        compiler_params=pltpu.CompilerParams(vmem_limit_bytes=16 * 1024 * 1024),
        name="hidden",
    )(*on_chip(own, minus, plus, ride), *off_chip(norm_gain.reshape(1, D)))
    payload, q, k, v, cum = pl.pallas_call(
        project_kernel,
        out_shape=(
            sds((4, PAYLOAD, DK), bf16),
            pltpu.HBM((SEG, DK), bf16),
            pltpu.HBM((SEG, DK), bf16),
            pltpu.HBM((SEG, DK), bf16),
            pltpu.HBM((2, SEG, DK), f32),
        ),
        in_specs=[VM] * 11,
        out_specs=(VM,) * 5,
        scratch_shapes=[
            pltpu.VMEM((144, D), bf16),
            pltpu.VMEM((D, 384), bf16),
            pltpu.VMEM((ROWS, 512), bf16),
        ],
        compiler_params=pltpu.CompilerParams(vmem_limit_bytes=24 * 1024 * 1024),
        name="project",
    )(
        *on_chip(near_hidden), *on_chip(low, high), *off_chip(modulation, norm_gain.reshape(1, D)),
        *on_chip(mine, other), *off_chip(decay_down.T, decay_up, decay_bias), *on_chip(ride),
    )
    got = lax.all_to_all(payload, "A", 0, 0, tiled=True)
    local, lift_f, lift_b = pl.pallas_call(
        local_kernel,
        out_shape=(sds((SEG, DK), f32), sds((SEG, DK), bf16), sds((SEG, DK), bf16)),
        in_specs=[VM] * 4,
        out_specs=(VM,) * 3,
        compiler_params=pltpu.CompilerParams(vmem_limit_bytes=12 * 1024 * 1024),
        name="local",
    )(*off_chip(q, k, v, cum))
    mixed = pl.pallas_call(
        combine_kernel,
        out_shape=sds((SEG, DK), bf16),
        in_specs=[VM] * 4,
        out_specs=VM,
        compiler_params=pltpu.CompilerParams(vmem_limit_bytes=12 * 1024 * 1024),
        name="combine",
    )(*on_chip(got, local, lift_f, lift_b))
    heads = lax.all_to_all(mixed.reshape(4, 128, DK), "B", 0, 0, tiled=True)
    partial = pl.pallas_call(
        output_kernel,
        out_shape=sds((128, D), bf16),
        in_specs=[VM] * 3,
        out_specs=VM,
        compiler_params=pltpu.CompilerParams(vmem_limit_bytes=16 * 1024 * 1024),
        name="output",
    )(*on_chip(heads), *off_chip(head_gain.reshape(1, 256)), *on_chip(out_weight))
    shares = lax.all_to_all(partial.reshape(4, 32, D), "tp", 0, 0, tiled=True)
    projected = shares.astype(f32).sum(axis=0)
    projected = lax.optimization_barrier(projected.astype(bf16)).astype(f32)
    return (latents.astype(f32) + modulation[0:1, 2 * D :] * projected).astype(bf16)


def solution(mesh):
    mesh = Mesh(mesh.devices.reshape(4, 4, 4, 4, 2), ("A", "B", "tp", "x", "core"))
    dp = ("x", "core")
    sp = ("A", "B")
    placed = (
        P((*dp, *sp, "tp"), None),
        P(dp, None),
        P((*dp, *sp), None),
        P(),
        P(),
        P(None, (*sp, "tp")),
        P(sp, "tp"),
        P(sp, "tp"),
        P(sp, "tp"),
        P(),
        P(None, None, "tp"),
        P(None, "tp"),
        P(None, (*dp, *sp), "tp"),
        P(),
        P("tp", None),
    )
    return jax.shard_map(
        device_body,
        mesh=mesh,
        in_specs=placed,
        out_specs=P((*dp, *sp, "tp"), None),
        check_vma=False,
    )
```

```python
import jax
import jax.numpy as jnp
from jax import lax
from jax.experimental import pallas as pl
from jax.experimental.pallas import tpu as pltpu
from jax.sharding import Mesh, PartitionSpec as P


D = 2048
DK = 128
RANK = 32
BLOCK = 64
CTX_LIFT = 4.0
EPS = 1e-06
SHARP = 16.0
SEG = 512
CTX_SEG = 64
ROWS = SEG + CTX_SEG
PAYLOAD = 328
bf16 = jnp.bfloat16
f32 = jnp.float32
VM = pl.BlockSpec(memory_space=pltpu.VMEM)
SM = pl.BlockSpec(memory_space=pltpu.SMEM)


def on_chip(*arrays):
    return tuple(pltpu.with_memory_space_constraint(a, pltpu.VMEM) for a in arrays)


def off_chip(*arrays):
    return tuple(pltpu.with_memory_space_constraint(a, pltpu.HBM) for a in arrays)


def to_everyone(x, axis):
    size = lax.axis_size(axis)
    return lax.all_to_all(jnp.broadcast_to(x[None], (size, *x.shape)), axis, 0, 0, tiled=True)


def three_parts(x):
    hi = x.astype(bf16)
    rest = x - hi.astype(f32)
    mid = rest.astype(bf16)
    lo = (rest - mid.astype(f32)).astype(bf16)
    return hi, mid, lo


def tri(rows, cols, upper):
    r = lax.broadcasted_iota(jnp.int32, (rows, cols), 0)
    c = lax.broadcasted_iota(jnp.int32, (rows, cols), 1)
    return (c >= r) if upper else (c <= r)


def summed_by(mask, a):
    m = mask.astype(f32).astype(bf16)
    stacked = jnp.concatenate(three_parts(a), axis=0)
    return jnp.dot(jnp.concatenate([m, m, m], axis=1), stacked, preferred_element_type=f32)


def nt(a, b):
    return lax.dot_general(a, b, (((1,), (1,)), ((), ())), preferred_element_type=f32)


def tn(a, b):
    return lax.dot_general(a, b, (((0,), (0,)), ((), ())), preferred_element_type=f32)


def rows_kernel(lat_ref, ctx_ref, sv_ref, cv_ref, mod_ref, rows_ref, mods_ref):
    y = lax.axis_index("tp")
    rows_ref[0:32, :] = lat_ref[...]
    ctx = ctx_ref[...].astype(f32)
    picked = ctx[12:16]
    for i in range(3):
        picked = jnp.where(y == i, ctx[4 * i : 4 * i + 4], picked)
    rows_ref[32:36, :] = picked.astype(bf16)
    both = jnp.concatenate([sv_ref[...], cv_ref[...]], axis=0)
    conditions = (both / (1.0 + jnp.exp(-both))).astype(bf16)
    local_mods = nt(conditions, mod_ref[...])
    for i in range(4):
        mods_ref[i] = local_mods


def pack_kernel(mods_ref, wq_ref, wk_ref, wv_ref, extra_ref, cut_ref):
    dp = lax.axis_index("x") * 2 + lax.axis_index("core")
    mods = jnp.concatenate([mods_ref[i] for i in range(4)], axis=1)
    hi, mid, _ = three_parts(mods)
    pieces = [p[:, 128 * j : 128 * (j + 1)].astype(f32) for p in (hi, mid) for j in range(3)]
    e_hi, e_mid, _ = three_parts(extra_ref[...])
    e_hi, e_mid = e_hi.astype(f32), e_mid.astype(f32)
    riding = []
    for h in range(2):
        added = [e_hi[h : h + 1], e_mid[h : h + 1], e_hi[2 + h : 3 + h], e_mid[2 + h : 3 + h]]
        riding.append(jnp.concatenate([*pieces, *added], axis=0).astype(bf16))
    mine = pl.ds(pl.multiple_of(dp * 16, 16), 16)
    for d in range(16):
        b = d % 4
        h = b // 2
        cut_ref[d, :, 0:128] = wq_ref[mine, h * 128 : (h + 1) * 128]
        cut_ref[d, :, 128:256] = wk_ref[mine, h * 128 : (h + 1) * 128]
        cut_ref[d, :, 256:384] = wv_ref[mine, b * 128 : (b + 1) * 128]
        cut_ref[d, :, 384:512] = riding[h]


def normed_rows(rows, which, mod_ref, gain_ref):
    v = rows.astype(f32)
    r = lax.rsqrt(jnp.mean(v * v, axis=-1, keepdims=True) + EPS)
    scale = gain_ref[...] * (1.0 + mod_ref[which : which + 1, D : 2 * D])
    return (v * r * scale + mod_ref[which : which + 1, 0:D]).astype(bf16)


def hidden_kernel(own_ref, minus_ref, plus_ref, ride_ref, gain_ref, h_ref, mod_ref):
    for z in range(16):
        r = ride_ref[z].astype(f32)
        for j in range(3):
            both = r[2 * j : 2 * j + 2] + r[6 + 2 * j : 8 + 2 * j]
            mod_ref[:, (z * 3 + j) * 128 : (z * 3 + j + 1) * 128] = both
    for slot, ref in enumerate((own_ref, minus_ref, plus_ref)):
        for j in range(4):
            at = slot * 144 + j * 32
            h_ref[at : at + 32, :] = normed_rows(ref[j * 32 : j * 32 + 32, :], 0, mod_ref, gain_ref)
        at = slot * 144 + 128
        h_ref[at : at + 16, :] = normed_rows(ref[128:144, :], 1, mod_ref, gain_ref)


def decays_of(low, up_ref, bias_ref):
    second = lax.axis_index("B") >= 2

    def of_head(a):
        return jnp.where(second, a[:, 128:256].astype(f32), a[:, 0:128].astype(f32))

    raw = []
    for z in range(2):
        up = of_head(up_ref[z]).astype(bf16)
        part = jnp.dot(low[:, z * RANK : (z + 1) * RANK], up, preferred_element_type=f32)
        raw.append(part + of_head(bias_ref[z : z + 1, :]))
    raw = jnp.concatenate(raw, axis=1)
    return (jnp.minimum(raw, 0.0) - jnp.log1p(jnp.exp(-jnp.abs(raw)))) * (1.0 / SHARP)


def near_kernel(
    h_ref, mine_ref, other_ref, down_ref, up_ref, bias_ref, w_ref, qkv_ref, logs_ref
):
    core = lax.axis_index("core")
    for xi in range(4):
        for z in range(16):
            at = z * 128 + xi * 32
            here = pl.ds(pl.multiple_of(at + core * 16, 16), 16)
            there = pl.ds(pl.multiple_of(at + 16 - core * 16, 16), 16)
            w_ref[here, :] = mine_ref[xi, z]
            w_ref[there, :] = other_ref[xi, z]
    rows = h_ref[...]
    low = nt(rows, down_ref[...]).astype(bf16)
    logs_ref[...] = decays_of(low, up_ref, bias_ref)
    qkv_ref[...] = jnp.dot(rows, w_ref[...], preferred_element_type=f32).astype(bf16)


def project_kernel(
    low_ref, high_ref, mod_ref, gain_ref, w_ref, qkv_ref, logs_ref,
    down_ref, up_ref, bias_ref, ride_ref,
    pay_ref, q_ref, k_ref, v_ref, cum_ref, far_ref, out_ref, all_logs_ref,
):
    seg, sub = lax.axis_index("A"), lax.axis_index("B")
    y = lax.axis_index("tp")
    for j in range(4):
        rows = (low_ref, high_ref)[j // 2][(j % 2) * 32 : (j % 2) * 32 + 32, :]
        far_ref[j * 32 : j * 32 + 32, :] = normed_rows(rows, 0, mod_ref, gain_ref)
    far_ref[128:144, :] = normed_rows(high_ref[64:80, :], 1, mod_ref, gain_ref)
    y_of = [y, (y + 3) % 4, (y + 1) % 4, (y + 2) % 4]
    rows = far_ref[...]
    low = nt(rows, down_ref[...]).astype(bf16)
    far_logs = decays_of(low, up_ref, bias_ref)
    far_qkv = jnp.dot(rows, w_ref[...], preferred_element_type=f32).astype(bf16)
    for n in range(4):
        for j in range(5):
            size = 32 if j < 4 else 16
            first = n * 144 + j * 32 if n < 3 else j * 32
            took = slice(first, first + size)
            if j < 4:
                at = pl.ds(pl.multiple_of((sub ^ j) * 128 + y_of[n] * 32, 32), size)
            else:
                at = pl.ds(SEG + n * 16, size)
            out_ref[at, :] = qkv_ref[took, :] if n < 3 else far_qkv[took]
            all_logs_ref[at, :] = logs_ref[took, :] if n < 3 else far_logs[took]
    out = out_ref[...]
    logs = all_logs_ref[...]
    q_ref[...] = out[:SEG, 0:128]
    k_ref[...] = out[:SEG, 128:256]
    v_ref[...] = out[:SEG, 256:384]
    ef, eb = [], []
    for zb in range(4):
        t = jnp.transpose(ride_ref[seg * 4 + zb].astype(f32))
        ef.append(t[:, 12:13] + t[:, 13:14])
        eb.append(t[:, 14:15] + t[:, 15:16])
    ef = jnp.concatenate(ef, axis=0)
    eb = jnp.concatenate(eb, axis=0)
    af = logs[:SEG, 0:128] + ef
    ab = logs[:SEG, 128:256] + eb
    low_mask = tri(BLOCK, BLOCK, False)
    up_mask = tri(BLOCK, BLOCK, True)
    wf, wb = [], []
    for n in range(SEG // BLOCK):
        sl = slice(n * BLOCK, (n + 1) * BLOCK)
        wf.append(summed_by(low_mask, af[sl]))
        wb.append(summed_by(up_mask, ab[sl]))
        cum_ref[0, sl, :] = wf[-1]
        cum_ref[1, sl, :] = wb[-1]
    tot_f = [w[BLOCK - 1 : BLOCK] for w in wf]
    tot_b = [w[0:1] for w in wb]
    dev_f = sum(tot_f)
    dev_b = sum(tot_b)
    kk = out[:SEG, 128:256].astype(f32)
    before = jnp.zeros((1, DK), f32)
    kf = []
    for n in range(SEG // BLOCK):
        kf.append(kk[n * BLOCK : (n + 1) * BLOCK] * jnp.exp(dev_f - before - wf[n]))
        before = before + tot_f[n]
    after = jnp.zeros((1, DK), f32)
    kb = [None] * (SEG // BLOCK)
    for n in reversed(range(SEG // BLOCK)):
        kb[n] = kk[n * BLOCK : (n + 1) * BLOCK] * jnp.exp(dev_b - after - wb[n])
        after = after + tot_b[n]
    both = jnp.concatenate(
        [jnp.concatenate(kf, 0).astype(bf16), jnp.concatenate(kb, 0).astype(bf16)], axis=1
    )
    states = tn(out[:SEG, 256:384], both).astype(bf16)

    def order(i):
        slot = i // 16
        step = jnp.where(slot == 0, 0, jnp.where(slot == 1, 3, slot - 1))
        return (((i % 16) // 4) ^ sub) * 16 + ((step + y) % 4) * 4 + i % 4

    r = order(lax.broadcasted_iota(jnp.int32, (CTX_SEG, CTX_SEG), 0))
    c = order(lax.broadcasted_iota(jnp.int32, (CTX_SEG, CTX_SEG), 1))
    later = summed_by(c > r, logs[SEG:, 0:128])
    earlier = summed_by(c < r, logs[SEG:, 128:256])
    ctx_f = jnp.sum(logs[SEG:, 0:128], axis=0, keepdims=True)
    ctx_b = jnp.sum(logs[SEG:, 128:256], axis=0, keepdims=True)
    ck = out[SEG:, 128:256].astype(f32)
    ckf = (ck * jnp.exp(later)).astype(bf16)
    ckb = (ck * jnp.exp(earlier)).astype(bf16)
    cv = out[SEG:, 256:384]
    zero = jnp.zeros((2, DK), bf16)
    for peer in range(4):
        ahead = peer > seg
        pay_ref[peer, 0:128, :] = jnp.where(ahead, states[:, 0:128], states[:, 128:256])
        pay_ref[peer, 128:192, :] = ckf
        pay_ref[peer, 192:256, :] = ckb
        pay_ref[peer, 256:320, :] = cv
        dev = jnp.where(ahead, dev_f, dev_b)
        two = [p for t in (dev, ctx_f, ctx_b) for p in three_parts(t)[:2]]
        pay_ref[peer, 320:328, :] = jnp.concatenate([*two, zero], axis=0)


def local_kernel(q_ref, k_ref, v_ref, cum_ref, o_ref, lift_f_ref, lift_b_ref):
    blocks = SEG // BLOCK
    low_mask = tri(BLOCK, BLOCK, False)
    up_mask = tri(BLOCK, BLOCK, True)
    tot_f = [cum_ref[0, (n + 1) * BLOCK - 1 : (n + 1) * BLOCK, :] for n in range(blocks)]
    tot_b = [cum_ref[1, n * BLOCK : n * BLOCK + 1, :] for n in range(blocks)]
    state = jnp.zeros((DK, DK), f32)
    before = jnp.zeros((1, DK), f32)
    for n in range(blocks):
        sl = slice(n * BLOCK, (n + 1) * BLOCK)
        q = q_ref[sl, :].astype(f32)
        k = k_ref[sl, :].astype(f32)
        v = v_ref[sl, :]
        wf = cum_ref[0, sl, :]
        wb = cum_ref[1, sl, :]
        mf = 0.5 * tot_f[n]
        mb = 0.5 * tot_b[n]
        sf = nt((q * jnp.exp(wf - mf)).astype(bf16), (k * jnp.exp(mf - wf)).astype(bf16))
        sb = nt((q * jnp.exp(wb - mb)).astype(bf16), (k * jnp.exp(mb - wb)).astype(bf16))
        scores = jnp.where(low_mask, sf, 0.0) + jnp.where(up_mask, sb, 0.0)
        out = jnp.dot(scores.astype(bf16), v, preferred_element_type=f32)
        qd = q * jnp.exp(wf)
        lift_f_ref[sl, :] = (qd * jnp.exp(before)).astype(bf16)
        if n > 0:
            out = out + nt(qd.astype(bf16), state.astype(bf16))
        o_ref[sl, :] = out
        if n < blocks - 1:
            state = jnp.exp(tot_f[n]) * state + tn(v, (k * jnp.exp(tot_f[n] - wf)).astype(bf16))
        before = before + tot_f[n]
    state = jnp.zeros((DK, DK), f32)
    after = jnp.zeros((1, DK), f32)
    for n in reversed(range(blocks)):
        sl = slice(n * BLOCK, (n + 1) * BLOCK)
        q = q_ref[sl, :].astype(f32)
        k = k_ref[sl, :].astype(f32)
        v = v_ref[sl, :]
        wb = cum_ref[1, sl, :]
        qd = q * jnp.exp(wb)
        lift_b_ref[sl, :] = (qd * jnp.exp(after)).astype(bf16)
        if n < blocks - 1:
            o_ref[sl, :] = o_ref[sl, :] + nt(qd.astype(bf16), state.astype(bf16))
        if n > 0:
            state = jnp.exp(tot_b[n]) * state + tn(v, (k * jnp.exp(tot_b[n] - wb)).astype(bf16))
        after = after + tot_b[n]


def combine_kernel(in_ref, o_ref, lift_f_ref, lift_b_ref, out_ref):
    seg = lax.axis_index("A")

    def vec(peer, at):
        rows = in_ref[peer, 320:328, :].astype(f32)
        return rows[at : at + 1] + rows[at + 1 : at + 2]

    ctx_f = jnp.zeros((DK, DK), f32)
    ctx_b = jnp.zeros((DK, DK), f32)
    for q in range(4):
        ctx_f = jnp.exp(vec(q, 2)) * ctx_f + tn(in_ref[q, 256:320, :], in_ref[q, 128:192, :])
    for q in reversed(range(4)):
        ctx_b = jnp.exp(vec(q, 4)) * ctx_b + tn(in_ref[q, 256:320, :], in_ref[q, 192:256, :])
    fwd = CTX_LIFT * ctx_f
    for a in range(3):
        moved = jnp.exp(vec(a, 0)) * fwd + in_ref[a, 0:128, :].astype(f32)
        fwd = jnp.where(a < seg, moved, fwd)
    bwd = CTX_LIFT * ctx_b
    for a in (3, 2, 1):
        moved = jnp.exp(vec(a, 0)) * bwd + in_ref[a, 0:128, :].astype(f32)
        bwd = jnp.where(a > seg, moved, bwd)
    out = o_ref[...] + nt(lift_f_ref[...], fwd.astype(bf16)) + nt(lift_b_ref[...], bwd.astype(bf16))
    out_ref[...] = out.astype(bf16)


def output_kernel(mix_ref, gain_ref, w_ref, out_ref):
    total = None
    for h in range(2):
        v = jnp.concatenate([mix_ref[2 * h], mix_ref[2 * h + 1]], axis=1).astype(f32)
        r = lax.rsqrt(jnp.mean(v * v, axis=-1, keepdims=True) + EPS)
        n = (v * r * gain_ref[...]).astype(bf16)
        part = jnp.dot(n, w_ref[h * 256 : (h + 1) * 256, :], preferred_element_type=f32)
        total = part if total is None else total + part
    out_ref[...] = total.astype(bf16)


def device_body(
    latents,
    sample_vector,
    context,
    context_vector,
    norm_gain,
    modulator,
    query_weight,
    key_weight,
    value_weight,
    decay_down,
    decay_up,
    decay_bias,
    decay_extra,
    head_gain,
    out_weight,
):
    sds = jax.ShapeDtypeStruct
    rows, mods = pl.pallas_call(
        rows_kernel,
        out_shape=(sds((36, D), bf16), sds((4, 2, 96), f32)),
        in_specs=[VM] * 5,
        out_specs=(VM, VM),
        compiler_params=pltpu.CompilerParams(vmem_limit_bytes=12 * 1024 * 1024),
        name="rows",
    )(*off_chip(latents, context, sample_vector, context_vector, modulator.T))
    mods = lax.all_to_all(mods, "tp", 0, 0, tiled=True)
    near = [rows]
    for j in range(1, 4):
        near.append(lax.ppermute(rows, "B", [(b, b ^ j) for b in range(4)]))
    cut = pl.pallas_call(
        pack_kernel,
        out_shape=sds((16, 16, 512), bf16),
        in_specs=[VM] * 5,
        out_specs=VM,
        compiler_params=pltpu.CompilerParams(vmem_limit_bytes=12 * 1024 * 1024),
        name="pack",
    )(
        *on_chip(mods),
        *off_chip(
            query_weight, key_weight, value_weight,
            jnp.moveaxis(decay_extra, 1, 2).reshape(4, 128),
        ),
    )
    rows_z = lax.all_to_all(cut, ("A", "B"), 0, 0, tiled=True)
    mine = to_everyone(rows_z[:, :, 0:384], "x")
    other = lax.ppermute(mine, "core", [(0, 1), (1, 0)])
    ride = rows_z[:, :, 384:512]

    own = jnp.concatenate([n[:32] for n in near] + [n[32:36] for n in near], axis=0)
    up_shift = [(i, (i + 1) % 4) for i in range(4)]
    down_shift = [(i, (i + 3) % 4) for i in range(4)]
    minus = lax.ppermute(own, "tp", up_shift)
    plus = lax.ppermute(own, "tp", down_shift)
    low = lax.ppermute(minus[:64], "tp", up_shift)
    high = lax.ppermute(plus[64:], "tp", down_shift)

    near_hidden, modulation = pl.pallas_call(
        hidden_kernel,
        out_shape=(sds((432, D), bf16), pltpu.HBM((2, 3 * D), f32)),
        in_specs=[VM] * 5,
        out_specs=(VM, VM),
        compiler_params=pltpu.CompilerParams(vmem_limit_bytes=16 * 1024 * 1024),
        name="hidden",
    )(*on_chip(own, minus, plus, ride), *off_chip(norm_gain.reshape(1, D)))
    weights, near_qkv, near_logs = pl.pallas_call(
        near_kernel,
        out_shape=(sds((D, 384), bf16), sds((432, 384), bf16), sds((432, 256), f32)),
        in_specs=[VM] * 6,
        out_specs=(VM,) * 3,
        compiler_params=pltpu.CompilerParams(vmem_limit_bytes=16 * 1024 * 1024),
        name="near",
    )(*on_chip(near_hidden, mine, other), *off_chip(decay_down.T, decay_up, decay_bias))
    payload, q, k, v, cum = pl.pallas_call(
        project_kernel,
        out_shape=(
            sds((4, PAYLOAD, DK), bf16),
            pltpu.HBM((SEG, DK), bf16),
            pltpu.HBM((SEG, DK), bf16),
            pltpu.HBM((SEG, DK), bf16),
            pltpu.HBM((2, SEG, DK), f32),
        ),
        in_specs=[VM] * 11,
        out_specs=(VM,) * 5,
        scratch_shapes=[
            pltpu.VMEM((144, D), bf16),
            pltpu.VMEM((ROWS, 384), bf16),
            pltpu.VMEM((ROWS, 256), f32),
        ],
        compiler_params=pltpu.CompilerParams(vmem_limit_bytes=20 * 1024 * 1024),
        name="project",
    )(
        *on_chip(low, high), *off_chip(modulation, norm_gain.reshape(1, D)),
        *on_chip(weights, near_qkv, near_logs),
        *off_chip(decay_down.T, decay_up, decay_bias), *on_chip(ride),
    )
    got = lax.all_to_all(payload, "A", 0, 0, tiled=True)
    local, lift_f, lift_b = pl.pallas_call(
        local_kernel,
        out_shape=(sds((SEG, DK), f32), sds((SEG, DK), bf16), sds((SEG, DK), bf16)),
        in_specs=[VM] * 4,
        out_specs=(VM,) * 3,
        compiler_params=pltpu.CompilerParams(vmem_limit_bytes=12 * 1024 * 1024),
        name="local",
    )(*off_chip(q, k, v, cum))
    mixed = pl.pallas_call(
        combine_kernel,
        out_shape=sds((SEG, DK), bf16),
        in_specs=[VM] * 4,
        out_specs=VM,
        compiler_params=pltpu.CompilerParams(vmem_limit_bytes=12 * 1024 * 1024),
        name="combine",
    )(*on_chip(got, local, lift_f, lift_b))
    heads = lax.all_to_all(mixed.reshape(4, 128, DK), "B", 0, 0, tiled=True)
    partial = pl.pallas_call(
        output_kernel,
        out_shape=sds((128, D), bf16),
        in_specs=[VM] * 3,
        out_specs=VM,
        compiler_params=pltpu.CompilerParams(vmem_limit_bytes=16 * 1024 * 1024),
        name="output",
    )(*on_chip(heads), *off_chip(head_gain.reshape(1, 256)), *on_chip(out_weight))
    shares = lax.all_to_all(partial.reshape(4, 32, D), "tp", 0, 0, tiled=True)
    projected = shares.astype(f32).sum(axis=0)
    projected = lax.optimization_barrier(projected.astype(bf16)).astype(f32)
    return (latents.astype(f32) + modulation[0:1, 2 * D :] * projected).astype(bf16)


def solution(mesh):
    mesh = Mesh(mesh.devices.reshape(4, 4, 4, 4, 2), ("A", "B", "tp", "x", "core"))
    dp = ("x", "core")
    sp = ("A", "B")
    placed = (
        P((*dp, *sp, "tp"), None),
        P(dp, None),
        P((*dp, *sp), None),
        P(),
        P(),
        P(None, (*sp, "tp")),
        P(sp, "tp"),
        P(sp, "tp"),
        P(sp, "tp"),
        P(),
        P(None, None, "tp"),
        P(None, "tp"),
        P(None, (*dp, *sp), "tp"),
        P(),
        P("tp", None),
    )
    return jax.shard_map(
        device_body,
        mesh=mesh,
        in_specs=placed,
        out_specs=P((*dp, *sp, "tp"), None),
        check_vma=False,
    )
```

```python
import jax
import jax.numpy as jnp
from jax import lax
from jax.experimental import pallas as pl
from jax.experimental.pallas import tpu as pltpu
from jax.sharding import Mesh, PartitionSpec as P


D = 2048
DK = 128
RANK = 32
BLOCK = 64
CTX_LIFT = 4.0
EPS = 1e-06
SHARP = 16.0
SEG = 512
CTX_SEG = 64
ROWS = SEG + CTX_SEG
PAYLOAD = 328
bf16 = jnp.bfloat16
f32 = jnp.float32
VM = pl.BlockSpec(memory_space=pltpu.VMEM)
SM = pl.BlockSpec(memory_space=pltpu.SMEM)


def on_chip(*arrays):
    return tuple(pltpu.with_memory_space_constraint(a, pltpu.VMEM) for a in arrays)


def off_chip(*arrays):
    return tuple(pltpu.with_memory_space_constraint(a, pltpu.HBM) for a in arrays)


def to_everyone(x, axis):
    size = lax.axis_size(axis)
    return lax.all_to_all(jnp.broadcast_to(x[None], (size, *x.shape)), axis, 0, 0, tiled=True)


def role(seg, sub):
    return sub ^ (seg // 2)


PEERS = [[4 * a + role(a, b) for a in range(4)] for b in range(4)]


def three_parts(x):
    hi = x.astype(bf16)
    rest = x - hi.astype(f32)
    mid = rest.astype(bf16)
    lo = (rest - mid.astype(f32)).astype(bf16)
    return hi, mid, lo


def tri(rows, cols, upper):
    r = lax.broadcasted_iota(jnp.int32, (rows, cols), 0)
    c = lax.broadcasted_iota(jnp.int32, (rows, cols), 1)
    return (c >= r) if upper else (c <= r)


def summed_by(mask, a):
    m = mask.astype(f32).astype(bf16)
    stacked = jnp.concatenate(three_parts(a), axis=0)
    return jnp.dot(jnp.concatenate([m, m, m], axis=1), stacked, preferred_element_type=f32)


def nt(a, b):
    return lax.dot_general(a, b, (((1,), (1,)), ((), ())), preferred_element_type=f32)


def tn(a, b):
    return lax.dot_general(a, b, (((0,), (0,)), ((), ())), preferred_element_type=f32)


def rows_kernel(lat_ref, ctx_ref, sv_ref, cv_ref, mod_ref, rows_ref, mods_ref):
    y = lax.axis_index("tp")
    rows_ref[0:32, :] = lat_ref[...]
    ctx = ctx_ref[...].astype(f32)
    picked = ctx[12:16]
    for i in range(3):
        picked = jnp.where(y == i, ctx[4 * i : 4 * i + 4], picked)
    rows_ref[32:36, :] = picked.astype(bf16)
    both = jnp.concatenate([sv_ref[...], cv_ref[...]], axis=0)
    conditions = (both / (1.0 + jnp.exp(-both))).astype(bf16)
    local_mods = nt(conditions, mod_ref[...])
    for i in range(4):
        mods_ref[i] = local_mods


def pack_kernel(mods_ref, wq_ref, wk_ref, wv_ref, extra_ref, cut_ref):
    dp = lax.axis_index("x") * 2 + lax.axis_index("core")
    mods = jnp.concatenate([mods_ref[i] for i in range(4)], axis=1)
    hi, mid, _ = three_parts(mods)
    pieces = [p[:, 128 * j : 128 * (j + 1)].astype(f32) for p in (hi, mid) for j in range(3)]
    e_hi, e_mid, _ = three_parts(extra_ref[...])
    e_hi, e_mid = e_hi.astype(f32), e_mid.astype(f32)
    riding = []
    for h in range(2):
        added = [e_hi[h : h + 1], e_mid[h : h + 1], e_hi[2 + h : 3 + h], e_mid[2 + h : 3 + h]]
        riding.append(jnp.concatenate([*pieces, *added], axis=0).astype(bf16))
    mine = pl.ds(pl.multiple_of(dp * 16, 16), 16)
    for d in range(16):
        b = role(d // 4, d % 4)
        h = b // 2
        cut_ref[d, :, 0:128] = wq_ref[mine, h * 128 : (h + 1) * 128]
        cut_ref[d, :, 128:256] = wk_ref[mine, h * 128 : (h + 1) * 128]
        cut_ref[d, :, 256:384] = wv_ref[mine, b * 128 : (b + 1) * 128]
        cut_ref[d, :, 384:512] = riding[h]


def normed_rows(rows, which, mod_ref, gain_ref):
    v = rows.astype(f32)
    r = lax.rsqrt(jnp.mean(v * v, axis=-1, keepdims=True) + EPS)
    scale = gain_ref[...] * (1.0 + mod_ref[which : which + 1, D : 2 * D])
    return (v * r * scale + mod_ref[which : which + 1, 0:D]).astype(bf16)


def hidden_kernel(own_ref, minus_ref, plus_ref, ride_ref, gain_ref, h_ref, mod_ref):
    for z in range(16):
        r = ride_ref[z].astype(f32)
        for j in range(3):
            both = r[2 * j : 2 * j + 2] + r[6 + 2 * j : 8 + 2 * j]
            mod_ref[:, (z * 3 + j) * 128 : (z * 3 + j + 1) * 128] = both
    for slot, ref in enumerate((own_ref, minus_ref, plus_ref)):
        for j in range(4):
            at = slot * 144 + j * 32
            h_ref[at : at + 32, :] = normed_rows(ref[j * 32 : j * 32 + 32, :], 0, mod_ref, gain_ref)
        at = slot * 144 + 128
        h_ref[at : at + 16, :] = normed_rows(ref[128:144, :], 1, mod_ref, gain_ref)


def decays_of(low, up_ref, bias_ref):
    second = lax.axis_index("B") >= 2

    def of_head(a):
        return jnp.where(second, a[:, 128:256].astype(f32), a[:, 0:128].astype(f32))

    raw = []
    for z in range(2):
        up = of_head(up_ref[z]).astype(bf16)
        part = jnp.dot(low[:, z * RANK : (z + 1) * RANK], up, preferred_element_type=f32)
        raw.append(part + of_head(bias_ref[z : z + 1, :]))
    raw = jnp.concatenate(raw, axis=1)
    return (jnp.minimum(raw, 0.0) - jnp.log1p(jnp.exp(-jnp.abs(raw)))) * (1.0 / SHARP)


def near_kernel(
    h_ref, mine_ref, other_ref, down_ref, up_ref, bias_ref, w_ref, qkv_ref, logs_ref
):
    core = lax.axis_index("core")
    for xi in range(4):
        for z in range(16):
            at = z * 128 + xi * 32
            here = pl.ds(pl.multiple_of(at + core * 16, 16), 16)
            there = pl.ds(pl.multiple_of(at + 16 - core * 16, 16), 16)
            w_ref[here, :] = mine_ref[xi, z]
            w_ref[there, :] = other_ref[xi, z]
    rows = h_ref[...]
    low = nt(rows, down_ref[...]).astype(bf16)
    logs_ref[...] = decays_of(low, up_ref, bias_ref)
    qkv_ref[...] = jnp.dot(rows, w_ref[...], preferred_element_type=f32).astype(bf16)


def project_kernel(
    low_ref, high_ref, mod_ref, gain_ref, w_ref, qkv_ref, logs_ref,
    down_ref, up_ref, bias_ref, ride_ref,
    pay_ref, q_ref, k_ref, v_ref, cum_ref, far_ref, out_ref, all_logs_ref,
):
    seg, sub = lax.axis_index("A"), lax.axis_index("B")
    y = lax.axis_index("tp")
    for j in range(4):
        rows = (low_ref, high_ref)[j // 2][(j % 2) * 32 : (j % 2) * 32 + 32, :]
        far_ref[j * 32 : j * 32 + 32, :] = normed_rows(rows, 0, mod_ref, gain_ref)
    far_ref[128:144, :] = normed_rows(high_ref[64:80, :], 1, mod_ref, gain_ref)
    y_of = [y, (y + 3) % 4, (y + 1) % 4, (y + 2) % 4]
    rows = far_ref[...]
    low = nt(rows, down_ref[...]).astype(bf16)
    far_logs = decays_of(low, up_ref, bias_ref)
    far_qkv = jnp.dot(rows, w_ref[...], preferred_element_type=f32).astype(bf16)
    for n in range(4):
        for j in range(5):
            size = 32 if j < 4 else 16
            first = n * 144 + j * 32 if n < 3 else j * 32
            took = slice(first, first + size)
            if j < 4:
                at = pl.ds(pl.multiple_of((sub ^ j) * 128 + y_of[n] * 32, 32), size)
            else:
                at = pl.ds(SEG + n * 16, size)
            out_ref[at, :] = qkv_ref[took, :] if n < 3 else far_qkv[took]
            all_logs_ref[at, :] = logs_ref[took, :] if n < 3 else far_logs[took]
    out = out_ref[...]
    logs = all_logs_ref[...]
    q_ref[...] = out[:SEG, 0:128]
    k_ref[...] = out[:SEG, 128:256]
    v_ref[...] = out[:SEG, 256:384]
    ef, eb = [], []
    for zb in range(4):
        t = jnp.transpose(ride_ref[seg * 4 + zb].astype(f32))
        ef.append(t[:, 12:13] + t[:, 13:14])
        eb.append(t[:, 14:15] + t[:, 15:16])
    ef = jnp.concatenate(ef, axis=0)
    eb = jnp.concatenate(eb, axis=0)
    af = logs[:SEG, 0:128] + ef
    ab = logs[:SEG, 128:256] + eb
    low_mask = tri(BLOCK, BLOCK, False)
    up_mask = tri(BLOCK, BLOCK, True)
    wf, wb = [], []
    for n in range(SEG // BLOCK):
        sl = slice(n * BLOCK, (n + 1) * BLOCK)
        wf.append(summed_by(low_mask, af[sl]))
        wb.append(summed_by(up_mask, ab[sl]))
        cum_ref[0, sl, :] = wf[-1]
        cum_ref[1, sl, :] = wb[-1]
    tot_f = [w[BLOCK - 1 : BLOCK] for w in wf]
    tot_b = [w[0:1] for w in wb]
    dev_f = sum(tot_f)
    dev_b = sum(tot_b)
    kk = out[:SEG, 128:256].astype(f32)
    before = jnp.zeros((1, DK), f32)
    kf = []
    for n in range(SEG // BLOCK):
        kf.append(kk[n * BLOCK : (n + 1) * BLOCK] * jnp.exp(dev_f - before - wf[n]))
        before = before + tot_f[n]
    after = jnp.zeros((1, DK), f32)
    kb = [None] * (SEG // BLOCK)
    for n in reversed(range(SEG // BLOCK)):
        kb[n] = kk[n * BLOCK : (n + 1) * BLOCK] * jnp.exp(dev_b - after - wb[n])
        after = after + tot_b[n]
    both = jnp.concatenate(
        [jnp.concatenate(kf, 0).astype(bf16), jnp.concatenate(kb, 0).astype(bf16)], axis=1
    )
    states = tn(out[:SEG, 256:384], both).astype(bf16)

    def order(i):
        slot = i // 16
        step = jnp.where(slot == 0, 0, jnp.where(slot == 1, 3, slot - 1))
        return (((i % 16) // 4) ^ sub) * 16 + ((step + y) % 4) * 4 + i % 4

    r = order(lax.broadcasted_iota(jnp.int32, (CTX_SEG, CTX_SEG), 0))
    c = order(lax.broadcasted_iota(jnp.int32, (CTX_SEG, CTX_SEG), 1))
    later = summed_by(c > r, logs[SEG:, 0:128])
    earlier = summed_by(c < r, logs[SEG:, 128:256])
    ctx_f = jnp.sum(logs[SEG:, 0:128], axis=0, keepdims=True)
    ctx_b = jnp.sum(logs[SEG:, 128:256], axis=0, keepdims=True)
    ck = out[SEG:, 128:256].astype(f32)
    ckf = (ck * jnp.exp(later)).astype(bf16)
    ckb = (ck * jnp.exp(earlier)).astype(bf16)
    cv = out[SEG:, 256:384]
    zero = jnp.zeros((2, DK), bf16)
    for peer in range(4):
        ahead = peer > seg
        pay_ref[peer, 0:128, :] = jnp.where(ahead, states[:, 0:128], states[:, 128:256])
        pay_ref[peer, 128:192, :] = ckf
        pay_ref[peer, 192:256, :] = ckb
        pay_ref[peer, 256:320, :] = cv
        dev = jnp.where(ahead, dev_f, dev_b)
        two = [p for t in (dev, ctx_f, ctx_b) for p in three_parts(t)[:2]]
        pay_ref[peer, 320:328, :] = jnp.concatenate([*two, zero], axis=0)


def local_kernel(q_ref, k_ref, v_ref, cum_ref, o_ref, lift_f_ref, lift_b_ref):
    blocks = SEG // BLOCK
    low_mask = tri(BLOCK, BLOCK, False)
    up_mask = tri(BLOCK, BLOCK, True)
    tot_f = [cum_ref[0, (n + 1) * BLOCK - 1 : (n + 1) * BLOCK, :] for n in range(blocks)]
    tot_b = [cum_ref[1, n * BLOCK : n * BLOCK + 1, :] for n in range(blocks)]
    state = jnp.zeros((DK, DK), f32)
    before = jnp.zeros((1, DK), f32)
    for n in range(blocks):
        sl = slice(n * BLOCK, (n + 1) * BLOCK)
        q = q_ref[sl, :].astype(f32)
        k = k_ref[sl, :].astype(f32)
        v = v_ref[sl, :]
        wf = cum_ref[0, sl, :]
        wb = cum_ref[1, sl, :]
        mf = 0.5 * tot_f[n]
        mb = 0.5 * tot_b[n]
        sf = nt((q * jnp.exp(wf - mf)).astype(bf16), (k * jnp.exp(mf - wf)).astype(bf16))
        sb = nt((q * jnp.exp(wb - mb)).astype(bf16), (k * jnp.exp(mb - wb)).astype(bf16))
        scores = jnp.where(low_mask, sf, 0.0) + jnp.where(up_mask, sb, 0.0)
        out = jnp.dot(scores.astype(bf16), v, preferred_element_type=f32)
        qd = q * jnp.exp(wf)
        lift_f_ref[sl, :] = (qd * jnp.exp(before)).astype(bf16)
        if n > 0:
            out = out + nt(qd.astype(bf16), state.astype(bf16))
        o_ref[sl, :] = out
        if n < blocks - 1:
            state = jnp.exp(tot_f[n]) * state + tn(v, (k * jnp.exp(tot_f[n] - wf)).astype(bf16))
        before = before + tot_f[n]
    state = jnp.zeros((DK, DK), f32)
    after = jnp.zeros((1, DK), f32)
    for n in reversed(range(blocks)):
        sl = slice(n * BLOCK, (n + 1) * BLOCK)
        q = q_ref[sl, :].astype(f32)
        k = k_ref[sl, :].astype(f32)
        v = v_ref[sl, :]
        wb = cum_ref[1, sl, :]
        qd = q * jnp.exp(wb)
        lift_b_ref[sl, :] = (qd * jnp.exp(after)).astype(bf16)
        if n < blocks - 1:
            o_ref[sl, :] = o_ref[sl, :] + nt(qd.astype(bf16), state.astype(bf16))
        if n > 0:
            state = jnp.exp(tot_b[n]) * state + tn(v, (k * jnp.exp(tot_b[n] - wb)).astype(bf16))
        after = after + tot_b[n]


def combine_kernel(in_ref, o_ref, lift_f_ref, lift_b_ref, out_ref):
    seg = lax.axis_index("A")

    def vec(peer, at):
        rows = in_ref[peer, 320:328, :].astype(f32)
        return rows[at : at + 1] + rows[at + 1 : at + 2]

    ctx_f = jnp.zeros((DK, DK), f32)
    ctx_b = jnp.zeros((DK, DK), f32)
    for q in range(4):
        ctx_f = jnp.exp(vec(q, 2)) * ctx_f + tn(in_ref[q, 256:320, :], in_ref[q, 128:192, :])
    for q in reversed(range(4)):
        ctx_b = jnp.exp(vec(q, 4)) * ctx_b + tn(in_ref[q, 256:320, :], in_ref[q, 192:256, :])
    fwd = CTX_LIFT * ctx_f
    for a in range(3):
        moved = jnp.exp(vec(a, 0)) * fwd + in_ref[a, 0:128, :].astype(f32)
        fwd = jnp.where(a < seg, moved, fwd)
    bwd = CTX_LIFT * ctx_b
    for a in (3, 2, 1):
        moved = jnp.exp(vec(a, 0)) * bwd + in_ref[a, 0:128, :].astype(f32)
        bwd = jnp.where(a > seg, moved, bwd)
    out = o_ref[...] + nt(lift_f_ref[...], fwd.astype(bf16)) + nt(lift_b_ref[...], bwd.astype(bf16))
    out_ref[...] = out.astype(bf16)


def output_kernel(mix_ref, gain_ref, w_ref, out_ref):
    total = None
    flip = lax.axis_index("A") // 2
    for h in range(2):
        v = jnp.concatenate([mix_ref[2 * h + flip], mix_ref[2 * h + 1 - flip]], axis=1).astype(f32)
        r = lax.rsqrt(jnp.mean(v * v, axis=-1, keepdims=True) + EPS)
        n = (v * r * gain_ref[...]).astype(bf16)
        part = jnp.dot(n, w_ref[h * 256 : (h + 1) * 256, :], preferred_element_type=f32)
        total = part if total is None else total + part
    out_ref[...] = total.astype(bf16)


def device_body(
    latents,
    sample_vector,
    context,
    context_vector,
    norm_gain,
    modulator,
    query_weight,
    key_weight,
    value_weight,
    decay_down,
    decay_up,
    decay_bias,
    decay_extra,
    head_gain,
    out_weight,
):
    sds = jax.ShapeDtypeStruct
    rows, mods = pl.pallas_call(
        rows_kernel,
        out_shape=(sds((36, D), bf16), sds((4, 2, 96), f32)),
        in_specs=[VM] * 5,
        out_specs=(VM, VM),
        compiler_params=pltpu.CompilerParams(vmem_limit_bytes=12 * 1024 * 1024),
        name="rows",
    )(*off_chip(latents, context, sample_vector, context_vector, modulator.T))
    mods = lax.all_to_all(mods, "tp", 0, 0, tiled=True)
    near = [rows]
    for j in range(1, 4):
        near.append(lax.ppermute(rows, "B", [(b, b ^ j) for b in range(4)]))
    cut = pl.pallas_call(
        pack_kernel,
        out_shape=sds((16, 16, 512), bf16),
        in_specs=[VM] * 5,
        out_specs=VM,
        compiler_params=pltpu.CompilerParams(vmem_limit_bytes=12 * 1024 * 1024),
        name="pack",
    )(
        *on_chip(mods),
        *off_chip(
            query_weight, key_weight, value_weight,
            jnp.moveaxis(decay_extra, 1, 2).reshape(4, 128),
        ),
    )
    rows_z = lax.all_to_all(cut, ("A", "B"), 0, 0, tiled=True)
    mine = to_everyone(rows_z[:, :, 0:384], "x")
    other = lax.ppermute(mine, "core", [(0, 1), (1, 0)])
    ride = rows_z[:, :, 384:512]

    own = jnp.concatenate([n[:32] for n in near] + [n[32:36] for n in near], axis=0)
    up_shift = [(i, (i + 1) % 4) for i in range(4)]
    down_shift = [(i, (i + 3) % 4) for i in range(4)]
    minus = lax.ppermute(own, "tp", up_shift)
    plus = lax.ppermute(own, "tp", down_shift)
    low = lax.ppermute(minus[:64], "tp", up_shift)
    high = lax.ppermute(plus[64:], "tp", down_shift)

    near_hidden, modulation = pl.pallas_call(
        hidden_kernel,
        out_shape=(sds((432, D), bf16), pltpu.HBM((2, 3 * D), f32)),
        in_specs=[VM] * 5,
        out_specs=(VM, VM),
        compiler_params=pltpu.CompilerParams(vmem_limit_bytes=16 * 1024 * 1024),
        name="hidden",
    )(*on_chip(own, minus, plus, ride), *off_chip(norm_gain.reshape(1, D)))
    weights, near_qkv, near_logs = pl.pallas_call(
        near_kernel,
        out_shape=(sds((D, 384), bf16), sds((432, 384), bf16), sds((432, 256), f32)),
        in_specs=[VM] * 6,
        out_specs=(VM,) * 3,
        compiler_params=pltpu.CompilerParams(vmem_limit_bytes=16 * 1024 * 1024),
        name="near",
    )(*on_chip(near_hidden, mine, other), *off_chip(decay_down.T, decay_up, decay_bias))
    payload, q, k, v, cum = pl.pallas_call(
        project_kernel,
        out_shape=(
            sds((4, PAYLOAD, DK), bf16),
            pltpu.HBM((SEG, DK), bf16),
            pltpu.HBM((SEG, DK), bf16),
            pltpu.HBM((SEG, DK), bf16),
            pltpu.HBM((2, SEG, DK), f32),
        ),
        in_specs=[VM] * 11,
        out_specs=(VM,) * 5,
        scratch_shapes=[
            pltpu.VMEM((144, D), bf16),
            pltpu.VMEM((ROWS, 384), bf16),
            pltpu.VMEM((ROWS, 256), f32),
        ],
        compiler_params=pltpu.CompilerParams(vmem_limit_bytes=20 * 1024 * 1024),
        name="project",
    )(
        *on_chip(low, high), *off_chip(modulation, norm_gain.reshape(1, D)),
        *on_chip(weights, near_qkv, near_logs),
        *off_chip(decay_down.T, decay_up, decay_bias), *on_chip(ride),
    )
    got = lax.all_to_all(
        payload, ("A", "B"), 0, 0, tiled=True, axis_index_groups=PEERS
    )
    local, lift_f, lift_b = pl.pallas_call(
        local_kernel,
        out_shape=(sds((SEG, DK), f32), sds((SEG, DK), bf16), sds((SEG, DK), bf16)),
        in_specs=[VM] * 4,
        out_specs=(VM,) * 3,
        compiler_params=pltpu.CompilerParams(vmem_limit_bytes=12 * 1024 * 1024),
        name="local",
    )(*off_chip(q, k, v, cum))
    mixed = pl.pallas_call(
        combine_kernel,
        out_shape=sds((SEG, DK), bf16),
        in_specs=[VM] * 4,
        out_specs=VM,
        compiler_params=pltpu.CompilerParams(vmem_limit_bytes=12 * 1024 * 1024),
        name="combine",
    )(*on_chip(got, local, lift_f, lift_b))
    heads = lax.all_to_all(mixed.reshape(4, 128, DK), "B", 0, 0, tiled=True)
    partial = pl.pallas_call(
        output_kernel,
        out_shape=sds((128, D), bf16),
        in_specs=[VM] * 3,
        out_specs=VM,
        compiler_params=pltpu.CompilerParams(vmem_limit_bytes=16 * 1024 * 1024),
        name="output",
    )(*on_chip(heads), *off_chip(head_gain.reshape(1, 256)), *on_chip(out_weight))
    shares = lax.all_to_all(partial.reshape(4, 32, D), "tp", 0, 0, tiled=True)
    projected = shares.astype(f32).sum(axis=0)
    projected = lax.optimization_barrier(projected.astype(bf16)).astype(f32)
    return (latents.astype(f32) + modulation[0:1, 2 * D :] * projected).astype(bf16)


def solution(mesh):
    mesh = Mesh(mesh.devices.reshape(4, 4, 4, 4, 2), ("A", "B", "tp", "x", "core"))
    dp = ("x", "core")
    sp = ("A", "B")
    placed = (
        P((*dp, *sp, "tp"), None),
        P(dp, None),
        P((*dp, *sp), None),
        P(),
        P(),
        P(None, (*sp, "tp")),
        P(sp, "tp"),
        P(sp, "tp"),
        P(sp, "tp"),
        P(),
        P(None, None, "tp"),
        P(None, "tp"),
        P(None, (*dp, *sp), "tp"),
        P(),
        P("tp", None),
    )
    return jax.shard_map(
        device_body,
        mesh=mesh,
        in_specs=placed,
        out_specs=P((*dp, *sp, "tp"), None),
        check_vma=False,
    )
```

```python
import jax
import jax.numpy as jnp
from jax import lax
from jax.experimental import pallas as pl
from jax.experimental.pallas import tpu as pltpu
from jax.sharding import Mesh, PartitionSpec as P


D = 2048
DK = 128
RANK = 32
BLOCK = 64
CTX_LIFT = 4.0
EPS = 1e-06
SHARP = 16.0
SEG = 512
CTX_SEG = 64
ROWS = SEG + CTX_SEG
PAYLOAD = 328
bf16 = jnp.bfloat16
f32 = jnp.float32
VM = pl.BlockSpec(memory_space=pltpu.VMEM)
SM = pl.BlockSpec(memory_space=pltpu.SMEM)


def on_chip(*arrays):
    return tuple(pltpu.with_memory_space_constraint(a, pltpu.VMEM) for a in arrays)


def off_chip(*arrays):
    return tuple(pltpu.with_memory_space_constraint(a, pltpu.HBM) for a in arrays)


def to_everyone(x, axis):
    size = lax.axis_size(axis)
    return lax.all_to_all(jnp.broadcast_to(x[None], (size, *x.shape)), axis, 0, 0, tiled=True)


def role(seg, sub):
    return sub ^ (seg // 2 * 2)


PEERS = [[4 * a + role(a, b) for a in range(4)] for b in range(4)]


def three_parts(x):
    hi = x.astype(bf16)
    rest = x - hi.astype(f32)
    mid = rest.astype(bf16)
    lo = (rest - mid.astype(f32)).astype(bf16)
    return hi, mid, lo


def tri(rows, cols, upper):
    r = lax.broadcasted_iota(jnp.int32, (rows, cols), 0)
    c = lax.broadcasted_iota(jnp.int32, (rows, cols), 1)
    return (c >= r) if upper else (c <= r)


def summed_by(mask, a):
    m = mask.astype(f32).astype(bf16)
    stacked = jnp.concatenate(three_parts(a), axis=0)
    return jnp.dot(jnp.concatenate([m, m, m], axis=1), stacked, preferred_element_type=f32)


def nt(a, b):
    return lax.dot_general(a, b, (((1,), (1,)), ((), ())), preferred_element_type=f32)


def tn(a, b):
    return lax.dot_general(a, b, (((0,), (0,)), ((), ())), preferred_element_type=f32)


def pack_kernel(
    lat_ref, ctx_ref, sv_ref, cv_ref, mod_ref, wq_ref, wk_ref, wv_ref, extra_ref, rows_ref, cut_ref
):
    y = lax.axis_index("tp")
    dp = lax.axis_index("x") * 2 + lax.axis_index("core")
    rows_ref[0:32, :] = lat_ref[...]
    ctx = ctx_ref[...].astype(f32)
    picked = ctx[12:16]
    for i in range(3):
        picked = jnp.where(y == i, ctx[4 * i : 4 * i + 4], picked)
    rows_ref[32:36, :] = picked.astype(bf16)

    both = jnp.concatenate([sv_ref[...], cv_ref[...]], axis=0)
    conditions = (both / (1.0 + jnp.exp(-both))).astype(bf16)
    local_mods = nt(conditions, mod_ref[...])
    mods = jnp.concatenate([p.astype(f32) for p in three_parts(local_mods)[:2]], axis=0)
    mods = jnp.concatenate([mods, jnp.zeros((4, 32), f32)], axis=1)
    e_hi, e_mid, _ = three_parts(extra_ref[...])
    e_hi, e_mid = e_hi.astype(f32), e_mid.astype(f32)
    riding = []
    for h in range(2):
        added = [e_hi[h : h + 1], e_mid[h : h + 1], e_hi[2 + h : 3 + h], e_mid[2 + h : 3 + h]]
        riding.append(jnp.concatenate([mods, *added], axis=0).astype(bf16))
    mine = pl.ds(pl.multiple_of(dp * 16, 16), 16)
    for d in range(16):
        b = role(d // 4, d % 4)
        h = b // 2
        cut_ref[d, 0:16, :] = wq_ref[mine, h * 128 : (h + 1) * 128]
        cut_ref[d, 16:32, :] = wk_ref[mine, h * 128 : (h + 1) * 128]
        cut_ref[d, 32:48, :] = wv_ref[mine, b * 128 : (b + 1) * 128]
        cut_ref[d, 48:56, :] = riding[h]


def normed_rows(rows, which, mod_ref, gain_ref):
    v = rows.astype(f32)
    r = lax.rsqrt(jnp.mean(v * v, axis=-1, keepdims=True) + EPS)
    scale = gain_ref[...] * (1.0 + mod_ref[which : which + 1, D : 2 * D])
    return (v * r * scale + mod_ref[which : which + 1, 0:D]).astype(bf16)


def hidden_kernel(
    own_ref, minus_ref, plus_ref, low_ref, high_ref, own_mods_ref, far_mods_ref, gain_ref,
    h_ref, mod_ref, mods_ref,
):
    y = lax.axis_index("tp")
    mods_ref[y] = own_mods_ref[...].astype(f32)
    mods_ref[(y + 3) % 4] = low_ref[64:72, :].astype(f32)
    mods_ref[(y + 1) % 4] = high_ref[80:88, :].astype(f32)
    mods_ref[(y + 2) % 4] = far_mods_ref[...].astype(f32)
    for z in range(16):
        at = slice(z * 128, z * 128 + 96)
        parts = [mods_ref[i, 0:2, at] + mods_ref[i, 2:4, at] for i in range(4)]
        mod_ref[:, z * 384 : (z + 1) * 384] = jnp.concatenate(parts, axis=1)
    for slot in range(4):
        for j in range(5):
            size = 32 if j < 4 else 16
            if slot < 3:
                rows = (own_ref, minus_ref, plus_ref)[slot][j * 32 : j * 32 + size, :]
            elif j < 2:
                rows = low_ref[j * 32 : j * 32 + 32, :]
            else:
                rows = high_ref[j * 32 - 64 : j * 32 - 64 + size, :]
            at = slot * 144 + j * 32
            h_ref[at : at + size, :] = normed_rows(rows, j // 4, mod_ref, gain_ref)


def decays_of(low, up_ref, bias_ref):
    second = role(lax.axis_index("A"), lax.axis_index("B")) >= 2

    def of_head(a):
        return jnp.where(second, a[:, 128:256].astype(f32), a[:, 0:128].astype(f32))

    raw = []
    for z in range(2):
        up = of_head(up_ref[z]).astype(bf16)
        part = jnp.dot(low[:, z * RANK : (z + 1) * RANK], up, preferred_element_type=f32)
        raw.append(part + of_head(bias_ref[z : z + 1, :]))
    raw = jnp.concatenate(raw, axis=1)
    return (jnp.minimum(raw, 0.0) - jnp.log1p(jnp.exp(-jnp.abs(raw)))) * (1.0 / SHARP)


def project_kernel(
    h_ref, mine_ref, other_ref, down_ref, up_ref, bias_ref, ride_ref,
    pay_ref, q_ref, k_ref, v_ref, cum_ref, w_ref, out_ref, all_logs_ref,
):
    seg, sub = lax.axis_index("A"), lax.axis_index("B")
    y, core = lax.axis_index("tp"), lax.axis_index("core")
    for xi in range(4):
        for z in range(16):
            at = z * 128 + xi * 32
            here = pl.ds(pl.multiple_of(at + core * 16, 16), 16)
            there = pl.ds(pl.multiple_of(at + 16 - core * 16, 16), 16)
            for j in range(3):
                cols = slice(j * 128, (j + 1) * 128)
                w_ref[here, cols] = mine_ref[xi, z, j * 16 : (j + 1) * 16, :]
                w_ref[there, cols] = other_ref[xi, z, j * 16 : (j + 1) * 16, :]
    y_of = [y, (y + 3) % 4, (y + 1) % 4, (y + 2) % 4]
    rows = h_ref[...]
    low = nt(rows, down_ref[...]).astype(bf16)
    slot_logs = decays_of(low, up_ref, bias_ref)
    slot_qkv = jnp.dot(rows, w_ref[...], preferred_element_type=f32).astype(bf16)
    for n in range(4):
        for j in range(5):
            size = 32 if j < 4 else 16
            took = slice(n * 144 + j * 32, n * 144 + j * 32 + size)
            if j < 4:
                at = pl.ds(pl.multiple_of((sub ^ j) * 128 + y_of[n] * 32, 32), size)
            else:
                at = pl.ds(SEG + n * 16, size)
            out_ref[at, :] = slot_qkv[took]
            all_logs_ref[at, :] = slot_logs[took]
    out = out_ref[...]
    logs = all_logs_ref[...]
    q_ref[...] = out[:SEG, 0:128]
    k_ref[...] = out[:SEG, 128:256]
    v_ref[...] = out[:SEG, 256:384]
    ef, eb = [], []
    for zb in range(4):
        t = jnp.transpose(ride_ref[seg * 4 + zb].astype(f32))
        ef.append(t[:, 4:5] + t[:, 5:6])
        eb.append(t[:, 6:7] + t[:, 7:8])
    ef = jnp.concatenate(ef, axis=0)
    eb = jnp.concatenate(eb, axis=0)
    af = logs[:SEG, 0:128] + ef
    ab = logs[:SEG, 128:256] + eb
    low_mask = tri(BLOCK, BLOCK, False)
    up_mask = tri(BLOCK, BLOCK, True)
    wf, wb = [], []
    for n in range(SEG // BLOCK):
        sl = slice(n * BLOCK, (n + 1) * BLOCK)
        wf.append(summed_by(low_mask, af[sl]))
        wb.append(summed_by(up_mask, ab[sl]))
        cum_ref[0, sl, :] = wf[-1]
        cum_ref[1, sl, :] = wb[-1]
    tot_f = [w[BLOCK - 1 : BLOCK] for w in wf]
    tot_b = [w[0:1] for w in wb]
    dev_f = sum(tot_f)
    dev_b = sum(tot_b)
    kk = out[:SEG, 128:256].astype(f32)
    before = jnp.zeros((1, DK), f32)
    kf = []
    for n in range(SEG // BLOCK):
        kf.append(kk[n * BLOCK : (n + 1) * BLOCK] * jnp.exp(dev_f - before - wf[n]))
        before = before + tot_f[n]
    after = jnp.zeros((1, DK), f32)
    kb = [None] * (SEG // BLOCK)
    for n in reversed(range(SEG // BLOCK)):
        kb[n] = kk[n * BLOCK : (n + 1) * BLOCK] * jnp.exp(dev_b - after - wb[n])
        after = after + tot_b[n]
    both = jnp.concatenate(
        [jnp.concatenate(kf, 0).astype(bf16), jnp.concatenate(kb, 0).astype(bf16)], axis=1
    )
    states = tn(out[:SEG, 256:384], both).astype(bf16)

    def order(i):
        slot = i // 16
        step = jnp.where(slot == 0, 0, jnp.where(slot == 1, 3, slot - 1))
        return (((i % 16) // 4) ^ sub) * 16 + ((step + y) % 4) * 4 + i % 4

    r = order(lax.broadcasted_iota(jnp.int32, (CTX_SEG, CTX_SEG), 0))
    c = order(lax.broadcasted_iota(jnp.int32, (CTX_SEG, CTX_SEG), 1))
    later = summed_by(c > r, logs[SEG:, 0:128])
    earlier = summed_by(c < r, logs[SEG:, 128:256])
    ctx_f = jnp.sum(logs[SEG:, 0:128], axis=0, keepdims=True)
    ctx_b = jnp.sum(logs[SEG:, 128:256], axis=0, keepdims=True)
    ck = out[SEG:, 128:256].astype(f32)
    ckf = (ck * jnp.exp(later)).astype(bf16)
    ckb = (ck * jnp.exp(earlier)).astype(bf16)
    cv = out[SEG:, 256:384]
    zero = jnp.zeros((2, DK), bf16)
    for peer in range(4):
        ahead = peer > seg
        pay_ref[peer, 0:128, :] = jnp.where(ahead, states[:, 0:128], states[:, 128:256])
        pay_ref[peer, 128:192, :] = ckf
        pay_ref[peer, 192:256, :] = ckb
        pay_ref[peer, 256:320, :] = cv
        dev = jnp.where(ahead, dev_f, dev_b)
        two = [p for t in (dev, ctx_f, ctx_b) for p in three_parts(t)[:2]]
        pay_ref[peer, 320:328, :] = jnp.concatenate([*two, zero], axis=0)


def local_kernel(q_ref, k_ref, v_ref, cum_ref, o_ref, lift_f_ref, lift_b_ref):
    blocks = SEG // BLOCK
    low_mask = tri(BLOCK, BLOCK, False)
    up_mask = tri(BLOCK, BLOCK, True)
    tot_f = [cum_ref[0, (n + 1) * BLOCK - 1 : (n + 1) * BLOCK, :] for n in range(blocks)]
    tot_b = [cum_ref[1, n * BLOCK : n * BLOCK + 1, :] for n in range(blocks)]
    state = jnp.zeros((DK, DK), f32)
    before = jnp.zeros((1, DK), f32)
    for n in range(blocks):
        sl = slice(n * BLOCK, (n + 1) * BLOCK)
        q = q_ref[sl, :].astype(f32)
        k = k_ref[sl, :].astype(f32)
        v = v_ref[sl, :]
        wf = cum_ref[0, sl, :]
        wb = cum_ref[1, sl, :]
        mf = 0.5 * tot_f[n]
        mb = 0.5 * tot_b[n]
        sf = nt((q * jnp.exp(wf - mf)).astype(bf16), (k * jnp.exp(mf - wf)).astype(bf16))
        sb = nt((q * jnp.exp(wb - mb)).astype(bf16), (k * jnp.exp(mb - wb)).astype(bf16))
        scores = jnp.where(low_mask, sf, 0.0) + jnp.where(up_mask, sb, 0.0)
        out = jnp.dot(scores.astype(bf16), v, preferred_element_type=f32)
        qd = q * jnp.exp(wf)
        lift_f_ref[sl, :] = (qd * jnp.exp(before)).astype(bf16)
        if n > 0:
            out = out + nt(qd.astype(bf16), state.astype(bf16))
        o_ref[sl, :] = out
        if n < blocks - 1:
            state = jnp.exp(tot_f[n]) * state + tn(v, (k * jnp.exp(tot_f[n] - wf)).astype(bf16))
        before = before + tot_f[n]
    state = jnp.zeros((DK, DK), f32)
    after = jnp.zeros((1, DK), f32)
    for n in reversed(range(blocks)):
        sl = slice(n * BLOCK, (n + 1) * BLOCK)
        q = q_ref[sl, :].astype(f32)
        k = k_ref[sl, :].astype(f32)
        v = v_ref[sl, :]
        wb = cum_ref[1, sl, :]
        qd = q * jnp.exp(wb)
        lift_b_ref[sl, :] = (qd * jnp.exp(after)).astype(bf16)
        if n < blocks - 1:
            o_ref[sl, :] = o_ref[sl, :] + nt(qd.astype(bf16), state.astype(bf16))
        if n > 0:
            state = jnp.exp(tot_b[n]) * state + tn(v, (k * jnp.exp(tot_b[n] - wb)).astype(bf16))
        after = after + tot_b[n]


def combine_kernel(in_ref, o_ref, lift_f_ref, lift_b_ref, out_ref):
    seg = lax.axis_index("A")

    def vec(peer, at):
        rows = in_ref[peer, 320:328, :].astype(f32)
        return rows[at : at + 1] + rows[at + 1 : at + 2]

    ctx_f = jnp.zeros((DK, DK), f32)
    ctx_b = jnp.zeros((DK, DK), f32)
    for q in range(4):
        ctx_f = jnp.exp(vec(q, 2)) * ctx_f + tn(in_ref[q, 256:320, :], in_ref[q, 128:192, :])
    for q in reversed(range(4)):
        ctx_b = jnp.exp(vec(q, 4)) * ctx_b + tn(in_ref[q, 256:320, :], in_ref[q, 192:256, :])
    fwd = CTX_LIFT * ctx_f
    for a in range(3):
        moved = jnp.exp(vec(a, 0)) * fwd + in_ref[a, 0:128, :].astype(f32)
        fwd = jnp.where(a < seg, moved, fwd)
    bwd = CTX_LIFT * ctx_b
    for a in (3, 2, 1):
        moved = jnp.exp(vec(a, 0)) * bwd + in_ref[a, 0:128, :].astype(f32)
        bwd = jnp.where(a > seg, moved, bwd)
    out = o_ref[...] + nt(lift_f_ref[...], fwd.astype(bf16)) + nt(lift_b_ref[...], bwd.astype(bf16))
    out_ref[...] = out.astype(bf16)


def output_kernel(mix_ref, gain_ref, w_ref, out_ref):
    total = None
    flip = lax.axis_index("A") // 2
    for h in range(2):
        at = 2 * (h ^ flip)
        v = jnp.concatenate([mix_ref[at], mix_ref[at + 1]], axis=1).astype(f32)
        r = lax.rsqrt(jnp.mean(v * v, axis=-1, keepdims=True) + EPS)
        n = (v * r * gain_ref[...]).astype(bf16)
        part = jnp.dot(n, w_ref[h * 256 : (h + 1) * 256, :], preferred_element_type=f32)
        total = part if total is None else total + part
    out_ref[...] = total.astype(bf16)


def device_body(
    latents,
    sample_vector,
    context,
    context_vector,
    norm_gain,
    modulator,
    query_weight,
    key_weight,
    value_weight,
    decay_down,
    decay_up,
    decay_bias,
    decay_extra,
    head_gain,
    out_weight,
):
    sds = jax.ShapeDtypeStruct
    rows, cut = pl.pallas_call(
        pack_kernel,
        out_shape=(sds((36, D), bf16), sds((16, 56, 128), bf16)),
        in_specs=[VM] * 9,
        out_specs=(VM, VM),
        compiler_params=pltpu.CompilerParams(vmem_limit_bytes=12 * 1024 * 1024),
        name="pack",
    )(
        *off_chip(
            latents, context, sample_vector, context_vector, modulator.T,
            query_weight, key_weight, value_weight,
            jnp.moveaxis(decay_extra, 1, 2).reshape(4, 128),
        )
    )
    near = [rows]
    for j in range(1, 4):
        near.append(lax.ppermute(rows, "B", [(b, b ^ j) for b in range(4)]))
    rows_z = lax.all_to_all(cut, ("A", "B"), 0, 0, tiled=True)
    mine = to_everyone(rows_z[:, 0:48], "x")
    other = lax.ppermute(mine, "core", [(0, 1), (1, 0)])
    ride = rows_z[:, 48:56]
    mods = jnp.transpose(ride, (1, 0, 2)).reshape(8, D)
    far_mods = lax.ppermute(mods, "tp", [(i, i ^ 2) for i in range(4)])

    own = jnp.concatenate([n[:32] for n in near] + [n[32:36] for n in near], axis=0)
    up_shift = [(i, (i + 1) % 4) for i in range(4)]
    down_shift = [(i, (i + 3) % 4) for i in range(4)]
    minus = lax.ppermute(own, "tp", up_shift)
    plus = lax.ppermute(own, "tp", down_shift)
    low = lax.ppermute(jnp.concatenate([minus[:64], mods]), "tp", up_shift)
    high = lax.ppermute(jnp.concatenate([plus[64:], mods]), "tp", down_shift)

    hidden, modulation = pl.pallas_call(
        hidden_kernel,
        out_shape=(sds((ROWS, D), bf16), pltpu.HBM((2, 3 * D), f32)),
        in_specs=[VM] * 8,
        out_specs=(VM, VM),
        scratch_shapes=[pltpu.VMEM((4, 8, D), f32)],
        compiler_params=pltpu.CompilerParams(vmem_limit_bytes=16 * 1024 * 1024),
        name="hidden",
    )(*on_chip(own, minus, plus, low, high, mods, far_mods), *off_chip(norm_gain.reshape(1, D)))
    payload, q, k, v, cum = pl.pallas_call(
        project_kernel,
        out_shape=(
            sds((4, PAYLOAD, DK), bf16),
            pltpu.HBM((SEG, DK), bf16),
            pltpu.HBM((SEG, DK), bf16),
            pltpu.HBM((SEG, DK), bf16),
            pltpu.HBM((2, SEG, DK), f32),
        ),
        in_specs=[VM] * 7,
        out_specs=(VM,) * 5,
        scratch_shapes=[
            pltpu.VMEM((D, 384), bf16),
            pltpu.VMEM((ROWS, 384), bf16),
            pltpu.VMEM((ROWS, 256), f32),
        ],
        compiler_params=pltpu.CompilerParams(vmem_limit_bytes=24 * 1024 * 1024),
        name="project",
    )(
        *on_chip(hidden, mine, other), *off_chip(decay_down.T, decay_up, decay_bias), *on_chip(ride),
    )
    got = lax.all_to_all(
        payload, ("A", "B"), 0, 0, tiled=True, axis_index_groups=PEERS
    )
    local, lift_f, lift_b = pl.pallas_call(
        local_kernel,
        out_shape=(sds((SEG, DK), f32), sds((SEG, DK), bf16), sds((SEG, DK), bf16)),
        in_specs=[VM] * 4,
        out_specs=(VM,) * 3,
        compiler_params=pltpu.CompilerParams(vmem_limit_bytes=12 * 1024 * 1024),
        name="local",
    )(*off_chip(q, k, v, cum))
    mixed = pl.pallas_call(
        combine_kernel,
        out_shape=sds((SEG, DK), bf16),
        in_specs=[VM] * 4,
        out_specs=VM,
        compiler_params=pltpu.CompilerParams(vmem_limit_bytes=12 * 1024 * 1024),
        name="combine",
    )(*on_chip(got, local, lift_f, lift_b))
    heads = lax.all_to_all(mixed.reshape(4, 128, DK), "B", 0, 0, tiled=True)
    partial = pl.pallas_call(
        output_kernel,
        out_shape=sds((128, D), bf16),
        in_specs=[VM] * 3,
        out_specs=VM,
        compiler_params=pltpu.CompilerParams(vmem_limit_bytes=16 * 1024 * 1024),
        name="output",
    )(*on_chip(heads), *off_chip(head_gain.reshape(1, 256)), *on_chip(out_weight))
    shares = lax.all_to_all(partial.reshape(4, 32, D), "tp", 0, 0, tiled=True)
    projected = shares.astype(f32).sum(axis=0)
    projected = lax.optimization_barrier(projected.astype(bf16)).astype(f32)
    return (latents.astype(f32) + modulation[0:1, 2 * D :] * projected).astype(bf16)


def solution(mesh):
    mesh = Mesh(mesh.devices.reshape(4, 4, 4, 4, 2), ("A", "B", "tp", "x", "core"))
    dp = ("x", "core")
    sp = ("A", "B")
    placed = (
        P((*dp, *sp, "tp"), None),
        P(dp, None),
        P((*dp, *sp), None),
        P(),
        P(),
        P(None, (*sp, "tp")),
        P(sp, "tp"),
        P(sp, "tp"),
        P(sp, "tp"),
        P(),
        P(None, None, "tp"),
        P(None, "tp"),
        P(None, (*dp, *sp), "tp"),
        P(),
        P("tp", None),
    )
    return jax.shard_map(
        device_body,
        mesh=mesh,
        in_specs=placed,
        out_specs=P((*dp, *sp, "tp"), None),
        check_vma=False,
    )
```

```python
import jax
import jax.numpy as jnp
from jax import lax
from jax.experimental import pallas as pl
from jax.experimental.pallas import tpu as pltpu
from jax.sharding import Mesh, PartitionSpec as P


D = 2048
DK = 128
RANK = 32
BLOCK = 64
CTX_LIFT = 4.0
EPS = 1e-06
SHARP = 16.0
SEG = 512
CTX_SEG = 64
ROWS = SEG + CTX_SEG
PAYLOAD = 328
bf16 = jnp.bfloat16
f32 = jnp.float32
VM = pl.BlockSpec(memory_space=pltpu.VMEM)
SM = pl.BlockSpec(memory_space=pltpu.SMEM)


def on_chip(*arrays):
    return tuple(pltpu.with_memory_space_constraint(a, pltpu.VMEM) for a in arrays)


def off_chip(*arrays):
    return tuple(pltpu.with_memory_space_constraint(a, pltpu.HBM) for a in arrays)


def to_everyone(x, axis):
    size = lax.axis_size(axis)
    return lax.all_to_all(jnp.broadcast_to(x[None], (size, *x.shape)), axis, 0, 0, tiled=True)


def role(seg, sub):
    return sub ^ (seg // 2 * 2)


PEERS = [[4 * a + role(a, b) for a in range(4)] for b in range(4)]


def three_parts(x):
    hi = x.astype(bf16)
    rest = x - hi.astype(f32)
    mid = rest.astype(bf16)
    lo = (rest - mid.astype(f32)).astype(bf16)
    return hi, mid, lo


def tri(rows, cols, upper):
    r = lax.broadcasted_iota(jnp.int32, (rows, cols), 0)
    c = lax.broadcasted_iota(jnp.int32, (rows, cols), 1)
    return (c >= r) if upper else (c <= r)


def summed_by(mask, a):
    m = mask.astype(f32).astype(bf16)
    stacked = jnp.concatenate(three_parts(a), axis=0)
    return jnp.dot(jnp.concatenate([m, m, m], axis=1), stacked, preferred_element_type=f32)


def nt(a, b):
    return lax.dot_general(a, b, (((1,), (1,)), ((), ())), preferred_element_type=f32)


def tn(a, b):
    return lax.dot_general(a, b, (((0,), (0,)), ((), ())), preferred_element_type=f32)


def pack_kernel(
    lat_ref, ctx_ref, sv_ref, cv_ref, mod_ref, wq_ref, wk_ref, wv_ref, extra_ref, rows_ref, cut_ref
):
    y = lax.axis_index("tp")
    dp = lax.axis_index("x") * 2 + lax.axis_index("core")
    rows_ref[0:32, :] = lat_ref[...]
    ctx = ctx_ref[...].astype(f32)
    picked = ctx[12:16]
    for i in range(3):
        picked = jnp.where(y == i, ctx[4 * i : 4 * i + 4], picked)
    rows_ref[32:36, :] = picked.astype(bf16)

    both = jnp.concatenate([sv_ref[...], cv_ref[...]], axis=0)
    conditions = (both / (1.0 + jnp.exp(-both))).astype(bf16)
    local_mods = nt(conditions, mod_ref[...])
    mods = jnp.concatenate([p.astype(f32) for p in three_parts(local_mods)[:2]], axis=0)
    mods = jnp.concatenate([mods, jnp.zeros((4, 32), f32)], axis=1)
    e_hi, e_mid, _ = three_parts(extra_ref[...])
    e_hi, e_mid = e_hi.astype(f32), e_mid.astype(f32)
    riding = []
    for h in range(2):
        added = [e_hi[h : h + 1], e_mid[h : h + 1], e_hi[2 + h : 3 + h], e_mid[2 + h : 3 + h]]
        riding.append(jnp.concatenate([mods, *added], axis=0).astype(bf16))
    mine = pl.ds(pl.multiple_of(dp * 16, 16), 16)
    for d in range(16):
        b = role(d // 4, d % 4)
        h = b // 2
        cut_ref[d, 0:16, :] = wq_ref[mine, h * 128 : (h + 1) * 128]
        cut_ref[d, 16:32, :] = wk_ref[mine, h * 128 : (h + 1) * 128]
        cut_ref[d, 32:48, :] = wv_ref[mine, b * 128 : (b + 1) * 128]
        cut_ref[d, 48:56, :] = riding[h]


def normed_rows(rows, which, mod_ref, gain_ref):
    v = rows.astype(f32)
    r = lax.rsqrt(jnp.mean(v * v, axis=-1, keepdims=True) + EPS)
    scale = gain_ref[...] * (1.0 + mod_ref[which : which + 1, D : 2 * D])
    return (v * r * scale + mod_ref[which : which + 1, 0:D]).astype(bf16)


def hidden_kernel(
    own_ref, minus_ref, plus_ref, low_ref, high_ref, own_mods_ref, far_mods_ref, gain_ref,
    h_ref, mod_ref, mods_ref,
):
    y = lax.axis_index("tp")
    mods_ref[y] = own_mods_ref[...].astype(f32)
    mods_ref[(y + 3) % 4] = low_ref[64:72, :].astype(f32)
    mods_ref[(y + 1) % 4] = high_ref[80:88, :].astype(f32)
    mods_ref[(y + 2) % 4] = far_mods_ref[...].astype(f32)
    for z in range(16):
        at = slice(z * 128, z * 128 + 96)
        parts = [mods_ref[i, 0:2, at] + mods_ref[i, 2:4, at] for i in range(4)]
        mod_ref[:, z * 384 : (z + 1) * 384] = jnp.concatenate(parts, axis=1)
    for slot in range(4):
        for j in range(5):
            size = 32 if j < 4 else 16
            if slot < 3:
                rows = (own_ref, minus_ref, plus_ref)[slot][j * 32 : j * 32 + size, :]
            elif j < 2:
                rows = low_ref[j * 32 : j * 32 + 32, :]
            else:
                rows = high_ref[j * 32 - 64 : j * 32 - 64 + size, :]
            at = slot * 144 + j * 32
            h_ref[at : at + size, :] = normed_rows(rows, j // 4, mod_ref, gain_ref)


def decays_of(low, up_ref, bias_ref):
    second = role(lax.axis_index("A"), lax.axis_index("B")) >= 2

    def of_head(a):
        return jnp.where(second, a[:, 128:256].astype(f32), a[:, 0:128].astype(f32))

    raw = []
    for z in range(2):
        up = of_head(up_ref[z]).astype(bf16)
        part = jnp.dot(low[:, z * RANK : (z + 1) * RANK], up, preferred_element_type=f32)
        raw.append(part + of_head(bias_ref[z : z + 1, :]))
    raw = jnp.concatenate(raw, axis=1)
    return (jnp.minimum(raw, 0.0) - jnp.log1p(jnp.exp(-jnp.abs(raw)))) * (1.0 / SHARP)


def project_kernel(
    h_ref, mine_ref, other_ref, down_ref, up_ref, bias_ref, ride_ref,
    pay_ref, q_ref, k_ref, v_ref, cum_ref, w_ref, out_ref, all_logs_ref,
):
    seg, sub = lax.axis_index("A"), lax.axis_index("B")
    y, core = lax.axis_index("tp"), lax.axis_index("core")
    for xi in range(4):
        for z in range(16):
            at = z * 128 + xi * 32
            here = pl.ds(pl.multiple_of(at + core * 16, 16), 16)
            there = pl.ds(pl.multiple_of(at + 16 - core * 16, 16), 16)
            for j in range(3):
                cols = slice(j * 128, (j + 1) * 128)
                w_ref[here, cols] = mine_ref[xi, z, j * 16 : (j + 1) * 16, :]
                w_ref[there, cols] = other_ref[xi, z, j * 16 : (j + 1) * 16, :]
    y_of = [y, (y + 3) % 4, (y + 1) % 4, (y + 2) % 4]
    rows = h_ref[...]
    low = nt(rows, down_ref[...]).astype(bf16)
    slot_logs = decays_of(low, up_ref, bias_ref)
    slot_qkv = jnp.dot(rows, w_ref[...], preferred_element_type=f32).astype(bf16)
    for n in range(4):
        for j in range(5):
            size = 32 if j < 4 else 16
            took = slice(n * 144 + j * 32, n * 144 + j * 32 + size)
            if j < 4:
                at = pl.ds(pl.multiple_of((sub ^ j) * 128 + y_of[n] * 32, 32), size)
            else:
                at = pl.ds(SEG + n * 16, size)
            out_ref[at, :] = slot_qkv[took]
            all_logs_ref[at, :] = slot_logs[took]
    out = out_ref[...]
    logs = all_logs_ref[...]
    q_ref[...] = out[:SEG, 0:128]
    k_ref[...] = out[:SEG, 128:256]
    v_ref[...] = out[:SEG, 256:384]
    ef, eb = [], []
    for zb in range(4):
        t = jnp.transpose(ride_ref[seg * 4 + zb].astype(f32))
        ef.append(t[:, 4:5] + t[:, 5:6])
        eb.append(t[:, 6:7] + t[:, 7:8])
    ef = jnp.concatenate(ef, axis=0)
    eb = jnp.concatenate(eb, axis=0)
    af = logs[:SEG, 0:128] + ef
    ab = logs[:SEG, 128:256] + eb
    low_mask = tri(BLOCK, BLOCK, False)
    up_mask = tri(BLOCK, BLOCK, True)
    wf, wb = [], []
    for n in range(SEG // BLOCK):
        sl = slice(n * BLOCK, (n + 1) * BLOCK)
        wf.append(summed_by(low_mask, af[sl]))
        wb.append(summed_by(up_mask, ab[sl]))
        cum_ref[0, sl, :] = wf[-1]
        cum_ref[1, sl, :] = wb[-1]
    tot_f = [w[BLOCK - 1 : BLOCK] for w in wf]
    tot_b = [w[0:1] for w in wb]
    dev_f = sum(tot_f)
    dev_b = sum(tot_b)
    kk = out[:SEG, 128:256].astype(f32)
    before = jnp.zeros((1, DK), f32)
    kf = []
    for n in range(SEG // BLOCK):
        kf.append(kk[n * BLOCK : (n + 1) * BLOCK] * jnp.exp(dev_f - before - wf[n]))
        before = before + tot_f[n]
    after = jnp.zeros((1, DK), f32)
    kb = [None] * (SEG // BLOCK)
    for n in reversed(range(SEG // BLOCK)):
        kb[n] = kk[n * BLOCK : (n + 1) * BLOCK] * jnp.exp(dev_b - after - wb[n])
        after = after + tot_b[n]
    both = jnp.concatenate(
        [jnp.concatenate(kf, 0).astype(bf16), jnp.concatenate(kb, 0).astype(bf16)], axis=1
    )
    states = tn(out[:SEG, 256:384], both).astype(bf16)

    def order(i):
        slot = i // 16
        step = jnp.where(slot == 0, 0, jnp.where(slot == 1, 3, slot - 1))
        return (((i % 16) // 4) ^ sub) * 16 + ((step + y) % 4) * 4 + i % 4

    r = order(lax.broadcasted_iota(jnp.int32, (CTX_SEG, CTX_SEG), 0))
    c = order(lax.broadcasted_iota(jnp.int32, (CTX_SEG, CTX_SEG), 1))
    later = summed_by(c > r, logs[SEG:, 0:128])
    earlier = summed_by(c < r, logs[SEG:, 128:256])
    ctx_f = jnp.sum(logs[SEG:, 0:128], axis=0, keepdims=True)
    ctx_b = jnp.sum(logs[SEG:, 128:256], axis=0, keepdims=True)
    ck = out[SEG:, 128:256].astype(f32)
    ckf = (ck * jnp.exp(later)).astype(bf16)
    ckb = (ck * jnp.exp(earlier)).astype(bf16)
    cv = out[SEG:, 256:384]
    zero = jnp.zeros((2, DK), bf16)
    for peer in range(4):
        ahead = peer > seg
        pay_ref[peer, 0:128, :] = jnp.where(ahead, states[:, 0:128], states[:, 128:256])
        pay_ref[peer, 128:192, :] = ckf
        pay_ref[peer, 192:256, :] = ckb
        pay_ref[peer, 256:320, :] = cv
        dev = jnp.where(ahead, dev_f, dev_b)
        two = [p for t in (dev, ctx_f, ctx_b) for p in three_parts(t)[:2]]
        pay_ref[peer, 320:328, :] = jnp.concatenate([*two, zero], axis=0)


def local_kernel(q_ref, k_ref, v_ref, cum_ref, o_ref, lift_f_ref, lift_b_ref):
    blocks = SEG // BLOCK
    low_mask = tri(BLOCK, BLOCK, False)
    up_mask = tri(BLOCK, BLOCK, True)
    tot_f = [cum_ref[0, (n + 1) * BLOCK - 1 : (n + 1) * BLOCK, :] for n in range(blocks)]
    tot_b = [cum_ref[1, n * BLOCK : n * BLOCK + 1, :] for n in range(blocks)]
    state = jnp.zeros((DK, DK), f32)
    before = jnp.zeros((1, DK), f32)
    for n in range(blocks):
        sl = slice(n * BLOCK, (n + 1) * BLOCK)
        q = q_ref[sl, :].astype(f32)
        k = k_ref[sl, :].astype(f32)
        v = v_ref[sl, :]
        wf = cum_ref[0, sl, :]
        wb = cum_ref[1, sl, :]
        mf = 0.5 * tot_f[n]
        mb = 0.5 * tot_b[n]
        sf = nt((q * jnp.exp(wf - mf)).astype(bf16), (k * jnp.exp(mf - wf)).astype(bf16))
        sb = nt((q * jnp.exp(wb - mb)).astype(bf16), (k * jnp.exp(mb - wb)).astype(bf16))
        scores = jnp.where(low_mask, sf, 0.0) + jnp.where(up_mask, sb, 0.0)
        out = jnp.dot(scores.astype(bf16), v, preferred_element_type=f32)
        qd = q * jnp.exp(wf)
        lift_f_ref[sl, :] = (qd * jnp.exp(before)).astype(bf16)
        if n > 0:
            out = out + nt(qd.astype(bf16), state.astype(bf16))
        o_ref[sl, :] = out
        if n < blocks - 1:
            state = jnp.exp(tot_f[n]) * state + tn(v, (k * jnp.exp(tot_f[n] - wf)).astype(bf16))
        before = before + tot_f[n]
    state = jnp.zeros((DK, DK), f32)
    after = jnp.zeros((1, DK), f32)
    for n in reversed(range(blocks)):
        sl = slice(n * BLOCK, (n + 1) * BLOCK)
        q = q_ref[sl, :].astype(f32)
        k = k_ref[sl, :].astype(f32)
        v = v_ref[sl, :]
        wb = cum_ref[1, sl, :]
        qd = q * jnp.exp(wb)
        lift_b_ref[sl, :] = (qd * jnp.exp(after)).astype(bf16)
        if n < blocks - 1:
            o_ref[sl, :] = o_ref[sl, :] + nt(qd.astype(bf16), state.astype(bf16))
        if n > 0:
            state = jnp.exp(tot_b[n]) * state + tn(v, (k * jnp.exp(tot_b[n] - wb)).astype(bf16))
        after = after + tot_b[n]


def combine_kernel(in_ref, o_ref, lift_f_ref, lift_b_ref, out_ref):
    seg = lax.axis_index("A")

    def vec(peer, at):
        rows = in_ref[peer, 320:328, :].astype(f32)
        return rows[at : at + 1] + rows[at + 1 : at + 2]

    ctx_f = jnp.zeros((DK, DK), f32)
    ctx_b = jnp.zeros((DK, DK), f32)
    for q in range(4):
        ctx_f = jnp.exp(vec(q, 2)) * ctx_f + tn(in_ref[q, 256:320, :], in_ref[q, 128:192, :])
    for q in reversed(range(4)):
        ctx_b = jnp.exp(vec(q, 4)) * ctx_b + tn(in_ref[q, 256:320, :], in_ref[q, 192:256, :])
    fwd = CTX_LIFT * ctx_f
    for a in range(3):
        moved = jnp.exp(vec(a, 0)) * fwd + in_ref[a, 0:128, :].astype(f32)
        fwd = jnp.where(a < seg, moved, fwd)
    bwd = CTX_LIFT * ctx_b
    for a in (3, 2, 1):
        moved = jnp.exp(vec(a, 0)) * bwd + in_ref[a, 0:128, :].astype(f32)
        bwd = jnp.where(a > seg, moved, bwd)
    out = o_ref[...] + nt(lift_f_ref[...], fwd.astype(bf16)) + nt(lift_b_ref[...], bwd.astype(bf16))
    out_ref[...] = out.astype(bf16)


def output_kernel(mix_ref, gain_ref, w_ref, out_ref):
    total = None
    flip = lax.axis_index("A") // 2
    for h in range(2):
        at = 2 * (h ^ flip)
        v = jnp.concatenate([mix_ref[at], mix_ref[at + 1]], axis=1).astype(f32)
        r = lax.rsqrt(jnp.mean(v * v, axis=-1, keepdims=True) + EPS)
        n = (v * r * gain_ref[...]).astype(bf16)
        part = jnp.dot(n, w_ref[h * 256 : (h + 1) * 256, :], preferred_element_type=f32)
        total = part if total is None else total + part
    out_ref[...] = total.astype(bf16)


def device_body(
    latents,
    sample_vector,
    context,
    context_vector,
    norm_gain,
    modulator,
    query_weight,
    key_weight,
    value_weight,
    decay_down,
    decay_up,
    decay_bias,
    decay_extra,
    head_gain,
    out_weight,
):
    sds = jax.ShapeDtypeStruct
    rows, cut = pl.pallas_call(
        pack_kernel,
        out_shape=(sds((36, D), bf16), pltpu.VMEM((16, 56, 128), bf16)),
        in_specs=[VM] * 9,
        out_specs=(VM, VM),
        compiler_params=pltpu.CompilerParams(vmem_limit_bytes=12 * 1024 * 1024),
        name="pack",
    )(
        *off_chip(
            latents, context, sample_vector, context_vector, modulator.T,
            query_weight, key_weight, value_weight,
            jnp.moveaxis(decay_extra, 1, 2).reshape(4, 128),
        )
    )
    near = [rows]
    for j in range(1, 4):
        near.append(lax.ppermute(rows, "B", [(b, b ^ j) for b in range(4)]))
    rows_z = lax.all_to_all(cut, ("A", "B"), 0, 0, tiled=True)
    mine = to_everyone(rows_z[:, 0:48], "x")
    other = lax.ppermute(mine, "core", [(0, 1), (1, 0)])
    ride = rows_z[:, 48:56]
    mods = jnp.transpose(ride, (1, 0, 2)).reshape(8, D)
    far_mods = lax.ppermute(mods, "tp", [(i, i ^ 2) for i in range(4)])

    own = jnp.concatenate([n[:32] for n in near] + [n[32:36] for n in near], axis=0)
    up_shift = [(i, (i + 1) % 4) for i in range(4)]
    down_shift = [(i, (i + 3) % 4) for i in range(4)]
    minus = lax.ppermute(own, "tp", up_shift)
    plus = lax.ppermute(own, "tp", down_shift)
    low = lax.ppermute(jnp.concatenate([minus[:64], mods]), "tp", up_shift)
    high = lax.ppermute(jnp.concatenate([plus[64:], mods]), "tp", down_shift)

    hidden, modulation = pl.pallas_call(
        hidden_kernel,
        out_shape=(sds((ROWS, D), bf16), pltpu.HBM((2, 3 * D), f32)),
        in_specs=[VM] * 8,
        out_specs=(VM, VM),
        scratch_shapes=[pltpu.VMEM((4, 8, D), f32)],
        compiler_params=pltpu.CompilerParams(vmem_limit_bytes=16 * 1024 * 1024),
        name="hidden",
    )(*on_chip(own, minus, plus, low, high, mods, far_mods), *off_chip(norm_gain.reshape(1, D)))
    payload, q, k, v, cum = pl.pallas_call(
        project_kernel,
        out_shape=(
            pltpu.VMEM((4, PAYLOAD, DK), bf16),
            pltpu.HBM((SEG, DK), bf16),
            pltpu.HBM((SEG, DK), bf16),
            pltpu.HBM((SEG, DK), bf16),
            pltpu.HBM((2, SEG, DK), f32),
        ),
        in_specs=[VM] * 7,
        out_specs=(VM,) * 5,
        scratch_shapes=[
            pltpu.VMEM((D, 384), bf16),
            pltpu.VMEM((ROWS, 384), bf16),
            pltpu.VMEM((ROWS, 256), f32),
        ],
        compiler_params=pltpu.CompilerParams(vmem_limit_bytes=24 * 1024 * 1024),
        name="project",
    )(
        *on_chip(hidden, mine, other), *off_chip(decay_down.T, decay_up, decay_bias), *on_chip(ride),
    )
    got = lax.all_to_all(
        payload, ("A", "B"), 0, 0, tiled=True, axis_index_groups=PEERS
    )
    local, lift_f, lift_b = pl.pallas_call(
        local_kernel,
        out_shape=(sds((SEG, DK), f32), sds((SEG, DK), bf16), sds((SEG, DK), bf16)),
        in_specs=[VM] * 4,
        out_specs=(VM,) * 3,
        compiler_params=pltpu.CompilerParams(vmem_limit_bytes=12 * 1024 * 1024),
        name="local",
    )(*off_chip(q, k, v, cum))
    mixed = pl.pallas_call(
        combine_kernel,
        out_shape=sds((SEG, DK), bf16),
        in_specs=[VM] * 4,
        out_specs=VM,
        compiler_params=pltpu.CompilerParams(vmem_limit_bytes=12 * 1024 * 1024),
        name="combine",
    )(*on_chip(got, local, lift_f, lift_b))
    heads = lax.all_to_all(mixed.reshape(4, 128, DK), "B", 0, 0, tiled=True)
    partial = pl.pallas_call(
        output_kernel,
        out_shape=pltpu.VMEM((128, D), bf16),
        in_specs=[VM] * 3,
        out_specs=VM,
        compiler_params=pltpu.CompilerParams(vmem_limit_bytes=16 * 1024 * 1024),
        name="output",
    )(*on_chip(heads), *off_chip(head_gain.reshape(1, 256)), *on_chip(out_weight))
    shares = lax.all_to_all(partial.reshape(4, 32, D), "tp", 0, 0, tiled=True)
    projected = shares.astype(f32).sum(axis=0)
    projected = lax.optimization_barrier(projected.astype(bf16)).astype(f32)
    return (latents.astype(f32) + modulation[0:1, 2 * D :] * projected).astype(bf16)


def solution(mesh):
    mesh = Mesh(mesh.devices.reshape(4, 4, 4, 4, 2), ("A", "B", "tp", "x", "core"))
    dp = ("x", "core")
    sp = ("A", "B")
    placed = (
        P((*dp, *sp, "tp"), None),
        P(dp, None),
        P((*dp, *sp), None),
        P(),
        P(),
        P(None, (*sp, "tp")),
        P(sp, "tp"),
        P(sp, "tp"),
        P(sp, "tp"),
        P(),
        P(None, None, "tp"),
        P(None, "tp"),
        P(None, (*dp, *sp), "tp"),
        P(),
        P("tp", None),
    )
    return jax.shard_map(
        device_body,
        mesh=mesh,
        in_specs=placed,
        out_specs=P((*dp, *sp, "tp"), None),
        check_vma=False,
    )
```

```python
import jax
import jax.numpy as jnp
from jax import lax
from jax.experimental import pallas as pl
from jax.experimental.pallas import tpu as pltpu
from jax.sharding import Mesh, PartitionSpec as P


D = 2048
DK = 128
RANK = 32
BLOCK = 64
CTX_LIFT = 4.0
EPS = 1e-06
SHARP = 16.0
SEG = 512
CTX_SEG = 64
ROWS = SEG + CTX_SEG
PAYLOAD = 328
bf16 = jnp.bfloat16
f32 = jnp.float32
VM = pl.BlockSpec(memory_space=pltpu.VMEM)
SM = pl.BlockSpec(memory_space=pltpu.SMEM)


def on_chip(*arrays):
    return tuple(pltpu.with_memory_space_constraint(a, pltpu.VMEM) for a in arrays)


def off_chip(*arrays):
    return tuple(pltpu.with_memory_space_constraint(a, pltpu.HBM) for a in arrays)


def to_everyone(x, axis):
    size = lax.axis_size(axis)
    return lax.all_to_all(jnp.broadcast_to(x[None], (size, *x.shape)), axis, 0, 0, tiled=True)


def role(seg, sub):
    return sub ^ (seg // 2 * 2)


PEERS = [[4 * a + role(a, b) for a in range(4)] for b in range(4)]


def three_parts(x):
    hi = x.astype(bf16)
    rest = x - hi.astype(f32)
    mid = rest.astype(bf16)
    lo = (rest - mid.astype(f32)).astype(bf16)
    return hi, mid, lo


def tri(rows, cols, upper):
    r = lax.broadcasted_iota(jnp.int32, (rows, cols), 0)
    c = lax.broadcasted_iota(jnp.int32, (rows, cols), 1)
    return (c >= r) if upper else (c <= r)


def summed_by(mask, a):
    m = mask.astype(f32).astype(bf16)
    stacked = jnp.concatenate(three_parts(a), axis=0)
    return jnp.dot(jnp.concatenate([m, m, m], axis=1), stacked, preferred_element_type=f32)


def nt(a, b):
    return lax.dot_general(a, b, (((1,), (1,)), ((), ())), preferred_element_type=f32)


def tn(a, b):
    return lax.dot_general(a, b, (((0,), (0,)), ((), ())), preferred_element_type=f32)


def pack_kernel(
    lat_ref, ctx_ref, sv_ref, cv_ref, mod_ref, wq_ref, wk_ref, wv_ref, extra_ref, rows_ref, cut_ref
):
    y = lax.axis_index("tp")
    dp = lax.axis_index("x") * 2 + lax.axis_index("core")
    rows_ref[0:32, :] = lat_ref[...]
    ctx = ctx_ref[...].astype(f32)
    picked = ctx[12:16]
    for i in range(3):
        picked = jnp.where(y == i, ctx[4 * i : 4 * i + 4], picked)
    rows_ref[32:36, :] = picked.astype(bf16)

    both = jnp.concatenate([sv_ref[...], cv_ref[...]], axis=0)
    conditions = (both / (1.0 + jnp.exp(-both))).astype(bf16)
    local_mods = nt(conditions, mod_ref[...])
    mods = jnp.concatenate([p.astype(f32) for p in three_parts(local_mods)[:2]], axis=0)
    mods = jnp.concatenate([mods, jnp.zeros((4, 32), f32)], axis=1)
    e_hi, e_mid, _ = three_parts(extra_ref[...])
    e_hi, e_mid = e_hi.astype(f32), e_mid.astype(f32)
    riding = []
    for h in range(2):
        added = [e_hi[h : h + 1], e_mid[h : h + 1], e_hi[2 + h : 3 + h], e_mid[2 + h : 3 + h]]
        riding.append(jnp.concatenate([mods, *added], axis=0).astype(bf16))
    mine = pl.ds(pl.multiple_of(dp * 16, 16), 16)
    for d in range(16):
        b = role(d // 4, d % 4)
        h = b // 2
        cut_ref[d, 0:16, :] = wq_ref[mine, h * 128 : (h + 1) * 128]
        cut_ref[d, 16:32, :] = wk_ref[mine, h * 128 : (h + 1) * 128]
        cut_ref[d, 32:48, :] = wv_ref[mine, b * 128 : (b + 1) * 128]
        cut_ref[d, 48:56, :] = riding[h]


def normed_rows(rows, which, mod_ref, gain_ref):
    v = rows.astype(f32)
    r = lax.rsqrt(jnp.mean(v * v, axis=-1, keepdims=True) + EPS)
    scale = gain_ref[...] * (1.0 + mod_ref[which : which + 1, D : 2 * D])
    return (v * r * scale + mod_ref[which : which + 1, 0:D]).astype(bf16)


def hidden_kernel(
    own_ref, minus_ref, plus_ref, low_ref, high_ref, own_mods_ref, far_mods_ref, gain_ref,
    h_ref, mod_ref, mods_ref,
):
    y = lax.axis_index("tp")
    mods_ref[y] = own_mods_ref[...].astype(f32)
    mods_ref[(y + 3) % 4] = low_ref[64:72, :].astype(f32)
    mods_ref[(y + 1) % 4] = high_ref[80:88, :].astype(f32)
    mods_ref[(y + 2) % 4] = far_mods_ref[...].astype(f32)
    for z in range(16):
        at = slice(z * 128, z * 128 + 96)
        parts = [mods_ref[i, 0:2, at] + mods_ref[i, 2:4, at] for i in range(4)]
        mod_ref[:, z * 384 : (z + 1) * 384] = jnp.concatenate(parts, axis=1)
    for slot in range(4):
        for j in range(5):
            size = 32 if j < 4 else 16
            if slot < 3:
                rows = (own_ref, minus_ref, plus_ref)[slot][j * 32 : j * 32 + size, :]
            elif j < 2:
                rows = low_ref[j * 32 : j * 32 + 32, :]
            else:
                rows = high_ref[j * 32 - 64 : j * 32 - 64 + size, :]
            at = slot * 144 + j * 32
            h_ref[at : at + size, :] = normed_rows(rows, j // 4, mod_ref, gain_ref)


def decays_of(low, up_ref, bias_ref):
    second = role(lax.axis_index("A"), lax.axis_index("B")) >= 2

    def of_head(a):
        return jnp.where(second, a[:, 128:256].astype(f32), a[:, 0:128].astype(f32))

    raw = []
    for z in range(2):
        up = of_head(up_ref[z]).astype(bf16)
        part = jnp.dot(low[:, z * RANK : (z + 1) * RANK], up, preferred_element_type=f32)
        raw.append(part + of_head(bias_ref[z : z + 1, :]))
    raw = jnp.concatenate(raw, axis=1)
    return (jnp.minimum(raw, 0.0) - jnp.log1p(jnp.exp(-jnp.abs(raw)))) * (1.0 / SHARP)


def project_kernel(
    h_ref, mine_ref, other_ref, down_ref, up_ref, bias_ref, ride_ref,
    pay_ref, q_ref, k_ref, v_ref, cum_ref, w_ref, out_ref, all_logs_ref,
):
    seg, sub = lax.axis_index("A"), lax.axis_index("B")
    y, core = lax.axis_index("tp"), lax.axis_index("core")
    for xi in range(4):
        for z in range(16):
            at = z * 128 + xi * 32
            here = pl.ds(pl.multiple_of(at + core * 16, 16), 16)
            there = pl.ds(pl.multiple_of(at + 16 - core * 16, 16), 16)
            for j in range(3):
                cols = slice(j * 128, (j + 1) * 128)
                w_ref[here, cols] = mine_ref[xi, z, j * 16 : (j + 1) * 16, :]
                w_ref[there, cols] = other_ref[xi, z, j * 16 : (j + 1) * 16, :]
    w_ref[:, 384:448] = down_ref[...]
    y_of = [y, (y + 3) % 4, (y + 1) % 4, (y + 2) % 4]
    res = jnp.dot(h_ref[...], w_ref[...], preferred_element_type=f32).astype(bf16)
    slot_logs = decays_of(res[:, 384:448], up_ref, bias_ref)
    slot_qkv = res[:, 0:384]
    for n in range(4):
        for j in range(5):
            size = 32 if j < 4 else 16
            took = slice(n * 144 + j * 32, n * 144 + j * 32 + size)
            if j < 4:
                at = pl.ds(pl.multiple_of((sub ^ j) * 128 + y_of[n] * 32, 32), size)
            else:
                at = pl.ds(SEG + n * 16, size)
            out_ref[at, :] = slot_qkv[took]
            all_logs_ref[at, :] = slot_logs[took]
    out = out_ref[...]
    logs = all_logs_ref[...]
    q_ref[...] = out[:SEG, 0:128]
    k_ref[...] = out[:SEG, 128:256]
    v_ref[...] = out[:SEG, 256:384]
    ef, eb = [], []
    for zb in range(4):
        t = jnp.transpose(ride_ref[seg * 4 + zb].astype(f32))
        ef.append(t[:, 4:5] + t[:, 5:6])
        eb.append(t[:, 6:7] + t[:, 7:8])
    ef = jnp.concatenate(ef, axis=0)
    eb = jnp.concatenate(eb, axis=0)
    af = logs[:SEG, 0:128] + ef
    ab = logs[:SEG, 128:256] + eb
    low_mask = tri(BLOCK, BLOCK, False)
    up_mask = tri(BLOCK, BLOCK, True)
    wf, wb = [], []
    for n in range(SEG // BLOCK):
        sl = slice(n * BLOCK, (n + 1) * BLOCK)
        wf.append(summed_by(low_mask, af[sl]))
        wb.append(summed_by(up_mask, ab[sl]))
        cum_ref[0, sl, :] = wf[-1]
        cum_ref[1, sl, :] = wb[-1]
    tot_f = [w[BLOCK - 1 : BLOCK] for w in wf]
    tot_b = [w[0:1] for w in wb]
    dev_f = sum(tot_f)
    dev_b = sum(tot_b)
    kk = out[:SEG, 128:256].astype(f32)
    before = jnp.zeros((1, DK), f32)
    kf = []
    for n in range(SEG // BLOCK):
        kf.append(kk[n * BLOCK : (n + 1) * BLOCK] * jnp.exp(dev_f - before - wf[n]))
        before = before + tot_f[n]
    after = jnp.zeros((1, DK), f32)
    kb = [None] * (SEG // BLOCK)
    for n in reversed(range(SEG // BLOCK)):
        kb[n] = kk[n * BLOCK : (n + 1) * BLOCK] * jnp.exp(dev_b - after - wb[n])
        after = after + tot_b[n]
    both = jnp.concatenate(
        [jnp.concatenate(kf, 0).astype(bf16), jnp.concatenate(kb, 0).astype(bf16)], axis=1
    )
    states = tn(out[:SEG, 256:384], both).astype(bf16)

    def order(i):
        slot = i // 16
        step = jnp.where(slot == 0, 0, jnp.where(slot == 1, 3, slot - 1))
        return (((i % 16) // 4) ^ sub) * 16 + ((step + y) % 4) * 4 + i % 4

    r = order(lax.broadcasted_iota(jnp.int32, (CTX_SEG, CTX_SEG), 0))
    c = order(lax.broadcasted_iota(jnp.int32, (CTX_SEG, CTX_SEG), 1))
    later = summed_by(c > r, logs[SEG:, 0:128])
    earlier = summed_by(c < r, logs[SEG:, 128:256])
    ctx_f = jnp.sum(logs[SEG:, 0:128], axis=0, keepdims=True)
    ctx_b = jnp.sum(logs[SEG:, 128:256], axis=0, keepdims=True)
    ck = out[SEG:, 128:256].astype(f32)
    ckf = (ck * jnp.exp(later)).astype(bf16)
    ckb = (ck * jnp.exp(earlier)).astype(bf16)
    cv = out[SEG:, 256:384]
    zero = jnp.zeros((2, DK), bf16)
    for peer in range(4):
        ahead = peer > seg
        pay_ref[peer, 0:128, :] = jnp.where(ahead, states[:, 0:128], states[:, 128:256])
        pay_ref[peer, 128:192, :] = ckf
        pay_ref[peer, 192:256, :] = ckb
        pay_ref[peer, 256:320, :] = cv
        dev = jnp.where(ahead, dev_f, dev_b)
        two = [p for t in (dev, ctx_f, ctx_b) for p in three_parts(t)[:2]]
        pay_ref[peer, 320:328, :] = jnp.concatenate([*two, zero], axis=0)


def local_kernel(q_ref, k_ref, v_ref, cum_ref, o_ref, lift_f_ref, lift_b_ref):
    blocks = SEG // BLOCK
    low_mask = tri(BLOCK, BLOCK, False)
    up_mask = tri(BLOCK, BLOCK, True)
    tot_f = [cum_ref[0, (n + 1) * BLOCK - 1 : (n + 1) * BLOCK, :] for n in range(blocks)]
    tot_b = [cum_ref[1, n * BLOCK : n * BLOCK + 1, :] for n in range(blocks)]
    state = jnp.zeros((DK, DK), f32)
    before = jnp.zeros((1, DK), f32)
    for n in range(blocks):
        sl = slice(n * BLOCK, (n + 1) * BLOCK)
        q = q_ref[sl, :].astype(f32)
        k = k_ref[sl, :].astype(f32)
        v = v_ref[sl, :]
        wf = cum_ref[0, sl, :]
        wb = cum_ref[1, sl, :]
        mf = 0.5 * tot_f[n]
        mb = 0.5 * tot_b[n]
        sf = nt((q * jnp.exp(wf - mf)).astype(bf16), (k * jnp.exp(mf - wf)).astype(bf16))
        sb = nt((q * jnp.exp(wb - mb)).astype(bf16), (k * jnp.exp(mb - wb)).astype(bf16))
        scores = jnp.where(low_mask, sf, 0.0) + jnp.where(up_mask, sb, 0.0)
        out = jnp.dot(scores.astype(bf16), v, preferred_element_type=f32)
        qd = q * jnp.exp(wf)
        lift_f_ref[sl, :] = (qd * jnp.exp(before)).astype(bf16)
        if n > 0:
            out = out + nt(qd.astype(bf16), state.astype(bf16))
        o_ref[sl, :] = out
        if n < blocks - 1:
            state = jnp.exp(tot_f[n]) * state + tn(v, (k * jnp.exp(tot_f[n] - wf)).astype(bf16))
        before = before + tot_f[n]
    state = jnp.zeros((DK, DK), f32)
    after = jnp.zeros((1, DK), f32)
    for n in reversed(range(blocks)):
        sl = slice(n * BLOCK, (n + 1) * BLOCK)
        q = q_ref[sl, :].astype(f32)
        k = k_ref[sl, :].astype(f32)
        v = v_ref[sl, :]
        wb = cum_ref[1, sl, :]
        qd = q * jnp.exp(wb)
        lift_b_ref[sl, :] = (qd * jnp.exp(after)).astype(bf16)
        if n < blocks - 1:
            o_ref[sl, :] = o_ref[sl, :] + nt(qd.astype(bf16), state.astype(bf16))
        if n > 0:
            state = jnp.exp(tot_b[n]) * state + tn(v, (k * jnp.exp(tot_b[n] - wb)).astype(bf16))
        after = after + tot_b[n]


def combine_kernel(in_ref, o_ref, lift_f_ref, lift_b_ref, out_ref):
    seg = lax.axis_index("A")

    def vec(peer, at):
        rows = in_ref[peer, 320:328, :].astype(f32)
        return rows[at : at + 1] + rows[at + 1 : at + 2]

    ctx_f = jnp.zeros((DK, DK), f32)
    ctx_b = jnp.zeros((DK, DK), f32)
    for q in range(4):
        ctx_f = jnp.exp(vec(q, 2)) * ctx_f + tn(in_ref[q, 256:320, :], in_ref[q, 128:192, :])
    for q in reversed(range(4)):
        ctx_b = jnp.exp(vec(q, 4)) * ctx_b + tn(in_ref[q, 256:320, :], in_ref[q, 192:256, :])
    fwd = CTX_LIFT * ctx_f
    for a in range(3):
        moved = jnp.exp(vec(a, 0)) * fwd + in_ref[a, 0:128, :].astype(f32)
        fwd = jnp.where(a < seg, moved, fwd)
    bwd = CTX_LIFT * ctx_b
    for a in (3, 2, 1):
        moved = jnp.exp(vec(a, 0)) * bwd + in_ref[a, 0:128, :].astype(f32)
        bwd = jnp.where(a > seg, moved, bwd)
    out = o_ref[...] + nt(lift_f_ref[...], fwd.astype(bf16)) + nt(lift_b_ref[...], bwd.astype(bf16))
    out_ref[...] = out.astype(bf16)


def output_kernel(mix_ref, gain_ref, w_ref, out_ref):
    total = None
    flip = lax.axis_index("A") // 2
    for h in range(2):
        at = 2 * (h ^ flip)
        v = jnp.concatenate([mix_ref[at], mix_ref[at + 1]], axis=1).astype(f32)
        r = lax.rsqrt(jnp.mean(v * v, axis=-1, keepdims=True) + EPS)
        n = (v * r * gain_ref[...]).astype(bf16)
        part = jnp.dot(n, w_ref[h * 256 : (h + 1) * 256, :], preferred_element_type=f32)
        total = part if total is None else total + part
    out_ref[...] = total.astype(bf16)


def device_body(
    latents,
    sample_vector,
    context,
    context_vector,
    norm_gain,
    modulator,
    query_weight,
    key_weight,
    value_weight,
    decay_down,
    decay_up,
    decay_bias,
    decay_extra,
    head_gain,
    out_weight,
):
    sds = jax.ShapeDtypeStruct
    rows, cut = pl.pallas_call(
        pack_kernel,
        out_shape=(sds((36, D), bf16), sds((16, 56, 128), bf16)),
        in_specs=[VM] * 9,
        out_specs=(VM, VM),
        compiler_params=pltpu.CompilerParams(vmem_limit_bytes=12 * 1024 * 1024),
        name="pack",
    )(
        *off_chip(
            latents, context, sample_vector, context_vector, modulator.T,
            query_weight, key_weight, value_weight,
            jnp.moveaxis(decay_extra, 1, 2).reshape(4, 128),
        )
    )
    down = lax.optimization_barrier(decay_down.T.reshape(64, D)).T
    near = [rows]
    for j in range(1, 4):
        near.append(lax.ppermute(rows, "B", [(b, b ^ j) for b in range(4)]))
    rows_z = lax.all_to_all(cut, ("A", "B"), 0, 0, tiled=True)
    mine = to_everyone(rows_z[:, 0:48], "x")
    other = lax.ppermute(mine, "core", [(0, 1), (1, 0)])
    ride = rows_z[:, 48:56]
    mods = jnp.transpose(ride, (1, 0, 2)).reshape(8, D)
    far_mods = lax.ppermute(mods, "tp", [(i, i ^ 2) for i in range(4)])

    own = jnp.concatenate([n[:32] for n in near] + [n[32:36] for n in near], axis=0)
    up_shift = [(i, (i + 1) % 4) for i in range(4)]
    down_shift = [(i, (i + 3) % 4) for i in range(4)]
    minus = lax.ppermute(own, "tp", up_shift)
    plus = lax.ppermute(own, "tp", down_shift)
    low = lax.ppermute(jnp.concatenate([minus[:64], mods]), "tp", up_shift)
    high = lax.ppermute(jnp.concatenate([plus[64:], mods]), "tp", down_shift)

    hidden, modulation = pl.pallas_call(
        hidden_kernel,
        out_shape=(sds((ROWS, D), bf16), pltpu.HBM((2, 3 * D), f32)),
        in_specs=[VM] * 8,
        out_specs=(VM, VM),
        scratch_shapes=[pltpu.VMEM((4, 8, D), f32)],
        compiler_params=pltpu.CompilerParams(vmem_limit_bytes=16 * 1024 * 1024),
        name="hidden",
    )(*on_chip(own, minus, plus, low, high, mods, far_mods), *off_chip(norm_gain.reshape(1, D)))
    payload, q, k, v, cum = pl.pallas_call(
        project_kernel,
        out_shape=(
            sds((4, PAYLOAD, DK), bf16),
            pltpu.HBM((SEG, DK), bf16),
            pltpu.HBM((SEG, DK), bf16),
            pltpu.HBM((SEG, DK), bf16),
            pltpu.HBM((2, SEG, DK), f32),
        ),
        in_specs=[VM] * 7,
        out_specs=(VM,) * 5,
        scratch_shapes=[
            pltpu.VMEM((D, 448), bf16),
            pltpu.VMEM((ROWS, 384), bf16),
            pltpu.VMEM((ROWS, 256), f32),
        ],
        compiler_params=pltpu.CompilerParams(vmem_limit_bytes=24 * 1024 * 1024),
        name="project",
    )(
        *on_chip(hidden, mine, other), *off_chip(down, decay_up, decay_bias), *on_chip(ride),
    )
    got = lax.all_to_all(
        payload, ("A", "B"), 0, 0, tiled=True, axis_index_groups=PEERS
    )
    local, lift_f, lift_b = pl.pallas_call(
        local_kernel,
        out_shape=(sds((SEG, DK), f32), sds((SEG, DK), bf16), sds((SEG, DK), bf16)),
        in_specs=[VM] * 4,
        out_specs=(VM,) * 3,
        compiler_params=pltpu.CompilerParams(vmem_limit_bytes=12 * 1024 * 1024),
        name="local",
    )(*off_chip(q, k, v, cum))
    mixed = pl.pallas_call(
        combine_kernel,
        out_shape=sds((SEG, DK), bf16),
        in_specs=[VM] * 4,
        out_specs=VM,
        compiler_params=pltpu.CompilerParams(vmem_limit_bytes=12 * 1024 * 1024),
        name="combine",
    )(*on_chip(got, local, lift_f, lift_b))
    heads = lax.all_to_all(mixed.reshape(4, 128, DK), "B", 0, 0, tiled=True)
    partial = pl.pallas_call(
        output_kernel,
        out_shape=sds((128, D), bf16),
        in_specs=[VM] * 3,
        out_specs=VM,
        compiler_params=pltpu.CompilerParams(vmem_limit_bytes=16 * 1024 * 1024),
        name="output",
    )(*on_chip(heads), *off_chip(head_gain.reshape(1, 256)), *on_chip(out_weight))
    shares = lax.all_to_all(partial.reshape(4, 32, D), "tp", 0, 0, tiled=True)
    projected = shares.astype(f32).sum(axis=0)
    projected = lax.optimization_barrier(projected.astype(bf16)).astype(f32)
    return (latents.astype(f32) + modulation[0:1, 2 * D :] * projected).astype(bf16)


def solution(mesh):
    mesh = Mesh(mesh.devices.reshape(4, 4, 4, 4, 2), ("A", "B", "tp", "x", "core"))
    dp = ("x", "core")
    sp = ("A", "B")
    placed = (
        P((*dp, *sp, "tp"), None),
        P(dp, None),
        P((*dp, *sp), None),
        P(),
        P(),
        P(None, (*sp, "tp")),
        P(sp, "tp"),
        P(sp, "tp"),
        P(sp, "tp"),
        P(),
        P(None, None, "tp"),
        P(None, "tp"),
        P(None, (*dp, *sp), "tp"),
        P(),
        P("tp", None),
    )
    return jax.shard_map(
        device_body,
        mesh=mesh,
        in_specs=placed,
        out_specs=P((*dp, *sp, "tp"), None),
        check_vma=False,
    )
```

```python
import jax
import jax.numpy as jnp
from jax import lax
from jax.experimental import pallas as pl
from jax.experimental.pallas import tpu as pltpu
from jax.sharding import Mesh, PartitionSpec as P


D = 2048
DK = 128
RANK = 32
BLOCK = 64
CTX_LIFT = 4.0
EPS = 1e-06
SHARP = 16.0
SEG = 512
CTX_SEG = 64
ROWS = SEG + CTX_SEG
PAYLOAD = 328
bf16 = jnp.bfloat16
f32 = jnp.float32
VM = pl.BlockSpec(memory_space=pltpu.VMEM)
SM = pl.BlockSpec(memory_space=pltpu.SMEM)


def on_chip(*arrays):
    return tuple(pltpu.with_memory_space_constraint(a, pltpu.VMEM) for a in arrays)


def off_chip(*arrays):
    return tuple(pltpu.with_memory_space_constraint(a, pltpu.HBM) for a in arrays)


def to_everyone(x, axis):
    size = lax.axis_size(axis)
    return lax.all_to_all(jnp.broadcast_to(x[None], (size, *x.shape)), axis, 0, 0, tiled=True)


def role(seg, sub):
    return sub ^ (seg // 2 * 2)


PEERS = [[4 * a + role(a, b) for a in range(4)] for b in range(4)]


def three_parts(x):
    hi = x.astype(bf16)
    rest = x - hi.astype(f32)
    mid = rest.astype(bf16)
    lo = (rest - mid.astype(f32)).astype(bf16)
    return hi, mid, lo


def tri(rows, cols, upper):
    r = lax.broadcasted_iota(jnp.int32, (rows, cols), 0)
    c = lax.broadcasted_iota(jnp.int32, (rows, cols), 1)
    return (c >= r) if upper else (c <= r)


def summed_by(mask, a):
    m = mask.astype(f32).astype(bf16)
    stacked = jnp.concatenate(three_parts(a), axis=0)
    return jnp.dot(jnp.concatenate([m, m, m], axis=1), stacked, preferred_element_type=f32)


def nt(a, b):
    return lax.dot_general(a, b, (((1,), (1,)), ((), ())), preferred_element_type=f32)


def tn(a, b):
    return lax.dot_general(a, b, (((0,), (0,)), ((), ())), preferred_element_type=f32)


def pack_kernel(
    lat_ref, ctx_ref, sv_ref, cv_ref, mod_ref, wq_ref, wk_ref, wv_ref, extra_ref, rows_ref, cut_ref
):
    y = lax.axis_index("tp")
    dp = lax.axis_index("x") * 2 + lax.axis_index("core")
    rows_ref[0:32, :] = lat_ref[...]
    ctx = ctx_ref[...].astype(f32)
    picked = ctx[12:16]
    for i in range(3):
        picked = jnp.where(y == i, ctx[4 * i : 4 * i + 4], picked)
    rows_ref[32:36, :] = picked.astype(bf16)

    both = jnp.concatenate([sv_ref[...], cv_ref[...]], axis=0)
    conditions = (both / (1.0 + jnp.exp(-both))).astype(bf16)
    local_mods = nt(conditions, mod_ref[...])
    mods = jnp.concatenate([p.astype(f32) for p in three_parts(local_mods)[:2]], axis=0)
    mods = jnp.concatenate([mods, jnp.zeros((4, 32), f32)], axis=1)
    e_hi, e_mid, _ = three_parts(extra_ref[...])
    e_hi, e_mid = e_hi.astype(f32), e_mid.astype(f32)
    riding = []
    for h in range(2):
        added = [e_hi[h : h + 1], e_mid[h : h + 1], e_hi[2 + h : 3 + h], e_mid[2 + h : 3 + h]]
        riding.append(jnp.concatenate([mods, *added], axis=0).astype(bf16))
    mine = pl.ds(pl.multiple_of(dp * 16, 16), 16)
    for d in range(16):
        b = role(d // 4, d % 4)
        h = b // 2
        cut_ref[d, 0:16, :] = wq_ref[mine, h * 128 : (h + 1) * 128]
        cut_ref[d, 16:32, :] = wk_ref[mine, h * 128 : (h + 1) * 128]
        cut_ref[d, 32:48, :] = wv_ref[mine, b * 128 : (b + 1) * 128]
        cut_ref[d, 48:56, :] = riding[h]


def normed_rows(rows, which, mod_ref, gain_ref):
    v = rows.astype(f32)
    r = lax.rsqrt(jnp.mean(v * v, axis=-1, keepdims=True) + EPS)
    scale = gain_ref[...] * (1.0 + mod_ref[which : which + 1, D : 2 * D])
    return (v * r * scale + mod_ref[which : which + 1, 0:D]).astype(bf16)


def hidden_kernel(
    own_ref, minus_ref, plus_ref, low_ref, high_ref, own_mods_ref, far_mods_ref, gain_ref,
    h_ref, gate_ref, mod_ref, mods_ref,
):
    y = lax.axis_index("tp")
    mods_ref[y] = own_mods_ref[...].astype(f32)
    mods_ref[(y + 3) % 4] = low_ref[64:72, :].astype(f32)
    mods_ref[(y + 1) % 4] = high_ref[80:88, :].astype(f32)
    mods_ref[(y + 2) % 4] = far_mods_ref[...].astype(f32)
    for z in range(16):
        at = slice(z * 128, z * 128 + 96)
        parts = [mods_ref[i, 0:2, at] + mods_ref[i, 2:4, at] for i in range(4)]
        mod_ref[:, z * 384 : (z + 1) * 384] = jnp.concatenate(parts, axis=1)
    gate_ref[...] = mod_ref[0:1, 2 * D : 3 * D]
    for slot in range(4):
        for j in range(5):
            size = 32 if j < 4 else 16
            if slot < 3:
                rows = (own_ref, minus_ref, plus_ref)[slot][j * 32 : j * 32 + size, :]
            elif j < 2:
                rows = low_ref[j * 32 : j * 32 + 32, :]
            else:
                rows = high_ref[j * 32 - 64 : j * 32 - 64 + size, :]
            at = slot * 144 + j * 32
            h_ref[at : at + size, :] = normed_rows(rows, j // 4, mod_ref, gain_ref)


def decays_of(low, up_ref, bias_ref):
    second = role(lax.axis_index("A"), lax.axis_index("B")) >= 2

    def of_head(a):
        return jnp.where(second, a[:, 128:256].astype(f32), a[:, 0:128].astype(f32))

    raw = []
    for z in range(2):
        up = of_head(up_ref[z]).astype(bf16)
        part = jnp.dot(low[:, z * RANK : (z + 1) * RANK], up, preferred_element_type=f32)
        raw.append(part + of_head(bias_ref[z : z + 1, :]))
    raw = jnp.concatenate(raw, axis=1)
    return (jnp.minimum(raw, 0.0) - jnp.log1p(jnp.exp(-jnp.abs(raw)))) * (1.0 / SHARP)


def project_kernel(
    h_ref, mine_ref, other_ref, down_ref, up_ref, bias_ref, ride_ref,
    pay_ref, q_ref, k_ref, v_ref, cum_ref, w_ref, out_ref, all_logs_ref,
):
    seg, sub = lax.axis_index("A"), lax.axis_index("B")
    y, core = lax.axis_index("tp"), lax.axis_index("core")
    for xi in range(4):
        for z in range(16):
            at = z * 128 + xi * 32
            here = pl.ds(pl.multiple_of(at + core * 16, 16), 16)
            there = pl.ds(pl.multiple_of(at + 16 - core * 16, 16), 16)
            for j in range(3):
                cols = slice(j * 128, (j + 1) * 128)
                w_ref[here, cols] = mine_ref[xi, z, j * 16 : (j + 1) * 16, :]
                w_ref[there, cols] = other_ref[xi, z, j * 16 : (j + 1) * 16, :]
    w_ref[:, 384:448] = down_ref[...]
    y_of = [y, (y + 3) % 4, (y + 1) % 4, (y + 2) % 4]
    res = jnp.dot(h_ref[...], w_ref[...], preferred_element_type=f32).astype(bf16)
    slot_logs = decays_of(res[:, 384:448], up_ref, bias_ref)
    slot_qkv = res[:, 0:384]
    for n in range(4):
        for j in range(5):
            size = 32 if j < 4 else 16
            took = slice(n * 144 + j * 32, n * 144 + j * 32 + size)
            if j < 4:
                at = pl.ds(pl.multiple_of((sub ^ j) * 128 + y_of[n] * 32, 32), size)
            else:
                at = pl.ds(SEG + n * 16, size)
            out_ref[at, :] = slot_qkv[took]
            all_logs_ref[at, :] = slot_logs[took]
    out = out_ref[...]
    logs = all_logs_ref[...]
    q_ref[...] = out[:SEG, 0:128]
    k_ref[...] = out[:SEG, 128:256]
    v_ref[...] = out[:SEG, 256:384]
    ef, eb = [], []
    for zb in range(4):
        t = jnp.transpose(ride_ref[seg * 4 + zb].astype(f32))
        ef.append(t[:, 4:5] + t[:, 5:6])
        eb.append(t[:, 6:7] + t[:, 7:8])
    ef = jnp.concatenate(ef, axis=0)
    eb = jnp.concatenate(eb, axis=0)
    af = logs[:SEG, 0:128] + ef
    ab = logs[:SEG, 128:256] + eb
    low_mask = tri(BLOCK, BLOCK, False)
    up_mask = tri(BLOCK, BLOCK, True)
    wf, wb = [], []
    for n in range(SEG // BLOCK):
        sl = slice(n * BLOCK, (n + 1) * BLOCK)
        wf.append(summed_by(low_mask, af[sl]))
        wb.append(summed_by(up_mask, ab[sl]))
        cum_ref[0, sl, :] = wf[-1]
        cum_ref[1, sl, :] = wb[-1]
    tot_f = [w[BLOCK - 1 : BLOCK] for w in wf]
    tot_b = [w[0:1] for w in wb]
    dev_f = sum(tot_f)
    dev_b = sum(tot_b)
    kk = out[:SEG, 128:256].astype(f32)
    before = jnp.zeros((1, DK), f32)
    kf = []
    for n in range(SEG // BLOCK):
        kf.append(kk[n * BLOCK : (n + 1) * BLOCK] * jnp.exp(dev_f - before - wf[n]))
        before = before + tot_f[n]
    after = jnp.zeros((1, DK), f32)
    kb = [None] * (SEG // BLOCK)
    for n in reversed(range(SEG // BLOCK)):
        kb[n] = kk[n * BLOCK : (n + 1) * BLOCK] * jnp.exp(dev_b - after - wb[n])
        after = after + tot_b[n]
    both = jnp.concatenate(
        [jnp.concatenate(kf, 0).astype(bf16), jnp.concatenate(kb, 0).astype(bf16)], axis=1
    )
    states = tn(out[:SEG, 256:384], both).astype(bf16)

    def order(i):
        slot = i // 16
        step = jnp.where(slot == 0, 0, jnp.where(slot == 1, 3, slot - 1))
        return (((i % 16) // 4) ^ sub) * 16 + ((step + y) % 4) * 4 + i % 4

    r = order(lax.broadcasted_iota(jnp.int32, (CTX_SEG, CTX_SEG), 0))
    c = order(lax.broadcasted_iota(jnp.int32, (CTX_SEG, CTX_SEG), 1))
    later = summed_by(c > r, logs[SEG:, 0:128])
    earlier = summed_by(c < r, logs[SEG:, 128:256])
    ctx_f = jnp.sum(logs[SEG:, 0:128], axis=0, keepdims=True)
    ctx_b = jnp.sum(logs[SEG:, 128:256], axis=0, keepdims=True)
    ck = out[SEG:, 128:256].astype(f32)
    ckf = (ck * jnp.exp(later)).astype(bf16)
    ckb = (ck * jnp.exp(earlier)).astype(bf16)
    cv = out[SEG:, 256:384]
    zero = jnp.zeros((2, DK), bf16)
    for peer in range(4):
        ahead = peer > seg
        pay_ref[peer, 0:128, :] = jnp.where(ahead, states[:, 0:128], states[:, 128:256])
        pay_ref[peer, 128:192, :] = ckf
        pay_ref[peer, 192:256, :] = ckb
        pay_ref[peer, 256:320, :] = cv
        dev = jnp.where(ahead, dev_f, dev_b)
        two = [p for t in (dev, ctx_f, ctx_b) for p in three_parts(t)[:2]]
        pay_ref[peer, 320:328, :] = jnp.concatenate([*two, zero], axis=0)


def local_kernel(q_ref, k_ref, v_ref, cum_ref, o_ref, lift_f_ref, lift_b_ref):
    blocks = SEG // BLOCK
    low_mask = tri(BLOCK, BLOCK, False)
    up_mask = tri(BLOCK, BLOCK, True)
    tot_f = [cum_ref[0, (n + 1) * BLOCK - 1 : (n + 1) * BLOCK, :] for n in range(blocks)]
    tot_b = [cum_ref[1, n * BLOCK : n * BLOCK + 1, :] for n in range(blocks)]
    state = jnp.zeros((DK, DK), f32)
    before = jnp.zeros((1, DK), f32)
    for n in range(blocks):
        sl = slice(n * BLOCK, (n + 1) * BLOCK)
        q = q_ref[sl, :].astype(f32)
        k = k_ref[sl, :].astype(f32)
        v = v_ref[sl, :]
        wf = cum_ref[0, sl, :]
        wb = cum_ref[1, sl, :]
        mf = 0.5 * tot_f[n]
        mb = 0.5 * tot_b[n]
        sf = nt((q * jnp.exp(wf - mf)).astype(bf16), (k * jnp.exp(mf - wf)).astype(bf16))
        sb = nt((q * jnp.exp(wb - mb)).astype(bf16), (k * jnp.exp(mb - wb)).astype(bf16))
        scores = jnp.where(low_mask, sf, 0.0) + jnp.where(up_mask, sb, 0.0)
        out = jnp.dot(scores.astype(bf16), v, preferred_element_type=f32)
        qd = q * jnp.exp(wf)
        lift_f_ref[sl, :] = (qd * jnp.exp(before)).astype(bf16)
        if n > 0:
            out = out + nt(qd.astype(bf16), state.astype(bf16))
        o_ref[sl, :] = out
        if n < blocks - 1:
            state = jnp.exp(tot_f[n]) * state + tn(v, (k * jnp.exp(tot_f[n] - wf)).astype(bf16))
        before = before + tot_f[n]
    state = jnp.zeros((DK, DK), f32)
    after = jnp.zeros((1, DK), f32)
    for n in reversed(range(blocks)):
        sl = slice(n * BLOCK, (n + 1) * BLOCK)
        q = q_ref[sl, :].astype(f32)
        k = k_ref[sl, :].astype(f32)
        v = v_ref[sl, :]
        wb = cum_ref[1, sl, :]
        qd = q * jnp.exp(wb)
        lift_b_ref[sl, :] = (qd * jnp.exp(after)).astype(bf16)
        if n < blocks - 1:
            o_ref[sl, :] = o_ref[sl, :] + nt(qd.astype(bf16), state.astype(bf16))
        if n > 0:
            state = jnp.exp(tot_b[n]) * state + tn(v, (k * jnp.exp(tot_b[n] - wb)).astype(bf16))
        after = after + tot_b[n]


def combine_kernel(in_ref, o_ref, lift_f_ref, lift_b_ref, out_ref):
    seg = lax.axis_index("A")

    def vec(peer, at):
        rows = in_ref[peer, 320:328, :].astype(f32)
        return rows[at : at + 1] + rows[at + 1 : at + 2]

    ctx_f = jnp.zeros((DK, DK), f32)
    ctx_b = jnp.zeros((DK, DK), f32)
    for q in range(4):
        ctx_f = jnp.exp(vec(q, 2)) * ctx_f + tn(in_ref[q, 256:320, :], in_ref[q, 128:192, :])
    for q in reversed(range(4)):
        ctx_b = jnp.exp(vec(q, 4)) * ctx_b + tn(in_ref[q, 256:320, :], in_ref[q, 192:256, :])
    fwd = CTX_LIFT * ctx_f
    for a in range(3):
        moved = jnp.exp(vec(a, 0)) * fwd + in_ref[a, 0:128, :].astype(f32)
        fwd = jnp.where(a < seg, moved, fwd)
    bwd = CTX_LIFT * ctx_b
    for a in (3, 2, 1):
        moved = jnp.exp(vec(a, 0)) * bwd + in_ref[a, 0:128, :].astype(f32)
        bwd = jnp.where(a > seg, moved, bwd)
    out = o_ref[...] + nt(lift_f_ref[...], fwd.astype(bf16)) + nt(lift_b_ref[...], bwd.astype(bf16))
    out_ref[...] = out.astype(bf16)


def output_kernel(mix_ref, gain_ref, w_ref, out_ref):
    total = None
    flip = lax.axis_index("A") // 2
    for h in range(2):
        at = 2 * (h ^ flip)
        v = jnp.concatenate([mix_ref[at], mix_ref[at + 1]], axis=1).astype(f32)
        r = lax.rsqrt(jnp.mean(v * v, axis=-1, keepdims=True) + EPS)
        n = (v * r * gain_ref[...]).astype(bf16)
        part = jnp.dot(n, w_ref[h * 256 : (h + 1) * 256, :], preferred_element_type=f32)
        total = part if total is None else total + part
    out_ref[...] = total.astype(bf16)


def device_body(
    latents,
    sample_vector,
    context,
    context_vector,
    norm_gain,
    modulator,
    query_weight,
    key_weight,
    value_weight,
    decay_down,
    decay_up,
    decay_bias,
    decay_extra,
    head_gain,
    out_weight,
):
    sds = jax.ShapeDtypeStruct
    rows, cut = pl.pallas_call(
        pack_kernel,
        out_shape=(sds((36, D), bf16), sds((16, 56, 128), bf16)),
        in_specs=[VM] * 9,
        out_specs=(VM, VM),
        compiler_params=pltpu.CompilerParams(vmem_limit_bytes=12 * 1024 * 1024),
        name="pack",
    )(
        *off_chip(
            latents, context, sample_vector, context_vector, modulator.T,
            query_weight, key_weight, value_weight,
            jnp.moveaxis(decay_extra, 1, 2).reshape(4, 128),
        )
    )
    down = lax.optimization_barrier(decay_down.T.reshape(64, D)).T
    near = [rows]
    for j in range(1, 4):
        near.append(lax.ppermute(rows, "B", [(b, b ^ j) for b in range(4)]))
    rows_z = lax.all_to_all(cut, ("A", "B"), 0, 0, tiled=True)
    mine = to_everyone(rows_z[:, 0:48], "x")
    other = lax.ppermute(mine, "core", [(0, 1), (1, 0)])
    ride = rows_z[:, 48:56]
    mods = jnp.transpose(ride, (1, 0, 2)).reshape(8, D)
    far_mods = lax.ppermute(mods, "tp", [(i, i ^ 2) for i in range(4)])

    own = jnp.concatenate([n[:32] for n in near] + [n[32:36] for n in near], axis=0)
    up_shift = [(i, (i + 1) % 4) for i in range(4)]
    down_shift = [(i, (i + 3) % 4) for i in range(4)]
    minus = lax.ppermute(own, "tp", up_shift)
    plus = lax.ppermute(own, "tp", down_shift)
    low = lax.ppermute(jnp.concatenate([minus[:64], mods]), "tp", up_shift)
    high = lax.ppermute(jnp.concatenate([plus[64:], mods]), "tp", down_shift)

    hidden, gate = pl.pallas_call(
        hidden_kernel,
        out_shape=(sds((ROWS, D), bf16), pltpu.HBM((1, D), f32)),
        in_specs=[VM] * 8,
        out_specs=(VM, VM),
        scratch_shapes=[pltpu.VMEM((2, 3 * D), f32), pltpu.VMEM((4, 8, D), f32)],
        compiler_params=pltpu.CompilerParams(vmem_limit_bytes=16 * 1024 * 1024),
        name="hidden",
    )(*on_chip(own, minus, plus, low, high, mods, far_mods), *off_chip(norm_gain.reshape(1, D)))
    payload, q, k, v, cum = pl.pallas_call(
        project_kernel,
        out_shape=(
            sds((4, PAYLOAD, DK), bf16),
            pltpu.HBM((SEG, DK), bf16),
            pltpu.HBM((SEG, DK), bf16),
            pltpu.HBM((SEG, DK), bf16),
            pltpu.HBM((2, SEG, DK), f32),
        ),
        in_specs=[VM] * 7,
        out_specs=(VM,) * 5,
        scratch_shapes=[
            pltpu.VMEM((D, 448), bf16),
            pltpu.VMEM((ROWS, 384), bf16),
            pltpu.VMEM((ROWS, 256), f32),
        ],
        compiler_params=pltpu.CompilerParams(vmem_limit_bytes=24 * 1024 * 1024),
        name="project",
    )(
        *on_chip(hidden, mine, other), *off_chip(down, decay_up, decay_bias), *on_chip(ride),
    )
    got = lax.all_to_all(
        payload, ("A", "B"), 0, 0, tiled=True, axis_index_groups=PEERS
    )
    local, lift_f, lift_b = pl.pallas_call(
        local_kernel,
        out_shape=(sds((SEG, DK), f32), sds((SEG, DK), bf16), sds((SEG, DK), bf16)),
        in_specs=[VM] * 4,
        out_specs=(VM,) * 3,
        compiler_params=pltpu.CompilerParams(vmem_limit_bytes=12 * 1024 * 1024),
        name="local",
    )(*off_chip(q, k, v, cum))
    mixed = pl.pallas_call(
        combine_kernel,
        out_shape=sds((SEG, DK), bf16),
        in_specs=[VM] * 4,
        out_specs=VM,
        compiler_params=pltpu.CompilerParams(vmem_limit_bytes=12 * 1024 * 1024),
        name="combine",
    )(*on_chip(got, local, lift_f, lift_b))
    heads = lax.all_to_all(mixed.reshape(4, 128, DK), "B", 0, 0, tiled=True)
    partial = pl.pallas_call(
        output_kernel,
        out_shape=sds((128, D), bf16),
        in_specs=[VM] * 3,
        out_specs=VM,
        compiler_params=pltpu.CompilerParams(vmem_limit_bytes=16 * 1024 * 1024),
        name="output",
    )(*on_chip(heads), *off_chip(head_gain.reshape(1, 256)), *on_chip(out_weight))
    shares = lax.all_to_all(partial.reshape(4, 32, D), "tp", 0, 0, tiled=True)
    projected = shares.astype(f32).sum(axis=0)
    projected = lax.reduce_precision(projected, 8, 7)
    return (latents.astype(f32) + gate * projected).astype(bf16)


def solution(mesh):
    mesh = Mesh(mesh.devices.reshape(4, 4, 4, 4, 2), ("A", "B", "tp", "x", "core"))
    dp = ("x", "core")
    sp = ("A", "B")
    placed = (
        P((*dp, *sp, "tp"), None),
        P(dp, None),
        P((*dp, *sp), None),
        P(),
        P(),
        P(None, (*sp, "tp")),
        P(sp, "tp"),
        P(sp, "tp"),
        P(sp, "tp"),
        P(),
        P(None, None, "tp"),
        P(None, "tp"),
        P(None, (*dp, *sp), "tp"),
        P(),
        P("tp", None),
    )
    return jax.shard_map(
        device_body,
        mesh=mesh,
        in_specs=placed,
        out_specs=P((*dp, *sp, "tp"), None),
        check_vma=False,
    )
```

```python
import jax
import jax.numpy as jnp
from jax import lax
from jax.experimental import pallas as pl
from jax.experimental.pallas import tpu as pltpu
from jax.sharding import Mesh, PartitionSpec as P


D = 2048
DK = 128
RANK = 32
BLOCK = 64
CTX_LIFT = 4.0
EPS = 1e-06
SHARP = 16.0
SEG = 512
CTX_SEG = 64
ROWS = SEG + CTX_SEG
PAYLOAD = 328
bf16 = jnp.bfloat16
f32 = jnp.float32
VM = pl.BlockSpec(memory_space=pltpu.VMEM)
SM = pl.BlockSpec(memory_space=pltpu.SMEM)


def on_chip(*arrays):
    return tuple(pltpu.with_memory_space_constraint(a, pltpu.VMEM) for a in arrays)


def off_chip(*arrays):
    return tuple(pltpu.with_memory_space_constraint(a, pltpu.HBM) for a in arrays)


def to_everyone(x, axis):
    size = lax.axis_size(axis)
    return lax.all_to_all(jnp.broadcast_to(x[None], (size, *x.shape)), axis, 0, 0, tiled=True)


def role(seg, sub):
    return sub ^ (seg // 2 * 2)


PEERS = [[4 * a + role(a, b) for a in range(4)] for b in range(4)]


def three_parts(x):
    hi = x.astype(bf16)
    rest = x - hi.astype(f32)
    mid = rest.astype(bf16)
    lo = (rest - mid.astype(f32)).astype(bf16)
    return hi, mid, lo


def tri(rows, cols, upper):
    r = lax.broadcasted_iota(jnp.int32, (rows, cols), 0)
    c = lax.broadcasted_iota(jnp.int32, (rows, cols), 1)
    return (c >= r) if upper else (c <= r)


def summed_by(mask, a):
    m = mask.astype(f32).astype(bf16)
    stacked = jnp.concatenate(three_parts(a), axis=0)
    return jnp.dot(jnp.concatenate([m, m, m], axis=1), stacked, preferred_element_type=f32)


def nt(a, b):
    return lax.dot_general(a, b, (((1,), (1,)), ((), ())), preferred_element_type=f32)


def tn(a, b):
    return lax.dot_general(a, b, (((0,), (0,)), ((), ())), preferred_element_type=f32)


def pack_kernel(
    lat_ref, ctx_ref, sv_ref, cv_ref, mod_ref, wq_ref, wk_ref, wv_ref, extra_ref, rows_ref, cut_ref
):
    y = lax.axis_index("tp")
    dp = lax.axis_index("x") * 2 + lax.axis_index("core")
    rows_ref[0:32, :] = lat_ref[...]
    ctx = ctx_ref[...].astype(f32)
    picked = ctx[12:16]
    for i in range(3):
        picked = jnp.where(y == i, ctx[4 * i : 4 * i + 4], picked)
    rows_ref[32:36, :] = picked.astype(bf16)

    both = jnp.concatenate([sv_ref[...], cv_ref[...]], axis=0)
    conditions = (both / (1.0 + jnp.exp(-both))).astype(bf16)
    local_mods = nt(conditions, mod_ref[...])
    mods = jnp.concatenate([p.astype(f32) for p in three_parts(local_mods)[:2]], axis=0)
    mods = jnp.concatenate([mods, jnp.zeros((4, 32), f32)], axis=1)
    e_hi, e_mid, _ = three_parts(extra_ref[...])
    e_hi, e_mid = e_hi.astype(f32), e_mid.astype(f32)
    riding = []
    for h in range(2):
        added = [e_hi[h : h + 1], e_mid[h : h + 1], e_hi[2 + h : 3 + h], e_mid[2 + h : 3 + h]]
        riding.append(jnp.concatenate([mods, *added], axis=0).astype(bf16))
    mine = pl.ds(pl.multiple_of(dp * 16, 16), 16)
    for d in range(16):
        b = role(d // 4, d % 4)
        h = b // 2
        cut_ref[d, 0:16, :] = wq_ref[mine, h * 128 : (h + 1) * 128]
        cut_ref[d, 16:32, :] = wk_ref[mine, h * 128 : (h + 1) * 128]
        cut_ref[d, 32:48, :] = wv_ref[mine, b * 128 : (b + 1) * 128]
        cut_ref[d, 48:56, :] = riding[h]


def normed_rows(rows, which, mod_ref, gain_ref):
    v = rows.astype(f32)
    r = lax.rsqrt(jnp.mean(v * v, axis=-1, keepdims=True) + EPS)
    scale = gain_ref[...] * (1.0 + mod_ref[which : which + 1, D : 2 * D])
    return (v * r * scale + mod_ref[which : which + 1, 0:D]).astype(bf16)


def hidden_kernel(
    own_ref, minus_ref, plus_ref, low_ref, high_ref, own_mods_ref, far_mods_ref, gain_ref,
    h_ref, gate_ref, mod_ref, mods_ref,
):
    y = lax.axis_index("tp")
    mods_ref[y] = own_mods_ref[...].astype(f32)
    mods_ref[(y + 3) % 4] = low_ref[64:72, :].astype(f32)
    mods_ref[(y + 1) % 4] = high_ref[80:88, :].astype(f32)
    mods_ref[(y + 2) % 4] = far_mods_ref[...].astype(f32)
    for z in range(16):
        at = slice(z * 128, z * 128 + 96)
        parts = [mods_ref[i, 0:2, at] + mods_ref[i, 2:4, at] for i in range(4)]
        mod_ref[:, z * 384 : (z + 1) * 384] = jnp.concatenate(parts, axis=1)
    gate_ref[...] = jnp.broadcast_to(mod_ref[0:1, 2 * D : 3 * D], (8, D))
    for slot in range(4):
        for j in range(5):
            size = 32 if j < 4 else 16
            if slot < 3:
                rows = (own_ref, minus_ref, plus_ref)[slot][j * 32 : j * 32 + size, :]
            elif j < 2:
                rows = low_ref[j * 32 : j * 32 + 32, :]
            else:
                rows = high_ref[j * 32 - 64 : j * 32 - 64 + size, :]
            at = slot * 144 + j * 32
            h_ref[at : at + size, :] = normed_rows(rows, j // 4, mod_ref, gain_ref)


def decays_of(low, up_ref, bias_ref):
    second = role(lax.axis_index("A"), lax.axis_index("B")) >= 2

    def of_head(a):
        return jnp.where(second, a[:, 128:256].astype(f32), a[:, 0:128].astype(f32))

    raw = []
    for z in range(2):
        up = of_head(up_ref[z]).astype(bf16)
        part = jnp.dot(low[:, z * RANK : (z + 1) * RANK], up, preferred_element_type=f32)
        raw.append(part + of_head(bias_ref[z : z + 1, :]))
    raw = jnp.concatenate(raw, axis=1)
    return (jnp.minimum(raw, 0.0) - jnp.log1p(jnp.exp(-jnp.abs(raw)))) * (1.0 / SHARP)


def project_kernel(
    h_ref, mine_ref, other_ref, down_ref, up_ref, bias_ref, ride_ref,
    pay_ref, q_ref, k_ref, v_ref, cum_ref, w_ref, out_ref, all_logs_ref,
):
    seg, sub = lax.axis_index("A"), lax.axis_index("B")
    y, core = lax.axis_index("tp"), lax.axis_index("core")
    for xi in range(4):
        for z in range(16):
            at = z * 128 + xi * 32
            here = pl.ds(pl.multiple_of(at + core * 16, 16), 16)
            there = pl.ds(pl.multiple_of(at + 16 - core * 16, 16), 16)
            for j in range(3):
                cols = slice(j * 128, (j + 1) * 128)
                w_ref[here, cols] = mine_ref[xi, z, j * 16 : (j + 1) * 16, :]
                w_ref[there, cols] = other_ref[xi, z, j * 16 : (j + 1) * 16, :]
    w_ref[:, 384:448] = down_ref[...]
    y_of = [y, (y + 3) % 4, (y + 1) % 4, (y + 2) % 4]
    res = jnp.dot(h_ref[...], w_ref[...], preferred_element_type=f32).astype(bf16)
    slot_logs = decays_of(res[:, 384:448], up_ref, bias_ref)
    slot_qkv = res[:, 0:384]
    for n in range(4):
        for j in range(5):
            size = 32 if j < 4 else 16
            took = slice(n * 144 + j * 32, n * 144 + j * 32 + size)
            if j < 4:
                at = pl.ds(pl.multiple_of((sub ^ j) * 128 + y_of[n] * 32, 32), size)
            else:
                at = pl.ds(SEG + n * 16, size)
            out_ref[at, :] = slot_qkv[took]
            all_logs_ref[at, :] = slot_logs[took]
    out = out_ref[...]
    logs = all_logs_ref[...]
    q_ref[...] = out[:SEG, 0:128]
    k_ref[...] = out[:SEG, 128:256]
    v_ref[...] = out[:SEG, 256:384]
    ef, eb = [], []
    for zb in range(4):
        t = jnp.transpose(ride_ref[seg * 4 + zb].astype(f32))
        ef.append(t[:, 4:5] + t[:, 5:6])
        eb.append(t[:, 6:7] + t[:, 7:8])
    ef = jnp.concatenate(ef, axis=0)
    eb = jnp.concatenate(eb, axis=0)
    af = logs[:SEG, 0:128] + ef
    ab = logs[:SEG, 128:256] + eb
    low_mask = tri(BLOCK, BLOCK, False)
    up_mask = tri(BLOCK, BLOCK, True)
    wf, wb = [], []
    for n in range(SEG // BLOCK):
        sl = slice(n * BLOCK, (n + 1) * BLOCK)
        wf.append(summed_by(low_mask, af[sl]))
        wb.append(summed_by(up_mask, ab[sl]))
        cum_ref[0, sl, :] = wf[-1]
        cum_ref[1, sl, :] = wb[-1]
    tot_f = [w[BLOCK - 1 : BLOCK] for w in wf]
    tot_b = [w[0:1] for w in wb]
    dev_f = sum(tot_f)
    dev_b = sum(tot_b)
    kk = out[:SEG, 128:256].astype(f32)
    before = jnp.zeros((1, DK), f32)
    kf = []
    for n in range(SEG // BLOCK):
        kf.append(kk[n * BLOCK : (n + 1) * BLOCK] * jnp.exp(dev_f - before - wf[n]))
        before = before + tot_f[n]
    after = jnp.zeros((1, DK), f32)
    kb = [None] * (SEG // BLOCK)
    for n in reversed(range(SEG // BLOCK)):
        kb[n] = kk[n * BLOCK : (n + 1) * BLOCK] * jnp.exp(dev_b - after - wb[n])
        after = after + tot_b[n]
    both = jnp.concatenate(
        [jnp.concatenate(kf, 0).astype(bf16), jnp.concatenate(kb, 0).astype(bf16)], axis=1
    )
    states = tn(out[:SEG, 256:384], both).astype(bf16)

    def order(i):
        slot = i // 16
        step = jnp.where(slot == 0, 0, jnp.where(slot == 1, 3, slot - 1))
        return (((i % 16) // 4) ^ sub) * 16 + ((step + y) % 4) * 4 + i % 4

    r = order(lax.broadcasted_iota(jnp.int32, (CTX_SEG, CTX_SEG), 0))
    c = order(lax.broadcasted_iota(jnp.int32, (CTX_SEG, CTX_SEG), 1))
    later = summed_by(c > r, logs[SEG:, 0:128])
    earlier = summed_by(c < r, logs[SEG:, 128:256])
    ctx_f = jnp.sum(logs[SEG:, 0:128], axis=0, keepdims=True)
    ctx_b = jnp.sum(logs[SEG:, 128:256], axis=0, keepdims=True)
    ck = out[SEG:, 128:256].astype(f32)
    ckf = (ck * jnp.exp(later)).astype(bf16)
    ckb = (ck * jnp.exp(earlier)).astype(bf16)
    cv = out[SEG:, 256:384]
    zero = jnp.zeros((2, DK), bf16)
    for peer in range(4):
        ahead = peer > seg
        pay_ref[peer, 0:128, :] = jnp.where(ahead, states[:, 0:128], states[:, 128:256])
        pay_ref[peer, 128:192, :] = ckf
        pay_ref[peer, 192:256, :] = ckb
        pay_ref[peer, 256:320, :] = cv
        dev = jnp.where(ahead, dev_f, dev_b)
        two = [p for t in (dev, ctx_f, ctx_b) for p in three_parts(t)[:2]]
        pay_ref[peer, 320:328, :] = jnp.concatenate([*two, zero], axis=0)


def local_kernel(q_ref, k_ref, v_ref, cum_ref, o_ref, lift_f_ref, lift_b_ref):
    blocks = SEG // BLOCK
    low_mask = tri(BLOCK, BLOCK, False)
    up_mask = tri(BLOCK, BLOCK, True)
    tot_f = [cum_ref[0, (n + 1) * BLOCK - 1 : (n + 1) * BLOCK, :] for n in range(blocks)]
    tot_b = [cum_ref[1, n * BLOCK : n * BLOCK + 1, :] for n in range(blocks)]
    state = jnp.zeros((DK, DK), f32)
    before = jnp.zeros((1, DK), f32)
    for n in range(blocks):
        sl = slice(n * BLOCK, (n + 1) * BLOCK)
        q = q_ref[sl, :].astype(f32)
        k = k_ref[sl, :].astype(f32)
        v = v_ref[sl, :]
        wf = cum_ref[0, sl, :]
        wb = cum_ref[1, sl, :]
        mf = 0.5 * tot_f[n]
        mb = 0.5 * tot_b[n]
        sf = nt((q * jnp.exp(wf - mf)).astype(bf16), (k * jnp.exp(mf - wf)).astype(bf16))
        sb = nt((q * jnp.exp(wb - mb)).astype(bf16), (k * jnp.exp(mb - wb)).astype(bf16))
        scores = jnp.where(low_mask, sf, 0.0) + jnp.where(up_mask, sb, 0.0)
        out = jnp.dot(scores.astype(bf16), v, preferred_element_type=f32)
        qd = q * jnp.exp(wf)
        lift_f_ref[sl, :] = (qd * jnp.exp(before)).astype(bf16)
        if n > 0:
            out = out + nt(qd.astype(bf16), state.astype(bf16))
        o_ref[sl, :] = out
        if n < blocks - 1:
            state = jnp.exp(tot_f[n]) * state + tn(v, (k * jnp.exp(tot_f[n] - wf)).astype(bf16))
        before = before + tot_f[n]
    state = jnp.zeros((DK, DK), f32)
    after = jnp.zeros((1, DK), f32)
    for n in reversed(range(blocks)):
        sl = slice(n * BLOCK, (n + 1) * BLOCK)
        q = q_ref[sl, :].astype(f32)
        k = k_ref[sl, :].astype(f32)
        v = v_ref[sl, :]
        wb = cum_ref[1, sl, :]
        qd = q * jnp.exp(wb)
        lift_b_ref[sl, :] = (qd * jnp.exp(after)).astype(bf16)
        if n < blocks - 1:
            o_ref[sl, :] = o_ref[sl, :] + nt(qd.astype(bf16), state.astype(bf16))
        if n > 0:
            state = jnp.exp(tot_b[n]) * state + tn(v, (k * jnp.exp(tot_b[n] - wb)).astype(bf16))
        after = after + tot_b[n]


def combine_kernel(in_ref, o_ref, lift_f_ref, lift_b_ref, out_ref):
    seg = lax.axis_index("A")

    def vec(peer, at):
        rows = in_ref[peer, 320:328, :].astype(f32)
        return rows[at : at + 1] + rows[at + 1 : at + 2]

    ctx_f = jnp.zeros((DK, DK), f32)
    ctx_b = jnp.zeros((DK, DK), f32)
    for q in range(4):
        ctx_f = jnp.exp(vec(q, 2)) * ctx_f + tn(in_ref[q, 256:320, :], in_ref[q, 128:192, :])
    for q in reversed(range(4)):
        ctx_b = jnp.exp(vec(q, 4)) * ctx_b + tn(in_ref[q, 256:320, :], in_ref[q, 192:256, :])
    fwd = CTX_LIFT * ctx_f
    for a in range(3):
        moved = jnp.exp(vec(a, 0)) * fwd + in_ref[a, 0:128, :].astype(f32)
        fwd = jnp.where(a < seg, moved, fwd)
    bwd = CTX_LIFT * ctx_b
    for a in (3, 2, 1):
        moved = jnp.exp(vec(a, 0)) * bwd + in_ref[a, 0:128, :].astype(f32)
        bwd = jnp.where(a > seg, moved, bwd)
    out = o_ref[...] + nt(lift_f_ref[...], fwd.astype(bf16)) + nt(lift_b_ref[...], bwd.astype(bf16))
    out_ref[...] = out.astype(bf16)


def output_kernel(mix_ref, gain_ref, w_ref, out_ref):
    total = None
    flip = lax.axis_index("A") // 2
    for h in range(2):
        at = 2 * (h ^ flip)
        v = jnp.concatenate([mix_ref[at], mix_ref[at + 1]], axis=1).astype(f32)
        r = lax.rsqrt(jnp.mean(v * v, axis=-1, keepdims=True) + EPS)
        n = (v * r * gain_ref[...]).astype(bf16)
        part = jnp.dot(n, w_ref[h * 256 : (h + 1) * 256, :], preferred_element_type=f32)
        total = part if total is None else total + part
    out_ref[...] = total.astype(bf16)


def device_body(
    latents,
    sample_vector,
    context,
    context_vector,
    norm_gain,
    modulator,
    query_weight,
    key_weight,
    value_weight,
    decay_down,
    decay_up,
    decay_bias,
    decay_extra,
    head_gain,
    out_weight,
):
    sds = jax.ShapeDtypeStruct
    rows, cut = pl.pallas_call(
        pack_kernel,
        out_shape=(sds((36, D), bf16), sds((16, 56, 128), bf16)),
        in_specs=[VM] * 9,
        out_specs=(VM, VM),
        compiler_params=pltpu.CompilerParams(vmem_limit_bytes=12 * 1024 * 1024),
        name="pack",
    )(
        *off_chip(
            latents, context, sample_vector, context_vector, modulator.T,
            query_weight, key_weight, value_weight,
            jnp.moveaxis(decay_extra, 1, 2).reshape(4, 128),
        )
    )
    down = lax.optimization_barrier(decay_down.T.reshape(64, D)).T
    near = [rows]
    for j in range(1, 4):
        near.append(lax.ppermute(rows, "B", [(b, b ^ j) for b in range(4)]))
    rows_z = lax.all_to_all(cut, ("A", "B"), 0, 0, tiled=True)
    mine = to_everyone(rows_z[:, 0:48], "x")
    other = lax.ppermute(mine, "core", [(0, 1), (1, 0)])
    ride = rows_z[:, 48:56]
    mods = jnp.transpose(ride, (1, 0, 2)).reshape(8, D)
    far_mods = lax.ppermute(mods, "tp", [(i, i ^ 2) for i in range(4)])

    own = jnp.concatenate([n[:32] for n in near] + [n[32:36] for n in near], axis=0)
    up_shift = [(i, (i + 1) % 4) for i in range(4)]
    down_shift = [(i, (i + 3) % 4) for i in range(4)]
    minus = lax.ppermute(own, "tp", up_shift)
    plus = lax.ppermute(own, "tp", down_shift)
    low = lax.ppermute(jnp.concatenate([minus[:64], mods]), "tp", up_shift)
    high = lax.ppermute(jnp.concatenate([plus[64:], mods]), "tp", down_shift)

    hidden, gate = pl.pallas_call(
        hidden_kernel,
        out_shape=(sds((ROWS, D), bf16), pltpu.HBM((8, D), f32)),
        in_specs=[VM] * 8,
        out_specs=(VM, VM),
        scratch_shapes=[pltpu.VMEM((2, 3 * D), f32), pltpu.VMEM((4, 8, D), f32)],
        compiler_params=pltpu.CompilerParams(vmem_limit_bytes=16 * 1024 * 1024),
        name="hidden",
    )(*off_chip(own), *on_chip(minus, plus, low, high, mods, far_mods), *off_chip(norm_gain.reshape(1, D)))
    payload, q, k, v, cum = pl.pallas_call(
        project_kernel,
        out_shape=(
            sds((4, PAYLOAD, DK), bf16),
            pltpu.HBM((SEG, DK), bf16),
            pltpu.HBM((SEG, DK), bf16),
            pltpu.HBM((SEG, DK), bf16),
            pltpu.HBM((2, SEG, DK), f32),
        ),
        in_specs=[VM] * 7,
        out_specs=(VM,) * 5,
        scratch_shapes=[
            pltpu.VMEM((D, 448), bf16),
            pltpu.VMEM((ROWS, 384), bf16),
            pltpu.VMEM((ROWS, 256), f32),
        ],
        compiler_params=pltpu.CompilerParams(vmem_limit_bytes=24 * 1024 * 1024),
        name="project",
    )(
        *on_chip(hidden, mine, other), *off_chip(down, decay_up, decay_bias), *on_chip(ride),
    )
    got = lax.all_to_all(
        payload, ("A", "B"), 0, 0, tiled=True, axis_index_groups=PEERS
    )
    local, lift_f, lift_b = pl.pallas_call(
        local_kernel,
        out_shape=(sds((SEG, DK), f32), sds((SEG, DK), bf16), sds((SEG, DK), bf16)),
        in_specs=[VM] * 4,
        out_specs=(VM,) * 3,
        compiler_params=pltpu.CompilerParams(vmem_limit_bytes=12 * 1024 * 1024),
        name="local",
    )(*off_chip(q, k, v, cum))
    mixed = pl.pallas_call(
        combine_kernel,
        out_shape=sds((SEG, DK), bf16),
        in_specs=[VM] * 4,
        out_specs=VM,
        compiler_params=pltpu.CompilerParams(vmem_limit_bytes=12 * 1024 * 1024),
        name="combine",
    )(*on_chip(got, local, lift_f, lift_b))
    heads = lax.all_to_all(mixed.reshape(4, 128, DK), "B", 0, 0, tiled=True)
    partial = pl.pallas_call(
        output_kernel,
        out_shape=sds((128, D), bf16),
        in_specs=[VM] * 3,
        out_specs=VM,
        compiler_params=pltpu.CompilerParams(vmem_limit_bytes=16 * 1024 * 1024),
        name="output",
    )(*on_chip(heads), *off_chip(head_gain.reshape(1, 256)), *on_chip(out_weight))
    shares = lax.all_to_all(partial.reshape(4, 32, D), "tp", 0, 0, tiled=True)
    projected = shares.astype(f32).sum(axis=0)
    projected = lax.reduce_precision(projected, 8, 7)
    eight = (4, 8, D)
    updated = latents.astype(f32).reshape(eight) + gate[None] * projected.reshape(eight)
    return updated.astype(bf16).reshape(32, D)


def solution(mesh):
    mesh = Mesh(mesh.devices.reshape(4, 4, 4, 4, 2), ("A", "B", "tp", "x", "core"))
    dp = ("x", "core")
    sp = ("A", "B")
    placed = (
        P((*dp, *sp, "tp"), None),
        P(dp, None),
        P((*dp, *sp), None),
        P(),
        P(),
        P(None, (*sp, "tp")),
        P(sp, "tp"),
        P(sp, "tp"),
        P(sp, "tp"),
        P(),
        P(None, None, "tp"),
        P(None, "tp"),
        P(None, (*dp, *sp), "tp"),
        P(),
        P("tp", None),
    )
    return jax.shard_map(
        device_body,
        mesh=mesh,
        in_specs=placed,
        out_specs=P((*dp, *sp, "tp"), None),
        check_vma=False,
    )
```
